32 devices in a mesh: sp: 8 (over z, core), tp: 4 (over y, x).
Axes of the slice: x: 2, y: 2, z: 4, core: 2. Of those that a mesh axis runs over, the one named last changes fastest.
Arguments:
- receptance: bfloat16 [2048, 4096], P('sp', 'tp'), may hold values from -6 to 6
- key_vectors: bfloat16 [2048, 4096], P('sp', 'tp'), may hold values from -13 to 13
- value_vectors: bfloat16 [2048, 4096], P('sp', 'tp'), may hold values from -6 to 6
- decay_logits: bfloat16 [2048, 4096], P('sp', 'tp'), may hold values from -20 to 2
- rate_logits: bfloat16 [2048, 4096], P('sp', 'tp'), may hold values from -8 to 4
- gate_logits: bfloat16 [2048, 4096], P('sp', 'tp'), may hold values from -6 to 6
- group_gain: float32 [4096], P('tp'), may hold values from 0.1 to 1.9
- residual: bfloat16 [2048, 4096], P('sp', 'tp'), may hold values from -24 to 24
- mixer_out: bfloat16 [4096, 4096], P(None, 'tp'), may hold values from -0.09375 to 0.09375
- norm_gain: float32 [4096], P('tp'), may hold values from 0.1 to 1.9
- expert_ids: int32 [2048, 2], P('sp'), may hold values from 0 to 7, as said below
- route_weight: float32 [2048, 2], P('sp'), may hold values from 0.25 to 1
- expert_gate: bfloat16 [8, 4096, 1024], P('sp', 'tp'), may hold values from -0.09375 to 0.09375
- expert_up: bfloat16 [8, 4096, 1024], P('sp', 'tp'), may hold values from -0.09375 to 0.09375
- expert_down: bfloat16 [8, 1024, 4096], P('sp', None, 'tp'), may hold values from -0.1875 to 0.1875
Outputs:
- updated: bfloat16 [2048, 4096], P('sp', 'tp')
The draws below stay inside these ranges and needn't reach their ends.
Inputs may be any that keep to these rules, and one draw needn't show every extreme that they name: `expert_ids`: the experts of a row are different and lie in one group of 2 consecutive experts. In the rows of one index of sp (aligned blocks of 256 rows) no expert is named by more than 128 rows, and in every such block some expert is named by exactly 128 rows.
All inputs are finite; a program needn't handle non-finite values.
Results may differ from the reference program's by a relative error of at most 0.013.
Values may be sent and summed in bfloat16 or wider, within the bound.
A program may use at most 128 MiB of HBM per device.

```python
import math
import jax
import jax.numpy as jnp
from jax import lax

D = 4096
WIDTH = 4096
HEAD = 64
HEADS = 64
FF = 1024
GROUPS = 4
TOP = 2
TOK_SP = 256
EXPERTS = 8
GROUP_EXPERTS = 2
CAP = 128
SLOTS = 1024
TOKENS = 2048
CUTS = 4
DBLK = 1024
N_SP = 8


def fast_heads(key, count):
    order = jax.random.permutation(jax.random.fold_in(key, 7101), HEADS)
    return order < count


def draw_decay_logits(key, part):
    flags = fast_heads(key, HEADS // 2)
    noise = 0.6 * jnp.clip(jax.random.normal(jax.random.fold_in(key, 2), (TOKENS, WIDTH), jnp.float32), -3.0, 3.0)
    per_head = jnp.where(flags, math.log(1.0 / 16.0), math.log(0.8 / TOKENS))
    base = jnp.repeat(per_head, HEAD)
    channel = 0.3 * jnp.clip(jax.random.normal(jax.random.fold_in(key, 3), (WIDTH,), jnp.float32), -3.0, 3.0)
    halves = TOKENS // (TOK_SP // 2)
    drift = jax.random.uniform(jax.random.fold_in(key, 4), (halves, 1), jnp.float32, -1.1, 1.1)
    drift = jnp.repeat(drift, TOK_SP // 2, axis=0)
    log_rate = jnp.minimum(base[None, :] + channel[None, :] + drift + noise, -0.7)
    shifted = log_rate + 0.5
    return (shifted - jnp.log1p(-jnp.exp(shifted))).astype(jnp.bfloat16)


def draw_rate_logits(key, part):
    flags = fast_heads(key, HEADS // 2)
    spread = 0.7 * jnp.clip(jax.random.normal(jax.random.fold_in(key, 5), (TOKENS, WIDTH), jnp.float32), -2.4, 2.4)
    mixed_channels = jax.random.bernoulli(jax.random.fold_in(key, 6), 0.5, (WIDTH,))
    strong = jnp.logical_or(jnp.repeat(flags, HEAD), mixed_channels)
    centre = jnp.where(strong, 2.3, -6.0)
    width_scale = jnp.where(strong, 1.0, 0.5)
    return (centre[None, :] + width_scale[None, :] * spread).astype(jnp.bfloat16)


def draw_key_vectors(key, part):
    direction = jnp.clip(jax.random.normal(jax.random.fold_in(key, 21), (HEADS, HEAD), jnp.float32), -3.0, 3.0)
    along = 1.0 + 0.4 * jnp.clip(jax.random.normal(jax.random.fold_in(key, 22), (TOKENS, HEADS), jnp.float32), -2.0, 2.0)
    rough = jnp.clip(jax.random.normal(jax.random.fold_in(key, 23), (TOKENS, HEADS, HEAD), jnp.float32), -4.0, 4.0)
    keys = 1.5 * along[:, :, None] * direction[None, :, :] + rough
    return keys.reshape(TOKENS, WIDTH).astype(jnp.bfloat16)


def draw_residual(key, part):
    column_blocks = max(D // 128, 1)
    scales = jnp.exp(jax.random.uniform(jax.random.fold_in(key, 11), (column_blocks,), jnp.float32, math.log(0.4), math.log(2.5)))
    scales = jnp.repeat(scales, D // column_blocks)
    base = jnp.clip(jax.random.normal(jax.random.fold_in(key, 12), (TOKENS, D), jnp.float32), -5.0, 5.0)
    return (base * scales[None, :]).astype(jnp.bfloat16)


def draw_expert_ids(key, part):
    anchor = jax.random.fold_in(key, 9001)
    full_group = jax.random.randint(jax.random.fold_in(anchor, 1), (), 0, GROUPS)
    full_lead = jax.random.randint(jax.random.fold_in(anchor, 2), (), 0, GROUP_EXPERTS)
    block_keys = jax.random.split(jax.random.fold_in(anchor, 3), TOKENS // TOK_SP)
    spots = jnp.arange(GROUPS, dtype=jnp.int32)
    others_width = max(GROUP_EXPERTS - 1, 1)

    def one_block(block_key):
        keys_here = jax.random.split(block_key, 5)
        order = jax.random.permutation(keys_here[0], TOK_SP).astype(jnp.int32)
        held = jax.random.randint(keys_here[1], (), CAP, TOK_SP // 2 + 1)
        shift = jax.random.randint(keys_here[2], (), 0, GROUPS - 1)
        leads = jax.random.randint(keys_here[3], (GROUPS,), 0, GROUP_EXPERTS)
        leads = jnp.where(spots == full_group, full_lead, leads)
        shuffles = jax.vmap(lambda subkey: jax.random.permutation(subkey, others_width))(jax.random.split(keys_here[4], GROUPS)).astype(jnp.int32)
        in_full = order < held
        others = order - held
        group = jnp.where(in_full, full_group, (full_group + 1 + (others + shift) % (GROUPS - 1)) % GROUPS)
        rank = jnp.where(in_full, order, others // (GROUPS - 1))
        lead = leads[group]
        shuffle_rows = shuffles[group]

        def other_expert(position):
            pick = jnp.take_along_axis(shuffle_rows, (position % others_width)[:, None], axis=1)[:, 0]
            return (lead + 1 + pick) % GROUP_EXPERTS
        early = rank < CAP
        late_pos = CAP + 2 * (rank - CAP)
        first_pick = jnp.where(early, lead, other_expert(late_pos))
        second_pick = jnp.where(early, other_expert(rank), other_expert(late_pos + 1))
        return jnp.stack([group * GROUP_EXPERTS + first_pick, group * GROUP_EXPERTS + second_pick], axis=1)
    chosen = jax.vmap(one_block)(block_keys)
    return chosen.reshape(TOKENS, TOP).astype(jnp.int32)


def block_levels(own_key, extent, pieces, least, top_value):
    def one(dim, parts):
        steps = jax.random.uniform(jax.random.fold_in(jax.random.fold_in(own_key, 6), dim), (parts,), jnp.float32, least / len(pieces), top_value / len(pieces))
        return jnp.repeat(jnp.exp(steps), extent[dim] // parts).reshape((-1,) + (1,) * (len(extent) - dim - 1))

    loudness = one(*pieces[0])
    for cut in pieces[1:]:
        loudness = loudness * one(*cut)
    return loudness


def normal_values(key, dims, width, bound, cuts=(), kind=jnp.bfloat16):
    values = jax.random.normal(key, dims, jnp.float32) * width
    if len(cuts) > 0:
        values = block_levels(key, dims, cuts, -0.22, 0.18) * values
    return jnp.clip(values, min=-bound, max=bound).astype(kind)


def setup_inputs(seed: int = 0) -> dict:
    key_list = jax.random.split(jax.random.key(seed), 16)
    return {
        "receptance": normal_values(key_list[0], (TOKENS, WIDTH), 1.0, 6.0, ((0, 8), (1, 4))),
        "key_vectors": draw_key_vectors(jax.random.fold_in(key_list[15], 71), 0),
        "value_vectors": normal_values(key_list[2], (TOKENS, WIDTH), 1.0, 6.0, ((0, 8), (1, 4))),
        "decay_logits": draw_decay_logits(jax.random.fold_in(key_list[15], 71), 0),
        "rate_logits": draw_rate_logits(jax.random.fold_in(key_list[15], 71), 0),
        "gate_logits": normal_values(key_list[5], (TOKENS, WIDTH), 1.5, 6.0, ((0, 8), (1, 4))),
        "group_gain": jnp.clip(1.0 + 0.18 * jax.random.normal(key_list[6], (WIDTH,), jnp.float32), 0.1, 1.9),
        "residual": draw_residual(jax.random.fold_in(key_list[15], 71), 0),
        "mixer_out": normal_values(key_list[8], (WIDTH, D), WIDTH ** -0.5, 0.09375, ((1, 4),)),
        "norm_gain": jnp.clip(1.0 + 0.18 * jax.random.normal(key_list[9], (D,), jnp.float32), 0.1, 1.9),
        "expert_ids": draw_expert_ids(jax.random.fold_in(key_list[15], 71), 0),
        "route_weight": jnp.clip(0.25 + 0.75 * jax.random.uniform(key_list[11], (TOKENS, TOP), jnp.float32) ** block_levels(key_list[11], (TOKENS, TOP), ((0, 8),), -0.2, 0.2), 0.25, 1.0),
        "expert_gate": normal_values(key_list[12], (EXPERTS, D, FF), D ** -0.5, 0.09375, ((0, 8), (1, 4))),
        "expert_up": normal_values(key_list[13], (EXPERTS, D, FF), D ** -0.5, 0.09375, ((0, 8), (1, 4))),
        "expert_down": normal_values(key_list[14], (EXPERTS, FF, D), FF ** -0.5, 0.1875, ((0, 8), (2, 4))),
    }


EPS_GROUP = 0.00064
EPS_NORM = 1e-06
HIGHEST = lax.Precision.HIGHEST

def by_heads(array):
    return array.astype(jnp.float32).reshape(array.shape[0], WIDTH // HEAD, HEAD)

def time_mix(receptance, key_vectors, value_vectors, decay_logits, rate_logits, gate_logits, group_gain):
    recept = by_heads(receptance)
    keyvec = by_heads(key_vectors)
    valvec = by_heads(value_vectors)
    decay = jnp.exp(-jnp.exp(-jax.nn.softplus(-by_heads(decay_logits)) - 0.5))
    unit_key = keyvec / jnp.sqrt(1.0 + lax.optimization_barrier(jnp.sum(keyvec * keyvec, axis=-1, keepdims=True)))
    correction = unit_key * jax.nn.sigmoid(by_heads(rate_logits))

    def advance(carried, inputs):
        recept_now, decay_now, key_now, value_now, unit_now, corr_now = inputs
        pulled = jnp.einsum('hij,hj->hi', carried, unit_now, precision=HIGHEST)
        carried = carried * decay_now[:, None, :] - pulled[:, :, None] * corr_now[:, None, :] + value_now[:, :, None] * key_now[:, None, :]
        return (carried, jnp.einsum('hij,hj->hi', carried, recept_now, precision=HIGHEST))
    initial = jnp.zeros((WIDTH // HEAD, HEAD, HEAD), jnp.float32)
    final_state, state_read = lax.scan(advance, initial, (recept, decay, keyvec, valvec, unit_key, correction))
    centred = state_read - lax.optimization_barrier(jnp.mean(state_read, axis=-1, keepdims=True))
    scaled = centred * lax.rsqrt(lax.optimization_barrier(jnp.mean(centred * centred, axis=-1, keepdims=True)) + EPS_GROUP)
    gated_out = scaled.reshape(TOKENS, WIDTH) * group_gain.astype(jnp.float32)[None, :] * jax.nn.sigmoid(gate_logits.astype(jnp.float32))
    return gated_out.astype(jnp.bfloat16)

def block_ranks(expert_ids):
    grouped = expert_ids.reshape(N_SP, TOK_SP * TOP)
    onehot = (grouped[:, :, None] == jnp.arange(EXPERTS, dtype=jnp.int32)[None, None, :]).astype(jnp.int32)
    earlier = jnp.cumsum(onehot, axis=1) - onehot
    return lax.optimization_barrier(jnp.sum(earlier * onehot, axis=2)).reshape(TOKENS, TOP).astype(jnp.int32)

def cut_product(chosen, matrix):
    rows_cut = chosen.astype(jnp.float32).reshape(chosen.shape[0], CUTS, DBLK)
    matrix_cut = matrix.astype(jnp.float32).reshape(CUTS, DBLK, matrix.shape[1])
    partials = jnp.einsum('scd,cdf->csf', rows_cut, matrix_cut)
    rounded = lax.optimization_barrier(partials.astype(jnp.bfloat16))
    return lax.optimization_barrier(jnp.sum(rounded.astype(jnp.float32), axis=0))

def reference(receptance, key_vectors, value_vectors, decay_logits, rate_logits, gate_logits, group_gain, residual, mixer_out, norm_gain, expert_ids, route_weight, expert_gate, expert_up, expert_down):
    mixed_rows = time_mix(receptance, key_vectors, value_vectors, decay_logits, rate_logits, gate_logits, group_gain)
    midway = (residual.astype(jnp.float32) + jnp.dot(mixed_rows, mixer_out, preferred_element_type=jnp.float32)).astype(jnp.bfloat16)
    midway_f = midway.astype(jnp.float32)
    inv_rms = lax.rsqrt(lax.optimization_barrier(jnp.mean(midway_f * midway_f, axis=1, keepdims=True)) + EPS_NORM)
    normed = (midway_f * norm_gain.astype(jnp.float32)[None, :] * inv_rms).astype(jnp.bfloat16)
    ranks = block_ranks(expert_ids)
    token_ids = jnp.arange(TOKENS, dtype=jnp.int32)
    within = ((token_ids // TOK_SP)[:, None] * CAP + ranks).astype(jnp.int32)
    owners = jnp.broadcast_to(token_ids[:, None], expert_ids.shape).astype(jnp.int32)
    slot_table = jnp.full((EXPERTS, SLOTS), TOKENS, jnp.int32).at[expert_ids, within].set(owners)
    slot_weight = jnp.zeros((EXPERTS, SLOTS), jnp.float32).at[expert_ids, within].set(route_weight.astype(jnp.float32))
    padded = jnp.concatenate([normed, jnp.zeros((1, D), jnp.bfloat16)], axis=0)

    def one_expert(running, inputs):
        table_row, weight_row, gate_mat, up_mat, down_mat = inputs
        chosen = padded[table_row]
        hidden = (jax.nn.silu(cut_product(chosen, gate_mat)) * cut_product(chosen, up_mat)).astype(jnp.bfloat16)
        result = jnp.dot(hidden, down_mat, preferred_element_type=jnp.float32).astype(jnp.bfloat16)
        running = running.at[table_row].add(result.astype(jnp.float32) * weight_row[:, None])
        return (running, None)
    routed, unused = lax.scan(one_expert, jnp.zeros((TOKENS + 1, D), jnp.float32), (slot_table, slot_weight, expert_gate, expert_up, expert_down))
    return (midway_f + routed[:TOKENS]).astype(jnp.bfloat16)
```

```python
import jax
import jax.numpy as jnp
from jax import lax
from jax.experimental import pallas as pl
from jax.experimental.pallas import tpu as pltpu
from jax.sharding import PartitionSpec as P

D = 4096
HEAD = 64
CHUNK = 128
EXP_HALF = 0.6065306597126334


EPS_GROUP = 0.00064
EPS_NORM = 1e-06


def split(x):
    hi = x.astype(jnp.bfloat16)
    lo = (x - hi.astype(jnp.float32)).astype(jnp.bfloat16)
    return hi, lo


def dot(a, b, dims):
    return lax.dot_general(a, b, (dims, ((), ())), preferred_element_type=jnp.float32)


NN = ((1,), (0,))
NT = ((1,), (1,))
TN = ((0,), (0,))


def dot3(a, b, dims=NN):
    return dot(a[0], b[0], dims) + (dot(a[0], b[1], dims) + dot(a[1], b[0], dims))


def dot2(a, b, dims=NN):
    return dot(a[0], b, dims) + dot(a[1], b, dims)


def sigmoid(x):
    return 1.0 / (1.0 + jnp.exp(-x))


def mix_kernel(r_ref, k_ref, v_ref, d_ref, a_ref, out_ref, state_ref):
    tokens = r_ref.shape[0]
    chunks = tokens // CHUNK
    row = lax.broadcasted_iota(jnp.int32, (CHUNK, CHUNK), 0)
    col = lax.broadcasted_iota(jnp.int32, (CHUNK, CHUNK), 1)
    strict = col < row
    causal = col <= row
    eye = jnp.where(col == row, 1.0, 0.0)
    ones_lower = jnp.where(causal, 1.0, 0.0).astype(jnp.bfloat16)
    low = lax.broadcasted_iota(jnp.int32, (CHUNK, 2 * HEAD), 1) < HEAD

    work = []
    for chunk in range(chunks):
        rows = pl.ds(chunk * CHUNK, CHUNK)
        recept = r_ref[rows, :].astype(jnp.float32)
        keyvec = k_ref[rows, :].astype(jnp.float32)
        logdec = -EXP_HALF * sigmoid(d_ref[rows, :].astype(jnp.float32))
        first, second = split(logdec)
        third = (logdec - first.astype(jnp.float32) - second.astype(jnp.float32)).astype(jnp.bfloat16)
        cum_in = dot(ones_lower, first, NN) + (
            dot(ones_lower, second, NN) + dot(ones_lower, third, NN)
        )
        cum_end = cum_in[CHUNK - 1 :, :]
        squares = keyvec * keyvec
        norms = jnp.where(
            low,
            jnp.sum(squares[:, :HEAD], axis=1, keepdims=True),
            jnp.sum(squares[:, HEAD:], axis=1, keepdims=True),
        )
        unit_key = keyvec * lax.rsqrt(1.0 + norms)
        correction = unit_key * sigmoid(a_ref[rows, :].astype(jnp.float32))
        growth = jnp.exp(-cum_in)
        tail = jnp.exp(cum_end - cum_in)
        r_scaled = recept * jnp.exp(cum_in)
        u_scaled = unit_key * jnp.exp(cum_in - logdec)
        queries = split(jnp.concatenate([u_scaled, r_scaled], axis=0))
        sources = split(jnp.concatenate([keyvec * growth, correction * growth], axis=0))
        tails = split(jnp.concatenate([keyvec * tail, -(correction * tail)], axis=0))
        keep = jnp.broadcast_to(jnp.exp(cum_end), (2 * HEAD, 2 * HEAD)).T
        values = v_ref[rows, :]
        for head in range(2):
            lanes = slice(head * HEAD, (head + 1) * HEAD)
            query = tuple(q[:, lanes] for q in queries)
            source = tuple(s[:, lanes] for s in sources)
            scores = dot3(query, source, NT)
            work.append(
                dict(
                    head=head,
                    chunk=chunk,
                    query=query,
                    tail=tuple(t[:, lanes] for t in tails),
                    keep=keep[lanes, :],
                    value=jnp.concatenate(
                        [values[:, lanes], jnp.zeros((CHUNK, HEAD), jnp.bfloat16)], axis=1
                    ),
                    key_both=split(
                        jnp.concatenate(
                            [
                                jnp.where(strict, scores[:CHUNK, :CHUNK], 0.0),
                                jnp.where(causal, scores[CHUNK:, :CHUNK], 0.0),
                            ],
                            axis=0,
                        )
                    ),
                    pull=jnp.where(strict, scores[:CHUNK, CHUNK:], 0.0),
                    corr_read=split(jnp.where(causal, scores[CHUNK:, CHUNK:], 0.0)),
                )
            )
    for item in work:
        item["inverse"] = eye - jnp.where(row // 2 == col // 2, item["pull"], 0.0)
        item["from_values"] = dot2(item["key_both"], item["value"])
    size = 2
    while size < CHUNK:
        joined = (row // (2 * size) == col // (2 * size)) & (row // size != col // size)
        halves = []
        for item in work:
            inverse = split(item["inverse"])
            between = split(jnp.where(joined, item["pull"], 0.0))
            halves.append((inverse, dot3(between, inverse)))
        for item, (inverse, half) in zip(work, halves):
            item["inverse"] = item["inverse"] - dot3(inverse, split(half))
        size *= 2
    key_row = lax.broadcasted_iota(jnp.int32, (HEAD, 2 * HEAD), 0)
    lane = lax.broadcasted_iota(jnp.int32, (HEAD, 2 * HEAD), 1)
    start = jnp.where(lane == key_row + HEAD, 1.0, 0.0)
    states = [start, start]
    for item in work:
        head = item["head"]
        state = states[head]
        from_start = dot3(item["query"], split(state)) + item["from_values"]
        pulled = dot3(split(item["inverse"]), split(from_start[:CHUNK]))
        pulled_parts = split(pulled)
        out_ref[pl.ds(item["chunk"] * CHUNK, CHUNK), pl.ds(head * 2 * HEAD, 2 * HEAD)] = (
            from_start[CHUNK:] - dot3(item["corr_read"], pulled_parts)
        )
        key_tail = tuple(t[:CHUNK] for t in item["tail"])
        corr_tail = tuple(t[CHUNK:] for t in item["tail"])
        states[head] = (
            item["keep"] * state
            + dot2(key_tail, item["value"], TN)
            + dot3(corr_tail, pulled_parts, TN)
        )
    for head in range(2):
        state_ref[pl.ds(head * HEAD, HEAD), :] = states[head].astype(jnp.bfloat16)


def read_kernel(place_ref, read_ref, maps_ref, gate_ref, gain_ref, out_ref):
    def one(step, carried):
        following = []
        for head in range(2):
            both = maps_ref[step, pl.ds(head * HEAD, HEAD), :]
            parts = split(carried[head])
            step_map = both[:, HEAD:]
            following.append(
                both[:, :HEAD].astype(jnp.float32)
                + dot(step_map, parts[0], NN)
                + dot(step_map, parts[1], NN)
            )
        return tuple(following)

    zero = jnp.zeros((HEAD, HEAD), jnp.float32)
    incoming = lax.fori_loop(0, place_ref[0], one, (zero, zero))
    scaled = []
    for head in range(2):
        both = read_ref[:, pl.ds(head * 2 * HEAD, 2 * HEAD)]
        state_read = both[:, :HEAD] + dot3(split(both[:, HEAD:]), split(incoming[head]))
        centred = state_read - jnp.mean(state_read, axis=1, keepdims=True)
        variance = jnp.mean(centred * centred, axis=1, keepdims=True)
        scaled.append(centred * lax.rsqrt(variance + EPS_GROUP))
    gated = (
        jnp.concatenate(scaled, axis=1)
        * gain_ref[...]
        * sigmoid(gate_ref[...].astype(jnp.float32))
    )
    out_ref[...] = gated.astype(jnp.bfloat16)


def time_mix(
    receptance, key_vectors, value_vectors, decay_logits, rate_logits, gate_logits, group_gain
):
    tokens_here, channels = receptance.shape
    pairs = channels // (2 * HEAD)
    wide = pl.BlockSpec((tokens_here, 2 * HEAD), lambda i: (0, i))
    double = pl.BlockSpec((tokens_here, 4 * HEAD), lambda i: (0, i))
    reads, states = pl.pallas_call(
        mix_kernel,
        grid=(pairs,),
        in_specs=[wide] * 5,
        out_specs=[double, pl.BlockSpec((2 * HEAD, 2 * HEAD), lambda i: (i, 0))],
        out_shape=[
            jax.ShapeDtypeStruct((tokens_here, 2 * channels), jnp.float32),
            jax.ShapeDtypeStruct((channels, 2 * HEAD), jnp.bfloat16),
        ],
        name="mix",
    )(receptance, key_vectors, value_vectors, decay_logits, rate_logits)
    maps = lax.all_gather(states, "sp")
    place = lax.axis_index("sp").astype(jnp.int32).reshape(1)
    return pl.pallas_call(
        read_kernel,
        grid=(pairs,),
        in_specs=[
            pl.BlockSpec(memory_space=pltpu.SMEM),
            double,
            pl.BlockSpec((maps.shape[0], 2 * HEAD, 2 * HEAD), lambda i: (0, i, 0)),
            wide,
            pl.BlockSpec((1, 2 * HEAD), lambda i: (0, i)),
        ],
        out_specs=wide,
        out_shape=jax.ShapeDtypeStruct((tokens_here, channels), jnp.bfloat16),
        name="read",
    )(place, reads, maps, gate_logits, group_gain.reshape(1, channels))


def exchange(x, axis, shape, source, target, collective_id, name):
    def kernel(x_ref, out_ref, stage, send_sem, recv_sem, local_sem):
        n = lax.axis_size(axis)
        me = lax.axis_index(axis)
        peers = [lax.rem(me + step, n) for step in range(1, n)]
        barrier = pltpu.get_barrier_semaphore()
        for peer in peers:
            pl.semaphore_signal(
                barrier, inc=1, device_id={axis: peer}, device_id_type=pl.DeviceIdType.MESH
            )
        pl.semaphore_wait(barrier, n - 1)
        copies = []
        for step, peer in enumerate(peers):
            copy = pltpu.make_async_remote_copy(
                src_ref=source(x_ref, peer),
                dst_ref=target(out_ref, me),
                send_sem=send_sem.at[step],
                recv_sem=recv_sem.at[step],
                device_id={axis: peer},
                device_id_type=pl.DeviceIdType.MESH,
            )
            copy.start()
            copies.append(copy)
        own = pltpu.make_async_copy(source(x_ref, me), stage, local_sem)
        own.start()
        own.wait()
        own = pltpu.make_async_copy(stage, target(out_ref, me), local_sem)
        own.start()
        own.wait()
        for copy in copies:
            copy.wait()

    n = lax.axis_size(axis)
    return pl.pallas_call(
        kernel,
        in_specs=[pl.BlockSpec(memory_space=pl.ANY)],
        out_specs=pl.BlockSpec(memory_space=pl.ANY),
        out_shape=jax.ShapeDtypeStruct(shape, x.dtype),
        scratch_shapes=[
            pltpu.VMEM(x.shape[-2:], x.dtype),
            pltpu.SemaphoreType.DMA((n - 1,)),
            pltpu.SemaphoreType.DMA((n - 1,)),
            pltpu.SemaphoreType.DMA,
        ],
        compiler_params=pltpu.CompilerParams(collective_id=collective_id, has_side_effects=True),
        name=name,
    )(x)


def gather_columns(x, axis, collective_id):
    rows, columns = x.shape
    return exchange(
        x,
        axis,
        (rows, lax.axis_size(axis) * columns),
        lambda ref, peer: ref,
        lambda ref, me: ref.at[:, pl.ds(pl.multiple_of(me * columns, columns), columns)],
        collective_id,
        "gather_columns",
    )


def gather_rows(x, axis, collective_id):
    rows, columns = x.shape
    return exchange(
        x,
        axis,
        (lax.axis_size(axis) * rows, columns),
        lambda ref, peer: ref,
        lambda ref, me: ref.at[pl.ds(pl.multiple_of(me * rows, rows), rows), :],
        collective_id,
        "gather_rows",
    )


def swap_blocks(x, axis, collective_id):
    return exchange(
        x, axis, x.shape, lambda ref, peer: ref.at[peer], lambda ref, me: ref.at[me],
        collective_id, "swap_blocks",
    )


MESH = pl.DeviceIdType.MESH
GROUPS = 4


def expert_kernel(
    normed_ref,
    midway_ref,
    ids_ref,
    weight_ref,
    gate_hbm,
    up_hbm,
    down_hbm,
    out_ref,
    gate_w,
    up_w,
    down_w,
    select,
    outgoing,
    aux_out,
    aux_in,
    rows_in,
    part_a,
    part_b,
    first_a,
    first_b,
    pass_a,
    pass_b,
    second_a,
    second_b,
    hidden_a,
    hidden_b,
    own_res,
    pair_out,
    pair_in,
    back_out,
    back_in,
    load_sem,
    disp_send,
    disp_recv,
    aux_send,
    aux_recv,
    fwd_send,
    fwd_recv,
    tp_send,
    tp_recv,
    pair_send,
    pair_recv,
    back_send,
    back_recv,
):
    tokens = normed_ref.shape[0]
    slots = outgoing.shape[1]
    quarter = slots // 4
    half = slots // 2
    width = hidden_a.shape[2]
    peers = GROUPS
    blocks = 2 * peers
    sp = lax.axis_index("sp")
    tp = lax.axis_index("tp")
    z, core = sp // 2, sp % 2
    y, x = tp // 2, tp % 2
    x_peer = y * 2 + (1 - x)
    y_peer = (1 - y) * 2 + x

    def chip(turn):
        step = (2 * turn - turn // 2) % 4
        return 2 * ((z // 2 + step // 2) % 2) + (z % 2 + step % 2) % 2

    loads = [
        pltpu.make_async_copy(source.at[0], target, load_sem.at[i])
        for i, (source, target) in enumerate(((gate_hbm, gate_w), (up_hbm, up_w), (down_hbm, down_w)))
    ]
    for load in loads:
        load.start()

    partner = {"sp": z * 2 + (1 - core)}
    barrier = pltpu.get_barrier_semaphore()
    friends = [partner, {"tp": x_peer}, {"tp": y_peer}]
    friends += [{"sp": chip(turn) * 2 + core} for turn in range(1, peers)]
    for friend in friends:
        pl.semaphore_signal(barrier, inc=1, device_id=friend, device_id_type=MESH)

    def remote(source, target, send, recv, device):
        return pltpu.make_async_remote_copy(
            src_ref=source, dst_ref=target, send_sem=send, recv_sem=recv,
            device_id=device, device_id_type=MESH,
        )

    def dispatch(turn):
        return remote(
            outgoing.at[turn], rows_in.at[2 * turn], disp_send.at[turn], disp_recv.at[turn],
            {"sp": chip(turn) * 2 + core},
        )

    def dispatch_aux(turn):
        return remote(
            aux_out.at[turn], aux_in.at[turn], aux_send.at[turn], aux_recv.at[turn],
            {"sp": chip(turn) * 2 + core},
        )

    def forward(turn):
        return remote(
            rows_in.at[2 * turn], rows_in.at[2 * turn + 1], fwd_send.at[turn], fwd_recv.at[turn], partner
        )

    def over_tp(kind, k, source, target, device):
        return remote(source, target, tp_send.at[kind, k], tp_recv.at[kind, k], {"tp": device})

    def rows(start, size):
        return pl.ds(pl.multiple_of(start, quarter), size)

    def sum_first(k):
        return (
            over_tp(0, k, part_a.at[k, rows(half * (1 - x), half)], first_a.at[k], x_peer),
            over_tp(1, k, part_b.at[k, rows(half * (1 - y), half)], first_b.at[k], y_peer),
        )

    def sum_second(k):
        return (
            over_tp(2, k, pass_a.at[k], second_a.at[k], y_peer),
            over_tp(3, k, pass_b.at[k], second_b.at[k], x_peer),
        )

    def spread_first(k):
        own_a = hidden_a.at[k, rows(half * x + quarter * y, quarter)]
        own_b = hidden_b.at[k, rows(half * y + quarter * x, quarter)]
        return (over_tp(4, k, own_a, own_a, y_peer), over_tp(5, k, own_b, own_b, x_peer))

    def spread_second(k):
        own_a = hidden_a.at[k, rows(half * x, half)]
        own_b = hidden_b.at[k, rows(half * y, half)]
        return (over_tp(6, k, own_a, own_a, x_peer), over_tp(7, k, own_b, own_b, y_peer))

    def pair(turn):
        return remote(pair_out.at[turn], pair_in.at[turn], pair_send.at[turn], pair_recv.at[turn], partner)

    def give_back(turn):
        return remote(
            back_out.at[turn], back_in.at[turn], back_send.at[turn], back_recv.at[turn],
            {"sp": chip(turn) * 2 + core},
        )

    ids = ids_ref[...]
    weights = weight_ref[...]
    lane = lax.broadcasted_iota(jnp.int32, (tokens, 128), 1)
    slot_lane = lax.broadcasted_iota(jnp.int32, (tokens, slots), 1).astype(jnp.float32)
    earlier = jnp.where(
        lax.broadcasted_iota(jnp.int32, (tokens, tokens), 1)
        < lax.broadcasted_iota(jnp.int32, (tokens, tokens), 0),
        1.0,
        0.0,
    ).astype(jnp.bfloat16)
    group_of = [chip(turn) for turn in range(peers)]
    member = [
        jnp.logical_and(ids[:, :1] >= 2 * group, ids[:, :1] < 2 * group + 2) for group in group_of
    ]
    members = jnp.zeros((tokens, 128), jnp.float32)
    for turn in range(peers):
        members = jnp.where(jnp.logical_and(lane == turn, member[turn]), 1.0, members)
    ranks = dot(earlier, members.astype(jnp.bfloat16), NN)
    normed = normed_ref[...]
    pl.semaphore_wait(barrier, len(friends))
    for turn in range(peers):
        chosen = jnp.where(
            jnp.logical_and(slot_lane == ranks[:, turn : turn + 1], member[turn]), 1.0, 0.0
        ).astype(jnp.bfloat16)
        select[turn] = chosen
        picked = dot(chosen, normed, TN).astype(jnp.bfloat16)
        if turn == 0:
            rows_in[0] = picked
            forward(0).start()
        else:
            outgoing[turn] = picked
            dispatch(turn).start()
        parts = jnp.zeros((tokens, 128), jnp.float32)
        for expert in range(2):
            name = 2 * group_of[turn] + expert
            value = jnp.where(ids[:, :1] == name, weights[:, :1], 0.0) + jnp.where(
                ids[:, 1:2] == name, weights[:, 1:2], 0.0
            )
            for piece in range(3):
                term = value.astype(jnp.bfloat16).astype(jnp.float32)
                parts = jnp.where(lane == 3 * expert + piece, term, parts)
                value = value - term
        by_slot = dot(parts.astype(jnp.bfloat16), chosen, TN)
        weight_rows = jnp.concatenate(
            [
                by_slot[0:1] + by_slot[1:2] + by_slot[2:3],
                by_slot[3:4] + by_slot[4:5] + by_slot[5:6],
                jnp.zeros((6, slots), jnp.float32),
            ],
            axis=0,
        )
        if turn == 0:
            aux_in[0] = weight_rows
        else:
            aux_out[turn] = weight_rows
            dispatch_aux(turn).start()
    for load in loads:
        load.wait()

    def step(t, carry):
        @pl.when(t < blocks)
        def _():
            k = t
            turn = k // 2

            @pl.when(jnp.logical_and(k % 2 == 0, k > 0))
            def _():
                dispatch(turn).wait_recv()
                forward(turn).start()

            @pl.when(k % 2 == 1)
            def _():
                forward(turn).wait_recv()

            block = rows_in[k]
            for part, columns in ((part_a, pl.ds(0, width)), (part_b, pl.ds(width, width))):
                part[k, :, :width] = dot(block, gate_w[:, columns], NN).astype(jnp.bfloat16)
                part[k, :, width:] = dot(block, up_w[:, columns], NN).astype(jnp.bfloat16)
            for copy in sum_first(k):
                copy.start()

        @pl.when(jnp.logical_and(t >= 1, t < blocks + 1))
        def _():
            k = t - 1
            copies = sum_first(k)
            nexts = sum_second(k)
            copies[0].wait_recv()
            pass_a[k] = (
                part_a[k, rows(half * x + quarter * (1 - y), quarter)].astype(jnp.float32)
                + first_a[k, rows(quarter * (1 - y), quarter)].astype(jnp.float32)
            ).astype(jnp.bfloat16)
            nexts[0].start()
            copies[1].wait_recv()
            pass_b[k] = (
                part_b[k, rows(half * y + quarter * (1 - x), quarter)].astype(jnp.float32)
                + first_b[k, rows(quarter * (1 - x), quarter)].astype(jnp.float32)
            ).astype(jnp.bfloat16)
            nexts[1].start()

        @pl.when(jnp.logical_and(t >= 2, t < blocks + 2))
        def _():
            k = t - 2
            copies = sum_second(k)
            nexts = spread_first(k)
            for i, (part, first, second, hidden, major, minor) in enumerate(
                (
                    (part_a, first_a, second_a, hidden_a, x, y),
                    (part_b, first_b, second_b, hidden_b, y, x),
                )
            ):
                copies[i].wait_recv()
                mine = rows(half * major + quarter * minor, quarter)
                total = (
                    part[k, mine].astype(jnp.float32)
                    + first[k, rows(quarter * minor, quarter)].astype(jnp.float32)
                    + second[k].astype(jnp.float32)
                )
                gate, up = total[:, :width], total[:, width:]
                hidden[k, mine] = (gate * sigmoid(gate) * up).astype(jnp.bfloat16)
                nexts[i].start()

        @pl.when(jnp.logical_and(t >= 3, t < blocks + 3))
        def _():
            k = t - 3
            for copy, follow in zip(spread_first(k), spread_second(k)):
                copy.wait_recv()
                follow.start()

        @pl.when(jnp.logical_and(t >= 4, t < blocks + 4))
        def _():
            k = t - 4
            turn = k // 2
            for copy in spread_second(k):
                copy.wait_recv()
            result = dot(hidden_a[k], down_w[:width, :], NN) + dot(hidden_b[k], down_w[width:, :], NN)

            @pl.when(k % 2 == 0)
            def _():
                own_res[turn] = result

            @pl.when(k % 2 == 1)
            def _():
                pair_out[turn] = result.astype(jnp.bfloat16)
                pair(turn).start()

        @pl.when(jnp.logical_and(t >= 6, t % 2 == 0))
        def _():
            turn = (t - 6) // 2

            @pl.when(turn > 0)
            def _():
                dispatch_aux(turn).wait_recv()

            pair(turn).wait_recv()
            columns = jnp.concatenate([aux_in[turn]] * (128 // 8), axis=0).T
            low, high = columns[:, 0:1], columns[:, 1:2]
            mine = jnp.where(core == 0, low, high)
            other = jnp.where(core == 0, high, low)
            both = (own_res[turn] * mine + pair_in[turn].astype(jnp.float32) * other).astype(
                jnp.bfloat16
            )

            @pl.when(turn == 0)
            def _():
                back_in[0] = both

            @pl.when(turn > 0)
            def _():
                back_out[turn] = both
                give_back(turn).start()

        return carry

    lax.fori_loop(0, blocks + 5, step, 0)
    total = midway_ref[...].astype(jnp.float32)
    for turn in range(peers):
        if turn > 0:
            give_back(turn).wait_recv()
        total = total + dot(select[turn], back_in[turn], NN)
    out_ref[...] = total.astype(jnp.bfloat16)

    for turn in range(peers):
        forward(turn).wait_send()
        pair(turn).wait_send()
        if turn > 0:
            dispatch(turn).wait_send()
            dispatch_aux(turn).wait_send()
            give_back(turn).wait_send()

    def drain(k, carry):
        for copies in (sum_first(k), sum_second(k), spread_first(k), spread_second(k)):
            for copy in copies:
                copy.wait_send()
        return carry

    lax.fori_loop(0, blocks, drain, 0)


def routed_experts(normed, midway, expert_ids, route_weight, expert_gate, expert_up, expert_down):
    tokens, features = normed.shape
    hidden = expert_gate.shape[2]
    half = hidden // 2
    slots = tokens // 2
    quarter = slots // 4
    peers = GROUPS
    blocks = 2 * peers
    bf = jnp.bfloat16
    whole = pl.BlockSpec(memory_space=pltpu.VMEM)
    far = pl.BlockSpec(memory_space=pl.ANY)
    dma = pltpu.SemaphoreType.DMA
    return pl.pallas_call(
        expert_kernel,
        in_specs=[whole] * 4 + [far] * 3,
        out_specs=whole,
        out_shape=jax.ShapeDtypeStruct((tokens, features), bf),
        scratch_shapes=[
            pltpu.VMEM((features, hidden), bf),
            pltpu.VMEM((features, hidden), bf),
            pltpu.VMEM((hidden, features), bf),
            pltpu.VMEM((peers, tokens, slots), bf),
            pltpu.VMEM((peers, slots, features), bf),
            pltpu.VMEM((peers, 8, slots), jnp.float32),
            pltpu.VMEM((peers, 8, slots), jnp.float32),
            pltpu.VMEM((blocks, slots, features), bf),
            pltpu.VMEM((blocks, slots, hidden), bf),
            pltpu.VMEM((blocks, slots, hidden), bf),
            pltpu.VMEM((blocks, slots // 2, hidden), bf),
            pltpu.VMEM((blocks, slots // 2, hidden), bf),
            pltpu.VMEM((blocks, quarter, hidden), bf),
            pltpu.VMEM((blocks, quarter, hidden), bf),
            pltpu.VMEM((blocks, quarter, hidden), bf),
            pltpu.VMEM((blocks, quarter, hidden), bf),
            pltpu.VMEM((blocks, slots, half), bf),
            pltpu.VMEM((blocks, slots, half), bf),
            pltpu.VMEM((peers, slots, features), jnp.float32),
            pltpu.VMEM((peers, slots, features), bf),
            pltpu.VMEM((peers, slots, features), bf),
            pltpu.VMEM((peers, slots, features), bf),
            pltpu.VMEM((peers, slots, features), bf),
            dma((3,)),
            dma((peers,)),
            dma((peers,)),
            dma((peers,)),
            dma((peers,)),
            dma((peers,)),
            dma((peers,)),
            dma((8, blocks)),
            dma((8, blocks)),
            dma((peers,)),
            dma((peers,)),
            dma((peers,)),
            dma((peers,)),
        ],
        compiler_params=pltpu.CompilerParams(
            collective_id=4, has_side_effects=True, vmem_limit_bytes=52 * 1024 * 1024
        ),
        name="experts",
    )(normed, midway, expert_ids, route_weight, expert_gate, expert_up, expert_down)


def local(
    receptance,
    key_vectors,
    value_vectors,
    decay_logits,
    rate_logits,
    gate_logits,
    group_gain,
    residual,
    mixer_out,
    norm_gain,
    expert_ids,
    route_weight,
    expert_gate,
    expert_up,
    expert_down,
):
    mixed_rows = time_mix(
        receptance, key_vectors, value_vectors, decay_logits, rate_logits, gate_logits, group_gain
    )
    tokens_here, features = residual.shape
    projected = jnp.dot(
        gather_columns(mixed_rows, "tp", 0),
        mixer_out,
        preferred_element_type=jnp.float32,
    )
    midway = (residual.astype(jnp.float32) + projected).astype(jnp.bfloat16)
    midway_f = midway.astype(jnp.float32)
    squares = lax.psum(jnp.sum(midway_f * midway_f, axis=1), "tp")
    inv_rms = lax.rsqrt(squares / D + EPS_NORM)
    normed = (midway_f * norm_gain[None, :] * inv_rms[:, None]).astype(jnp.bfloat16)
    routes = expert_ids.shape[1]
    paired_cores = lax.axis_size("sp") == 2 * GROUPS and lax.axis_size("tp") == 4
    if paired_cores and expert_gate.shape[0] == 1:
        return routed_experts(
            normed, midway, expert_ids, route_weight, expert_gate, expert_up, expert_down
        )
    experts_all = lax.axis_size("sp") * expert_gate.shape[0]
    capacity = 2 * tokens_here * routes // experts_all
    flat_ids = expert_ids.reshape(-1)
    onehot = (flat_ids[:, None] == jnp.arange(experts_all, dtype=jnp.int32)[None, :]).astype(
        jnp.int32
    )
    earlier_count = jnp.sum((jnp.cumsum(onehot, axis=0) - onehot) * onehot, axis=1)
    slot_of = flat_ids * capacity + earlier_count
    owner_token = jnp.arange(tokens_here * routes, dtype=jnp.int32) // routes
    slot_table = (
        jnp.full((experts_all * capacity,), tokens_here, jnp.int32).at[slot_of].set(owner_token)
    )
    padded = jnp.concatenate([normed, jnp.zeros((1, features), jnp.bfloat16)], axis=0)
    outgoing = padded[slot_table].reshape(experts_all, capacity, features)
    arrived = swap_blocks(outgoing, "sp", 2)
    arrived_rows = arrived.reshape(-1, features)
    paired = jnp.concatenate([expert_gate[0], expert_up[0]], axis=1)
    gate_up = lax.psum_scatter(
        jnp.dot(arrived_rows, paired, preferred_element_type=jnp.float32).astype(jnp.bfloat16),
        "tp",
        scatter_dimension=0,
        tiled=True,
    ).astype(jnp.float32)
    half_width = paired.shape[1] // 2
    hidden = (jax.nn.silu(gate_up[:, :half_width]) * gate_up[:, half_width:]).astype(jnp.bfloat16)
    expert_res = jnp.dot(
        gather_rows(hidden, "tp", 1),
        expert_down[0],
        preferred_element_type=jnp.float32,
    )
    returned = swap_blocks(
        expert_res.astype(jnp.bfloat16).reshape(-1, capacity, features), "sp", 3
    )
    picked = (
        returned.reshape(-1, features)[slot_of]
        .astype(jnp.float32)
        .reshape(tokens_here, routes, features)
    )
    routed_sum = jnp.sum(picked * route_weight[:, :, None], axis=1)
    return (midway_f + routed_sum).astype(jnp.bfloat16)


def solution(mesh):
    placed = (
        P("sp", "tp"),
        P("sp", "tp"),
        P("sp", "tp"),
        P("sp", "tp"),
        P("sp", "tp"),
        P("sp", "tp"),
        P("tp"),
        P("sp", "tp"),
        P(None, "tp"),
        P("tp"),
        P("sp", None),
        P("sp", None),
        P("sp", "tp", None),
        P("sp", "tp", None),
        P("sp", None, "tp"),
    )
    return jax.shard_map(
        local, mesh=mesh, in_specs=placed, out_specs=P("sp", "tp"), check_vma=False
    )
```

```python
import jax
import jax.numpy as jnp
from jax import lax
from jax.experimental import pallas as pl
from jax.experimental.pallas import tpu as pltpu
from jax.sharding import PartitionSpec as P

D = 4096
HEAD = 64
CHUNK = 128
EXP_HALF = 0.6065306597126334


EPS_GROUP = 0.00064
EPS_NORM = 1e-06


def split(x):
    hi = x.astype(jnp.bfloat16)
    lo = (x - hi.astype(jnp.float32)).astype(jnp.bfloat16)
    return hi, lo


def dot(a, b, dims):
    return lax.dot_general(a, b, (dims, ((), ())), preferred_element_type=jnp.float32)


NN = ((1,), (0,))
NT = ((1,), (1,))
TN = ((0,), (0,))


def dot3(a, b, dims=NN):
    return dot(a[0], b[0], dims) + (dot(a[0], b[1], dims) + dot(a[1], b[0], dims))


def dot2(a, b, dims=NN):
    return dot(a[0], b, dims) + dot(a[1], b, dims)


def sigmoid(x):
    return 1.0 / (1.0 + jnp.exp(-x))


def mix_kernel(r_ref, k_ref, v_ref, d_ref, a_ref, out_ref, state_ref):
    tokens = r_ref.shape[0]
    chunks = tokens // CHUNK
    row = lax.broadcasted_iota(jnp.int32, (CHUNK, CHUNK), 0)
    col = lax.broadcasted_iota(jnp.int32, (CHUNK, CHUNK), 1)
    strict = col < row
    causal = col <= row
    eye = jnp.where(col == row, 1.0, 0.0)
    ones_lower = jnp.where(causal, 1.0, 0.0).astype(jnp.bfloat16)
    low = lax.broadcasted_iota(jnp.int32, (CHUNK, 2 * HEAD), 1) < HEAD

    work = []
    for chunk in range(chunks):
        rows = pl.ds(chunk * CHUNK, CHUNK)
        recept = r_ref[rows, :].astype(jnp.float32)
        keyvec = k_ref[rows, :].astype(jnp.float32)
        logdec = -EXP_HALF * sigmoid(d_ref[rows, :].astype(jnp.float32))
        first, second = split(logdec)
        third = (logdec - first.astype(jnp.float32) - second.astype(jnp.float32)).astype(jnp.bfloat16)
        cum_in = dot(ones_lower, first, NN) + (
            dot(ones_lower, second, NN) + dot(ones_lower, third, NN)
        )
        cum_end = cum_in[CHUNK - 1 :, :]
        squares = keyvec * keyvec
        norms = jnp.where(
            low,
            jnp.sum(squares[:, :HEAD], axis=1, keepdims=True),
            jnp.sum(squares[:, HEAD:], axis=1, keepdims=True),
        )
        unit_key = keyvec * lax.rsqrt(1.0 + norms)
        correction = unit_key * sigmoid(a_ref[rows, :].astype(jnp.float32))
        growth = jnp.exp(-cum_in)
        tail = jnp.exp(cum_end - cum_in)
        r_scaled = recept * jnp.exp(cum_in)
        u_scaled = unit_key * jnp.exp(cum_in - logdec)
        queries = split(jnp.concatenate([u_scaled, r_scaled], axis=0))
        sources = split(jnp.concatenate([keyvec * growth, correction * growth], axis=0))
        tails = split(jnp.concatenate([keyvec * tail, -(correction * tail)], axis=0))
        keep = jnp.broadcast_to(jnp.exp(cum_end), (2 * HEAD, 2 * HEAD)).T
        values = v_ref[rows, :]
        for head in range(2):
            lanes = slice(head * HEAD, (head + 1) * HEAD)
            query = tuple(q[:, lanes] for q in queries)
            source = tuple(s[:, lanes] for s in sources)
            scores = dot3(query, source, NT)
            work.append(
                dict(
                    head=head,
                    chunk=chunk,
                    query=query,
                    tail=tuple(t[:, lanes] for t in tails),
                    keep=keep[lanes, :],
                    value=jnp.concatenate(
                        [values[:, lanes], jnp.zeros((CHUNK, HEAD), jnp.bfloat16)], axis=1
                    ),
                    key_both=split(
                        jnp.concatenate(
                            [
                                jnp.where(strict, scores[:CHUNK, :CHUNK], 0.0),
                                jnp.where(causal, scores[CHUNK:, :CHUNK], 0.0),
                            ],
                            axis=0,
                        )
                    ),
                    pull=jnp.where(strict, scores[:CHUNK, CHUNK:], 0.0),
                    corr_read=split(jnp.where(causal, scores[CHUNK:, CHUNK:], 0.0)),
                )
            )
    for item in work:
        item["inverse"] = eye - jnp.where(row // 2 == col // 2, item["pull"], 0.0)
        item["from_values"] = dot2(item["key_both"], item["value"])
    size = 2
    while size < CHUNK:
        joined = (row // (2 * size) == col // (2 * size)) & (row // size != col // size)
        halves = []
        for item in work:
            inverse = split(item["inverse"])
            between = split(jnp.where(joined, item["pull"], 0.0))
            halves.append((inverse, dot3(between, inverse)))
        for item, (inverse, half) in zip(work, halves):
            item["inverse"] = item["inverse"] - dot3(inverse, split(half))
        size *= 2
    key_row = lax.broadcasted_iota(jnp.int32, (HEAD, 2 * HEAD), 0)
    lane = lax.broadcasted_iota(jnp.int32, (HEAD, 2 * HEAD), 1)
    start = jnp.where(lane == key_row + HEAD, 1.0, 0.0)
    states = [start, start]
    for item in work:
        head = item["head"]
        state = states[head]
        from_start = dot3(item["query"], split(state)) + item["from_values"]
        pulled = dot3(split(item["inverse"]), split(from_start[:CHUNK]))
        pulled_parts = split(pulled)
        out_ref[pl.ds(item["chunk"] * CHUNK, CHUNK), pl.ds(head * 2 * HEAD, 2 * HEAD)] = (
            from_start[CHUNK:] - dot3(item["corr_read"], pulled_parts)
        )
        key_tail = tuple(t[:CHUNK] for t in item["tail"])
        corr_tail = tuple(t[CHUNK:] for t in item["tail"])
        states[head] = (
            item["keep"] * state
            + dot2(key_tail, item["value"], TN)
            + dot3(corr_tail, pulled_parts, TN)
        )
    for head in range(2):
        state_ref[pl.ds(head * HEAD, HEAD), :] = states[head].astype(jnp.bfloat16)


def read_kernel(place_ref, read_ref, maps_ref, gate_ref, gain_ref, out_ref):
    def one(step, carried):
        following = []
        for head in range(2):
            both = maps_ref[step, pl.ds(head * HEAD, HEAD), :]
            parts = split(carried[head])
            step_map = both[:, HEAD:]
            following.append(
                both[:, :HEAD].astype(jnp.float32)
                + dot(step_map, parts[0], NN)
                + dot(step_map, parts[1], NN)
            )
        return tuple(following)

    zero = jnp.zeros((HEAD, HEAD), jnp.float32)
    incoming = lax.fori_loop(0, place_ref[0], one, (zero, zero))
    scaled = []
    for head in range(2):
        both = read_ref[:, pl.ds(head * 2 * HEAD, 2 * HEAD)]
        state_read = both[:, :HEAD] + dot3(split(both[:, HEAD:]), split(incoming[head]))
        centred = state_read - jnp.mean(state_read, axis=1, keepdims=True)
        variance = jnp.mean(centred * centred, axis=1, keepdims=True)
        scaled.append(centred * lax.rsqrt(variance + EPS_GROUP))
    gated = (
        jnp.concatenate(scaled, axis=1)
        * gain_ref[...]
        * sigmoid(gate_ref[...].astype(jnp.float32))
    )
    out_ref[...] = gated.astype(jnp.bfloat16)


def time_mix(
    receptance, key_vectors, value_vectors, decay_logits, rate_logits, gate_logits, group_gain
):
    tokens_here, channels = receptance.shape
    pairs = channels // (2 * HEAD)
    wide = pl.BlockSpec((tokens_here, 2 * HEAD), lambda i: (0, i))
    double = pl.BlockSpec((tokens_here, 4 * HEAD), lambda i: (0, i))
    reads, states = pl.pallas_call(
        mix_kernel,
        grid=(pairs,),
        in_specs=[wide] * 5,
        out_specs=[double, pl.BlockSpec((2 * HEAD, 2 * HEAD), lambda i: (i, 0))],
        out_shape=[
            jax.ShapeDtypeStruct((tokens_here, 2 * channels), jnp.float32),
            jax.ShapeDtypeStruct((channels, 2 * HEAD), jnp.bfloat16),
        ],
        name="mix",
    )(receptance, key_vectors, value_vectors, decay_logits, rate_logits)
    maps = lax.all_gather(states, "sp")
    place = lax.axis_index("sp").astype(jnp.int32).reshape(1)
    return pl.pallas_call(
        read_kernel,
        grid=(pairs,),
        in_specs=[
            pl.BlockSpec(memory_space=pltpu.SMEM),
            double,
            pl.BlockSpec((maps.shape[0], 2 * HEAD, 2 * HEAD), lambda i: (0, i, 0)),
            wide,
            pl.BlockSpec((1, 2 * HEAD), lambda i: (0, i)),
        ],
        out_specs=wide,
        out_shape=jax.ShapeDtypeStruct((tokens_here, channels), jnp.bfloat16),
        name="read",
    )(place, reads, maps, gate_logits, group_gain.reshape(1, channels))


def exchange(x, axis, shape, source, target, collective_id, name):
    def kernel(x_ref, out_ref, stage, send_sem, recv_sem, local_sem):
        n = lax.axis_size(axis)
        me = lax.axis_index(axis)
        peers = [lax.rem(me + step, n) for step in range(1, n)]
        barrier = pltpu.get_barrier_semaphore()
        for peer in peers:
            pl.semaphore_signal(
                barrier, inc=1, device_id={axis: peer}, device_id_type=pl.DeviceIdType.MESH
            )
        pl.semaphore_wait(barrier, n - 1)
        copies = []
        for step, peer in enumerate(peers):
            copy = pltpu.make_async_remote_copy(
                src_ref=source(x_ref, peer),
                dst_ref=target(out_ref, me),
                send_sem=send_sem.at[step],
                recv_sem=recv_sem.at[step],
                device_id={axis: peer},
                device_id_type=pl.DeviceIdType.MESH,
            )
            copy.start()
            copies.append(copy)
        own = pltpu.make_async_copy(source(x_ref, me), stage, local_sem)
        own.start()
        own.wait()
        own = pltpu.make_async_copy(stage, target(out_ref, me), local_sem)
        own.start()
        own.wait()
        for copy in copies:
            copy.wait()

    n = lax.axis_size(axis)
    return pl.pallas_call(
        kernel,
        in_specs=[pl.BlockSpec(memory_space=pl.ANY)],
        out_specs=pl.BlockSpec(memory_space=pl.ANY),
        out_shape=jax.ShapeDtypeStruct(shape, x.dtype),
        scratch_shapes=[
            pltpu.VMEM(x.shape[-2:], x.dtype),
            pltpu.SemaphoreType.DMA((n - 1,)),
            pltpu.SemaphoreType.DMA((n - 1,)),
            pltpu.SemaphoreType.DMA,
        ],
        compiler_params=pltpu.CompilerParams(collective_id=collective_id, has_side_effects=True),
        name=name,
    )(x)


def gather_columns(x, axis, collective_id):
    rows, columns = x.shape
    return exchange(
        x,
        axis,
        (rows, lax.axis_size(axis) * columns),
        lambda ref, peer: ref,
        lambda ref, me: ref.at[:, pl.ds(pl.multiple_of(me * columns, columns), columns)],
        collective_id,
        "gather_columns",
    )


def gather_rows(x, axis, collective_id):
    rows, columns = x.shape
    return exchange(
        x,
        axis,
        (lax.axis_size(axis) * rows, columns),
        lambda ref, peer: ref,
        lambda ref, me: ref.at[pl.ds(pl.multiple_of(me * rows, rows), rows), :],
        collective_id,
        "gather_rows",
    )


def swap_blocks(x, axis, collective_id):
    return exchange(
        x, axis, x.shape, lambda ref, peer: ref.at[peer], lambda ref, me: ref.at[me],
        collective_id, "swap_blocks",
    )


MESH = pl.DeviceIdType.MESH
GROUPS = 4


def pack_left(a):
    hi, lo = split(a)
    return jnp.concatenate([hi, lo], axis=1)


def pack_right(b):
    both = jnp.concatenate(split(b), axis=1)
    return jnp.concatenate([both, both], axis=0)


def dot_packed(left, right):
    out = dot(left, right, NN)
    n = out.shape[1] // 2
    return out[:, :n] + out[:, n:]


def three(a, axis, second):
    hi, lo = split(a)
    return jnp.concatenate([hi, hi, lo] if second else [hi, lo, hi], axis=axis)


def mix_heads(recept_in, key_in, values_in, decay_in, rate_in, write_read, write_state):
    tokens, width = recept_in.shape
    chunks = tokens // CHUNK
    pairs = width // (2 * HEAD)
    row = lax.broadcasted_iota(jnp.int32, (CHUNK, CHUNK), 0)
    col = lax.broadcasted_iota(jnp.int32, (CHUNK, CHUNK), 1)
    strict = col < row
    causal = col <= row
    eye = jnp.where(col == row, 1.0, 0.0)
    ones_lower = jnp.where(causal, 1.0, 0.0).astype(jnp.bfloat16)
    ones_twice = jnp.concatenate([ones_lower, ones_lower], axis=1)
    low = lax.broadcasted_iota(jnp.int32, (CHUNK, 2 * HEAD), 1) < HEAD
    nothing = jnp.zeros((CHUNK, 2 * HEAD), jnp.bfloat16)

    work = []
    for chunk in range(chunks):
        rows = slice(chunk * CHUNK, (chunk + 1) * CHUNK)
        for pair in range(pairs):
            lanes = slice(pair * 2 * HEAD, (pair + 1) * 2 * HEAD)
            recept = recept_in[rows, lanes].astype(jnp.float32)
            keyvec = key_in[rows, lanes].astype(jnp.float32)
            values = values_in[rows, lanes]
            logdec = -EXP_HALF * sigmoid(decay_in[rows, lanes].astype(jnp.float32))
            first, second = split(logdec)
            third = (logdec - first.astype(jnp.float32) - second.astype(jnp.float32)).astype(
                jnp.bfloat16
            )
            cum_in = dot_packed(
                ones_twice,
                jnp.concatenate(
                    [
                        jnp.concatenate([first, third], axis=1),
                        jnp.concatenate([second, nothing], axis=1),
                    ],
                    axis=0,
                ),
            )
            cum_end = cum_in[CHUNK - 1 :, :]
            squares = keyvec * keyvec
            norms = jnp.where(
                low,
                jnp.sum(squares[:, :HEAD], axis=1, keepdims=True),
                jnp.sum(squares[:, HEAD:], axis=1, keepdims=True),
            )
            unit_key = keyvec * lax.rsqrt(1.0 + norms)
            correction = unit_key * sigmoid(rate_in[rows, lanes].astype(jnp.float32))
            growth = jnp.exp(-cum_in)
            tail = jnp.exp(cum_end - cum_in)
            r_scaled = recept * jnp.exp(cum_in)
            u_scaled = unit_key * jnp.exp(cum_in - logdec)
            queries = jnp.concatenate([u_scaled, r_scaled], axis=0)
            sources = jnp.concatenate([keyvec * growth, correction * growth], axis=0)
            tails = jnp.concatenate([(keyvec * tail).T, -(correction * tail).T], axis=1)
            tail_hi, tail_lo = split(tails)
            keep = jnp.broadcast_to(jnp.exp(cum_end), (2 * HEAD, 2 * HEAD)).T
            for head in range(2):
                part = slice(head * HEAD, (head + 1) * HEAD)
                query = three(queries[:, part], 1, False)
                scores = dot(query, three(sources[:, part], 1, True), NT)
                value = jnp.concatenate(
                    [values[:, part], jnp.zeros((CHUNK, HEAD), jnp.bfloat16)], axis=1
                )
                work.append(
                    dict(
                        head=2 * pair + head,
                        chunk=chunk,
                        query=query,
                        tail=jnp.concatenate([tail_hi[part, :], tail_lo[part, :]], axis=0),
                        keep=keep[part, :],
                        value=value,
                        key_both=pack_left(
                            jnp.concatenate(
                                [
                                    jnp.where(strict, scores[:CHUNK, :CHUNK], 0.0),
                                    jnp.where(causal, scores[CHUNK:, :CHUNK], 0.0),
                                ],
                                axis=0,
                            )
                        ),
                        pull=jnp.where(strict, scores[:CHUNK, CHUNK:], 0.0),
                        corr_read=pack_left(jnp.where(causal, scores[CHUNK:, CHUNK:], 0.0)),
                    )
                )
    for item in work:
        item["inverse"] = eye - jnp.where(row // 2 == col // 2, item["pull"], 0.0)
        value = item["value"]
        item["from_values"] = dot(
            item["key_both"], jnp.concatenate([value, value], axis=0), NN
        )
    size = 2
    while size < CHUNK:
        joined = (row // (2 * size) == col // (2 * size)) & (row // size != col // size)
        halves = []
        for item in work:
            between = pack_left(jnp.where(joined, item["pull"], 0.0))
            halves.append(dot_packed(between, pack_right(item["inverse"])))
        for item, half in zip(work, halves):
            item["inverse"] = item["inverse"] - dot_packed(
                pack_left(item["inverse"]), pack_right(half)
            )
        size *= 2
    key_row = lax.broadcasted_iota(jnp.int32, (HEAD, 2 * HEAD), 0)
    lane = lax.broadcasted_iota(jnp.int32, (HEAD, 2 * HEAD), 1)
    start = jnp.where(lane == key_row + HEAD, 1.0, 0.0)
    states = [start] * (2 * pairs)
    for chunk in range(chunks):
        items = [item for item in work if item["chunk"] == chunk]
        froms = [
            dot(item["query"], three(states[item["head"]], 0, True), NN) + item["from_values"]
            for item in items
        ]
        pulls = [
            dot_packed(pack_left(item["inverse"]), pack_right(value[:CHUNK]))
            for item, value in zip(items, froms)
        ]
        for item, value, pulled in zip(items, froms, pulls):
            head = item["head"]
            write_read(
                chunk, head, value[CHUNK:] - dot_packed(item["corr_read"], pack_right(pulled))
            )
            hi, lo = split(pulled)
            right = jnp.concatenate(
                [
                    jnp.concatenate([item["value"], hi], axis=0),
                    jnp.concatenate([nothing, lo], axis=0),
                ],
                axis=1,
            )
            out = dot(item["tail"], right, NN)
            states[head] = (
                item["keep"] * states[head]
                + (out[:HEAD, : 2 * HEAD] + out[HEAD:, : 2 * HEAD])
                + out[:HEAD, 2 * HEAD :]
            )
    for head in range(2 * pairs):
        write_state(head, states[head].astype(jnp.bfloat16))


def mixer_kernel(
    r_ref,
    k_ref,
    v_ref,
    d_ref,
    a_ref,
    gate_ref,
    gain_ref,
    residual_ref,
    norm_ref,
    mixer_hbm,
    normed_ref,
    midway_ref,
    mixer_w,
    reads,
    maps_own,
    maps_in,
    joint,
    carry_out,
    carry_in,
    gathered,
    acc,
    sums,
    load_sem,
    swap_send,
    swap_recv,
    chain_send,
    chain_recv,
    gather_send,
    gather_recv,
    sum_send,
    sum_recv,
):
    tokens, features = residual_ref.shape
    steps, _, wide = reads.shape
    width = wide // 2
    heads = width // HEAD
    tps = lax.axis_size("tp")
    chips = lax.axis_size("sp") // 2
    sp = lax.axis_index("sp")
    tp = lax.axis_index("tp")
    z, core = sp // 2, sp % 2
    partner = {"sp": z * 2 + (1 - core)}
    peers = [{"tp": (tp + shift) % tps} for shift in range(1, tps)]

    def load(step, block):
        return pltpu.make_async_copy(
            mixer_hbm.at[pl.ds(pl.multiple_of(block * steps * width + step * width, width), width), :],
            mixer_w.at[step, pl.ds(block * width, width), :],
            load_sem.at[step, block],
        )

    def load_all(step, carry):
        for block in range(tps):
            load(step, block).start()
        return carry

    lax.fori_loop(0, steps, load_all, 0)

    barrier = pltpu.get_barrier_semaphore()
    friends = [partner] + peers
    friends += [{"sp": ((z + shift) % chips) * 2 + core} for shift in (1, chips - 1)]
    for friend in friends:
        pl.semaphore_signal(barrier, inc=1, device_id=friend, device_id_type=MESH)
    acc[...] = residual_ref[...].astype(jnp.float32)
    pl.semaphore_wait(barrier, len(friends))

    def remote(source, target, send, recv, device):
        return pltpu.make_async_remote_copy(
            src_ref=source, dst_ref=target, send_sem=send, recv_sem=recv,
            device_id=device, device_id_type=MESH,
        )

    def swap(j):
        return remote(maps_own.at[j], maps_in.at[j], swap_send.at[j], swap_recv.at[j], partner)

    def chain(j):
        return remote(
            carry_out.at[j], carry_in.at[j], chain_send.at[j], chain_recv.at[j],
            {"sp": ((z + 1) % chips) * 2 + core},
        )

    def columns():
        return pl.ds(pl.multiple_of(tp * width, width), width)

    def gather(j):
        own = gathered.at[j, :, columns()]
        return [
            remote(own, own, gather_send.at[i, j], gather_recv.at[i, j], peer)
            for i, peer in enumerate(peers)
        ]

    def mix(i):
        lanes = pl.ds(pl.multiple_of(i * width, width), width)

        def write_read(chunk, head, value):
            reads[i, pl.ds(chunk * CHUNK, CHUNK), pl.ds(head * 2 * HEAD, 2 * HEAD)] = value

        def write_state(head, value):
            maps_own[i, pl.ds(head * HEAD, HEAD), :] = value

        mix_heads(
            r_ref[:, lanes], k_ref[:, lanes], v_ref[:, lanes], d_ref[:, lanes], a_ref[:, lanes],
            write_read, write_state,
        )
        swap(i).start()

    half_lane = lax.broadcasted_iota(jnp.int32, (HEAD, 2 * HEAD), 1) < HEAD

    def join(j):
        swap(j).wait_recv()
        for head in range(heads):
            part = pl.ds(head * HEAD, HEAD)
            own, other = maps_own[j, part, :], maps_in[j, part, :]
            first = jnp.where(core == 0, own, other)
            second = jnp.where(core == 0, other, own)
            both = dot(second[:, HEAD:], first, NN)
            joint[j, part, :] = both + jnp.where(half_lane, second.astype(jnp.float32), 0.0)

    def follow(j):
        @pl.when(z > 0)
        def _():
            chain(j).wait_recv()

        @pl.when(z == 0)
        def _():
            carry_in[j] = jnp.zeros((HEAD, width), jnp.float32)

        carried = [carry_in[j, :, pl.ds(head * HEAD, HEAD)] for head in range(heads)]
        carried_parts = [split(value) for value in carried]
        following = []
        for head in range(heads):
            both = joint[j, pl.ds(head * HEAD, HEAD), :]
            following.append(both[:, :HEAD] + dot3(split(both[:, HEAD:]), carried_parts[head]))
        carry_out[j] = jnp.concatenate(following, axis=1)

        @pl.when(z < chips - 1)
        def _():
            chain(j).start()

        mine = []
        for head in range(heads):
            other = maps_in[j, pl.ds(head * HEAD, HEAD), :]
            passed = other[:, :HEAD].astype(jnp.float32) + (
                dot(other[:, HEAD:], carried_parts[head][0], NN)
                + dot(other[:, HEAD:], carried_parts[head][1], NN)
            )
            mine.append(jnp.where(core == 0, carried[head], passed))
        lanes = pl.ds(pl.multiple_of(j * width, width), width)
        blank = jnp.zeros((HEAD, 2 * HEAD), jnp.bfloat16)
        scaled = []
        for head in range(heads):
            both = reads[j, :, pl.ds(head * 2 * HEAD, 2 * HEAD)]
            state = jnp.concatenate([blank, jnp.concatenate(split(mine[head]), axis=1)], axis=0)
            out = dot(pack_left(both), jnp.concatenate([state, state], axis=0), NN)
            state_read = both[:, :HEAD] + (out[:, :HEAD] + out[:, HEAD:])
            centred = state_read - jnp.mean(state_read, axis=1, keepdims=True)
            variance = jnp.mean(centred * centred, axis=1, keepdims=True)
            scaled.append(centred * lax.rsqrt(variance + EPS_GROUP))
        gated = (
            jnp.concatenate(scaled, axis=1)
            * gain_ref[:, lanes]
            * sigmoid(gate_ref[:, lanes].astype(jnp.float32))
        )
        gathered[j, :, columns()] = gated.astype(jnp.bfloat16)
        for copy in gather(j):
            copy.start()

    def project(j):
        for block in range(tps):
            load(j, block).wait()
        for copy in gather(j):
            copy.wait_recv()
        acc[...] += dot(gathered[j], mixer_w[j], NN)

    def within(j):
        return jnp.logical_and(j >= 0, j < steps)

    def step(t, carry):
        @pl.when(within(t - 2 - z))
        def _():
            follow(t - 2 - z)

        @pl.when(within(t - 4 - z))
        def _():
            project(t - 4 - z)

        @pl.when(within(t))
        def _():
            mix(t)

        @pl.when(within(t - 1))
        def _():
            join(t - 1)

        return carry

    lax.fori_loop(0, steps + chips + 3, step, 0)

    midway = acc[...].astype(jnp.bfloat16)
    midway_ref[...] = midway
    midway_f = midway.astype(jnp.float32)
    squares = jnp.sum(midway_f * midway_f, axis=1, keepdims=True)
    sums[0] = jnp.broadcast_to(squares, (tokens, 128)).T[:8, :]
    copies = [
        remote(sums.at[0], sums.at[i + 1], sum_send.at[i], sum_recv.at[i], peer)
        for i, peer in enumerate(peers)
    ]
    for copy in copies:
        copy.start()
    scaled = midway_f * norm_ref[...]
    for copy in copies:
        copy.wait_recv()
    total = sums[0]
    for i in range(1, tps):
        total = total + sums[i]
    total = jnp.concatenate([total] * (128 // 8), axis=0).T[:, :1]
    normed_ref[...] = (scaled * lax.rsqrt(total / D + EPS_NORM)).astype(jnp.bfloat16)

    for copy in copies:
        copy.wait_send()

    def drain(j, carry):
        swap(j).wait_send()

        @pl.when(z < chips - 1)
        def _():
            chain(j).wait_send()

        for copy in gather(j):
            copy.wait_send()
        return carry

    lax.fori_loop(0, steps, drain, 0)


HEADS_PER_STEP = 2


def mixed_tokens(
    receptance, key_vectors, value_vectors, decay_logits, rate_logits, gate_logits, group_gain,
    residual, mixer_out, norm_gain,
):
    tokens, channels = receptance.shape
    features = residual.shape[1]
    tps = lax.axis_size("tp")
    width = HEADS_PER_STEP * HEAD
    steps = channels // width
    bf = jnp.bfloat16
    f32 = jnp.float32
    whole = pl.BlockSpec(memory_space=pltpu.VMEM)
    dma = pltpu.SemaphoreType.DMA
    return pl.pallas_call(
        mixer_kernel,
        in_specs=[whole] * 9 + [pl.BlockSpec(memory_space=pl.ANY)],
        out_specs=[whole, whole],
        out_shape=[jax.ShapeDtypeStruct((tokens, features), bf)] * 2,
        scratch_shapes=[
            pltpu.VMEM((steps, tps * width, features), bf),
            pltpu.VMEM((steps, tokens, 2 * width), f32),
            pltpu.VMEM((steps, width, 2 * HEAD), bf),
            pltpu.VMEM((steps, width, 2 * HEAD), bf),
            pltpu.VMEM((steps, width, 2 * HEAD), f32),
            pltpu.VMEM((steps, HEAD, width), f32),
            pltpu.VMEM((steps, HEAD, width), f32),
            pltpu.VMEM((steps, tokens, tps * width), bf),
            pltpu.VMEM((tokens, features), f32),
            pltpu.VMEM((tps, 8, tokens), f32),
            dma((steps, tps)),
            dma((steps,)),
            dma((steps,)),
            dma((steps,)),
            dma((steps,)),
            dma((tps - 1, steps)),
            dma((tps - 1, steps)),
            dma((tps - 1,)),
            dma((tps - 1,)),
        ],
        compiler_params=pltpu.CompilerParams(
            collective_id=5, has_side_effects=True, vmem_limit_bytes=56 * 1024 * 1024
        ),
        name="mixer",
    )(
        receptance, key_vectors, value_vectors, decay_logits, rate_logits, gate_logits,
        group_gain.reshape(1, channels), residual, norm_gain.reshape(1, features), mixer_out,
    )


def expert_kernel(
    normed_ref,
    midway_ref,
    ids_ref,
    weight_ref,
    gate_hbm,
    up_hbm,
    down_hbm,
    out_ref,
    gate_w,
    up_w,
    down_w,
    select,
    outgoing,
    aux_out,
    aux_in,
    rows_in,
    part_a,
    part_b,
    first_a,
    first_b,
    pass_a,
    pass_b,
    second_a,
    second_b,
    hidden_a,
    hidden_b,
    own_res,
    pair_out,
    pair_in,
    back_out,
    back_in,
    load_sem,
    disp_send,
    disp_recv,
    aux_send,
    aux_recv,
    fwd_send,
    fwd_recv,
    tp_send,
    tp_recv,
    pair_send,
    pair_recv,
    back_send,
    back_recv,
):
    tokens = normed_ref.shape[0]
    slots = outgoing.shape[1]
    quarter = slots // 4
    half = slots // 2
    width = hidden_a.shape[2]
    peers = GROUPS
    blocks = 2 * peers
    sp = lax.axis_index("sp")
    tp = lax.axis_index("tp")
    z, core = sp // 2, sp % 2
    y, x = tp // 2, tp % 2
    x_peer = y * 2 + (1 - x)
    y_peer = (1 - y) * 2 + x

    def chip(turn):
        step = (2 * turn - turn // 2) % 4
        return 2 * ((z // 2 + step // 2) % 2) + (z % 2 + step % 2) % 2

    loads = [
        pltpu.make_async_copy(source.at[0], target, load_sem.at[i])
        for i, (source, target) in enumerate(((gate_hbm, gate_w), (up_hbm, up_w), (down_hbm, down_w)))
    ]
    for load in loads:
        load.start()

    partner = {"sp": z * 2 + (1 - core)}
    barrier = pltpu.get_barrier_semaphore()
    friends = [partner, {"tp": x_peer}, {"tp": y_peer}]
    friends += [{"sp": chip(turn) * 2 + core} for turn in range(1, peers)]
    for friend in friends:
        pl.semaphore_signal(barrier, inc=1, device_id=friend, device_id_type=MESH)

    def remote(source, target, send, recv, device):
        return pltpu.make_async_remote_copy(
            src_ref=source, dst_ref=target, send_sem=send, recv_sem=recv,
            device_id=device, device_id_type=MESH,
        )

    def dispatch(turn):
        return remote(
            outgoing.at[turn], rows_in.at[2 * turn], disp_send.at[turn], disp_recv.at[turn],
            {"sp": chip(turn) * 2 + core},
        )

    def dispatch_aux(turn):
        return remote(
            aux_out.at[turn], aux_in.at[turn], aux_send.at[turn], aux_recv.at[turn],
            {"sp": chip(turn) * 2 + core},
        )

    def forward(turn):
        return remote(
            rows_in.at[2 * turn], rows_in.at[2 * turn + 1], fwd_send.at[turn], fwd_recv.at[turn], partner
        )

    def over_tp(kind, k, source, target, device):
        return remote(source, target, tp_send.at[kind, k], tp_recv.at[kind, k], {"tp": device})

    def rows(start, size):
        return pl.ds(pl.multiple_of(start, quarter), size)

    def sum_first(k):
        return (
            over_tp(0, k, part_a.at[k, rows(half * (1 - x), half)], first_a.at[k], x_peer),
            over_tp(1, k, part_b.at[k, rows(half * (1 - y), half)], first_b.at[k], y_peer),
        )

    def sum_second(k):
        return (
            over_tp(2, k, pass_a.at[k], second_a.at[k], y_peer),
            over_tp(3, k, pass_b.at[k], second_b.at[k], x_peer),
        )

    def spread_first(k):
        own_a = hidden_a.at[k, rows(half * x + quarter * y, quarter)]
        own_b = hidden_b.at[k, rows(half * y + quarter * x, quarter)]
        return (over_tp(4, k, own_a, own_a, y_peer), over_tp(5, k, own_b, own_b, x_peer))

    def spread_second(k):
        own_a = hidden_a.at[k, rows(half * x, half)]
        own_b = hidden_b.at[k, rows(half * y, half)]
        return (over_tp(6, k, own_a, own_a, x_peer), over_tp(7, k, own_b, own_b, y_peer))

    def pair(turn):
        return remote(pair_out.at[turn], pair_in.at[turn], pair_send.at[turn], pair_recv.at[turn], partner)

    def give_back(turn):
        return remote(
            back_out.at[turn], back_in.at[turn], back_send.at[turn], back_recv.at[turn],
            {"sp": chip(turn) * 2 + core},
        )

    ids = ids_ref[...]
    weights = weight_ref[...]
    lane = lax.broadcasted_iota(jnp.int32, (tokens, 128), 1)
    slot_lane = lax.broadcasted_iota(jnp.int32, (tokens, slots), 1).astype(jnp.float32)
    earlier = jnp.where(
        lax.broadcasted_iota(jnp.int32, (tokens, tokens), 1)
        < lax.broadcasted_iota(jnp.int32, (tokens, tokens), 0),
        1.0,
        0.0,
    ).astype(jnp.bfloat16)
    group_of = [chip(turn) for turn in range(peers)]
    member = [
        jnp.logical_and(ids[:, :1] >= 2 * group, ids[:, :1] < 2 * group + 2) for group in group_of
    ]
    members = jnp.zeros((tokens, 128), jnp.float32)
    for turn in range(peers):
        members = jnp.where(jnp.logical_and(lane == turn, member[turn]), 1.0, members)
    ranks = dot(earlier, members.astype(jnp.bfloat16), NN)
    normed = normed_ref[...]
    pl.semaphore_wait(barrier, len(friends))
    for turn in range(peers):
        chosen = jnp.where(
            jnp.logical_and(slot_lane == ranks[:, turn : turn + 1], member[turn]), 1.0, 0.0
        ).astype(jnp.bfloat16)
        select[turn] = chosen
        picked = dot(chosen, normed, TN).astype(jnp.bfloat16)
        if turn == 0:
            rows_in[0] = picked
            forward(0).start()
        else:
            outgoing[turn] = picked
            dispatch(turn).start()
        parts = jnp.zeros((tokens, 128), jnp.float32)
        for expert in range(2):
            name = 2 * group_of[turn] + expert
            value = jnp.where(ids[:, :1] == name, weights[:, :1], 0.0) + jnp.where(
                ids[:, 1:2] == name, weights[:, 1:2], 0.0
            )
            for piece in range(3):
                term = value.astype(jnp.bfloat16).astype(jnp.float32)
                parts = jnp.where(lane == 3 * expert + piece, term, parts)
                value = value - term
        by_slot = dot(parts.astype(jnp.bfloat16), chosen, TN)
        weight_rows = jnp.concatenate(
            [
                by_slot[0:1] + by_slot[1:2] + by_slot[2:3],
                by_slot[3:4] + by_slot[4:5] + by_slot[5:6],
                jnp.zeros((6, slots), jnp.float32),
            ],
            axis=0,
        )
        if turn == 0:
            aux_in[0] = weight_rows
        else:
            aux_out[turn] = weight_rows
            dispatch_aux(turn).start()
    for load in loads:
        load.wait()

    def step(t, carry):
        @pl.when(t < blocks)
        def _():
            k = t
            turn = k // 2

            @pl.when(jnp.logical_and(k % 2 == 0, k > 0))
            def _():
                dispatch(turn).wait_recv()
                forward(turn).start()

            @pl.when(k % 2 == 1)
            def _():
                forward(turn).wait_recv()

            block = rows_in[k]
            for part, columns in ((part_a, pl.ds(0, width)), (part_b, pl.ds(width, width))):
                part[k, :, :width] = dot(block, gate_w[:, columns], NN).astype(jnp.bfloat16)
                part[k, :, width:] = dot(block, up_w[:, columns], NN).astype(jnp.bfloat16)
            for copy in sum_first(k):
                copy.start()

        @pl.when(jnp.logical_and(t >= 1, t < blocks + 1))
        def _():
            k = t - 1
            copies = sum_first(k)
            nexts = sum_second(k)
            copies[0].wait_recv()
            pass_a[k] = (
                part_a[k, rows(half * x + quarter * (1 - y), quarter)].astype(jnp.float32)
                + first_a[k, rows(quarter * (1 - y), quarter)].astype(jnp.float32)
            ).astype(jnp.bfloat16)
            nexts[0].start()
            copies[1].wait_recv()
            pass_b[k] = (
                part_b[k, rows(half * y + quarter * (1 - x), quarter)].astype(jnp.float32)
                + first_b[k, rows(quarter * (1 - x), quarter)].astype(jnp.float32)
            ).astype(jnp.bfloat16)
            nexts[1].start()

        @pl.when(jnp.logical_and(t >= 2, t < blocks + 2))
        def _():
            k = t - 2
            copies = sum_second(k)
            nexts = spread_first(k)
            for i, (part, first, second, hidden, major, minor) in enumerate(
                (
                    (part_a, first_a, second_a, hidden_a, x, y),
                    (part_b, first_b, second_b, hidden_b, y, x),
                )
            ):
                copies[i].wait_recv()
                mine = rows(half * major + quarter * minor, quarter)
                total = (
                    part[k, mine].astype(jnp.float32)
                    + first[k, rows(quarter * minor, quarter)].astype(jnp.float32)
                    + second[k].astype(jnp.float32)
                )
                gate, up = total[:, :width], total[:, width:]
                hidden[k, mine] = (gate * sigmoid(gate) * up).astype(jnp.bfloat16)
                nexts[i].start()

        @pl.when(jnp.logical_and(t >= 3, t < blocks + 3))
        def _():
            k = t - 3
            for copy, follow in zip(spread_first(k), spread_second(k)):
                copy.wait_recv()
                follow.start()

        @pl.when(jnp.logical_and(t >= 4, t < blocks + 4))
        def _():
            k = t - 4
            turn = k // 2
            for copy in spread_second(k):
                copy.wait_recv()
            result = dot(hidden_a[k], down_w[:width, :], NN) + dot(hidden_b[k], down_w[width:, :], NN)

            @pl.when(k % 2 == 0)
            def _():
                own_res[turn] = result

            @pl.when(k % 2 == 1)
            def _():
                pair_out[turn] = result.astype(jnp.bfloat16)
                pair(turn).start()

        @pl.when(jnp.logical_and(t >= 6, t % 2 == 0))
        def _():
            turn = (t - 6) // 2

            @pl.when(turn > 0)
            def _():
                dispatch_aux(turn).wait_recv()

            pair(turn).wait_recv()
            columns = jnp.concatenate([aux_in[turn]] * (128 // 8), axis=0).T
            low, high = columns[:, 0:1], columns[:, 1:2]
            mine = jnp.where(core == 0, low, high)
            other = jnp.where(core == 0, high, low)
            both = (own_res[turn] * mine + pair_in[turn].astype(jnp.float32) * other).astype(
                jnp.bfloat16
            )

            @pl.when(turn == 0)
            def _():
                back_in[0] = both

            @pl.when(turn > 0)
            def _():
                back_out[turn] = both
                give_back(turn).start()

        return carry

    lax.fori_loop(0, blocks + 5, step, 0)
    total = midway_ref[...].astype(jnp.float32)
    for turn in range(peers):
        if turn > 0:
            give_back(turn).wait_recv()
        total = total + dot(select[turn], back_in[turn], NN)
    out_ref[...] = total.astype(jnp.bfloat16)

    for turn in range(peers):
        forward(turn).wait_send()
        pair(turn).wait_send()
        if turn > 0:
            dispatch(turn).wait_send()
            dispatch_aux(turn).wait_send()
            give_back(turn).wait_send()

    def drain(k, carry):
        for copies in (sum_first(k), sum_second(k), spread_first(k), spread_second(k)):
            for copy in copies:
                copy.wait_send()
        return carry

    lax.fori_loop(0, blocks, drain, 0)


def routed_experts(normed, midway, expert_ids, route_weight, expert_gate, expert_up, expert_down):
    tokens, features = normed.shape
    hidden = expert_gate.shape[2]
    half = hidden // 2
    slots = tokens // 2
    quarter = slots // 4
    peers = GROUPS
    blocks = 2 * peers
    bf = jnp.bfloat16
    whole = pl.BlockSpec(memory_space=pltpu.VMEM)
    far = pl.BlockSpec(memory_space=pl.ANY)
    dma = pltpu.SemaphoreType.DMA
    return pl.pallas_call(
        expert_kernel,
        in_specs=[whole] * 4 + [far] * 3,
        out_specs=whole,
        out_shape=jax.ShapeDtypeStruct((tokens, features), bf),
        scratch_shapes=[
            pltpu.VMEM((features, hidden), bf),
            pltpu.VMEM((features, hidden), bf),
            pltpu.VMEM((hidden, features), bf),
            pltpu.VMEM((peers, tokens, slots), bf),
            pltpu.VMEM((peers, slots, features), bf),
            pltpu.VMEM((peers, 8, slots), jnp.float32),
            pltpu.VMEM((peers, 8, slots), jnp.float32),
            pltpu.VMEM((blocks, slots, features), bf),
            pltpu.VMEM((blocks, slots, hidden), bf),
            pltpu.VMEM((blocks, slots, hidden), bf),
            pltpu.VMEM((blocks, slots // 2, hidden), bf),
            pltpu.VMEM((blocks, slots // 2, hidden), bf),
            pltpu.VMEM((blocks, quarter, hidden), bf),
            pltpu.VMEM((blocks, quarter, hidden), bf),
            pltpu.VMEM((blocks, quarter, hidden), bf),
            pltpu.VMEM((blocks, quarter, hidden), bf),
            pltpu.VMEM((blocks, slots, half), bf),
            pltpu.VMEM((blocks, slots, half), bf),
            pltpu.VMEM((peers, slots, features), jnp.float32),
            pltpu.VMEM((peers, slots, features), bf),
            pltpu.VMEM((peers, slots, features), bf),
            pltpu.VMEM((peers, slots, features), bf),
            pltpu.VMEM((peers, slots, features), bf),
            dma((3,)),
            dma((peers,)),
            dma((peers,)),
            dma((peers,)),
            dma((peers,)),
            dma((peers,)),
            dma((peers,)),
            dma((8, blocks)),
            dma((8, blocks)),
            dma((peers,)),
            dma((peers,)),
            dma((peers,)),
            dma((peers,)),
        ],
        compiler_params=pltpu.CompilerParams(
            collective_id=4, has_side_effects=True, vmem_limit_bytes=52 * 1024 * 1024
        ),
        name="experts",
    )(normed, midway, expert_ids, route_weight, expert_gate, expert_up, expert_down)


def local(
    receptance,
    key_vectors,
    value_vectors,
    decay_logits,
    rate_logits,
    gate_logits,
    group_gain,
    residual,
    mixer_out,
    norm_gain,
    expert_ids,
    route_weight,
    expert_gate,
    expert_up,
    expert_down,
):
    paired_cores = lax.axis_size("sp") == 2 * GROUPS and lax.axis_size("tp") == 4
    if paired_cores and expert_gate.shape[0] == 1:
        normed, midway = mixed_tokens(
            receptance, key_vectors, value_vectors, decay_logits, rate_logits, gate_logits,
            group_gain, residual, mixer_out, norm_gain,
        )
        return routed_experts(
            normed, midway, expert_ids, route_weight, expert_gate, expert_up, expert_down
        )
    mixed_rows = time_mix(
        receptance, key_vectors, value_vectors, decay_logits, rate_logits, gate_logits, group_gain
    )
    tokens_here, features = residual.shape
    projected = jnp.dot(
        gather_columns(mixed_rows, "tp", 0),
        mixer_out,
        preferred_element_type=jnp.float32,
    )
    midway = (residual.astype(jnp.float32) + projected).astype(jnp.bfloat16)
    midway_f = midway.astype(jnp.float32)
    squares = lax.psum(jnp.sum(midway_f * midway_f, axis=1), "tp")
    inv_rms = lax.rsqrt(squares / D + EPS_NORM)
    normed = (midway_f * norm_gain[None, :] * inv_rms[:, None]).astype(jnp.bfloat16)
    routes = expert_ids.shape[1]
    experts_all = lax.axis_size("sp") * expert_gate.shape[0]
    capacity = 2 * tokens_here * routes // experts_all
    flat_ids = expert_ids.reshape(-1)
    onehot = (flat_ids[:, None] == jnp.arange(experts_all, dtype=jnp.int32)[None, :]).astype(
        jnp.int32
    )
    earlier_count = jnp.sum((jnp.cumsum(onehot, axis=0) - onehot) * onehot, axis=1)
    slot_of = flat_ids * capacity + earlier_count
    owner_token = jnp.arange(tokens_here * routes, dtype=jnp.int32) // routes
    slot_table = (
        jnp.full((experts_all * capacity,), tokens_here, jnp.int32).at[slot_of].set(owner_token)
    )
    padded = jnp.concatenate([normed, jnp.zeros((1, features), jnp.bfloat16)], axis=0)
    outgoing = padded[slot_table].reshape(experts_all, capacity, features)
    arrived = swap_blocks(outgoing, "sp", 2)
    arrived_rows = arrived.reshape(-1, features)
    paired = jnp.concatenate([expert_gate[0], expert_up[0]], axis=1)
    gate_up = lax.psum_scatter(
        jnp.dot(arrived_rows, paired, preferred_element_type=jnp.float32).astype(jnp.bfloat16),
        "tp",
        scatter_dimension=0,
        tiled=True,
    ).astype(jnp.float32)
    half_width = paired.shape[1] // 2
    hidden = (jax.nn.silu(gate_up[:, :half_width]) * gate_up[:, half_width:]).astype(jnp.bfloat16)
    expert_res = jnp.dot(
        gather_rows(hidden, "tp", 1),
        expert_down[0],
        preferred_element_type=jnp.float32,
    )
    returned = swap_blocks(
        expert_res.astype(jnp.bfloat16).reshape(-1, capacity, features), "sp", 3
    )
    picked = (
        returned.reshape(-1, features)[slot_of]
        .astype(jnp.float32)
        .reshape(tokens_here, routes, features)
    )
    routed_sum = jnp.sum(picked * route_weight[:, :, None], axis=1)
    return (midway_f + routed_sum).astype(jnp.bfloat16)


def solution(mesh):
    placed = (
        P("sp", "tp"),
        P("sp", "tp"),
        P("sp", "tp"),
        P("sp", "tp"),
        P("sp", "tp"),
        P("sp", "tp"),
        P("tp"),
        P("sp", "tp"),
        P(None, "tp"),
        P("tp"),
        P("sp", None),
        P("sp", None),
        P("sp", "tp", None),
        P("sp", "tp", None),
        P("sp", None, "tp"),
    )
    return jax.shard_map(
        local, mesh=mesh, in_specs=placed, out_specs=P("sp", "tp"), check_vma=False
    )
```

```python
import jax
import jax.numpy as jnp
from jax import lax
from jax.experimental import pallas as pl
from jax.experimental.pallas import tpu as pltpu
from jax.sharding import PartitionSpec as P

D = 4096
HEAD = 64
CHUNK = 128
EXP_HALF = 0.6065306597126334


EPS_GROUP = 0.00064
EPS_NORM = 1e-06


def split(x):
    hi = x.astype(jnp.bfloat16)
    lo = (x - hi.astype(jnp.float32)).astype(jnp.bfloat16)
    return hi, lo


def dot(a, b, dims):
    return lax.dot_general(a, b, (dims, ((), ())), preferred_element_type=jnp.float32)


NN = ((1,), (0,))
NT = ((1,), (1,))
TN = ((0,), (0,))


def dot3(a, b, dims=NN):
    return dot(a[0], b[0], dims) + (dot(a[0], b[1], dims) + dot(a[1], b[0], dims))


def dot2(a, b, dims=NN):
    return dot(a[0], b, dims) + dot(a[1], b, dims)


def sigmoid(x):
    return 1.0 / (1.0 + jnp.exp(-x))


def mix_kernel(r_ref, k_ref, v_ref, d_ref, a_ref, out_ref, state_ref):
    tokens = r_ref.shape[0]
    chunks = tokens // CHUNK
    row = lax.broadcasted_iota(jnp.int32, (CHUNK, CHUNK), 0)
    col = lax.broadcasted_iota(jnp.int32, (CHUNK, CHUNK), 1)
    strict = col < row
    causal = col <= row
    eye = jnp.where(col == row, 1.0, 0.0)
    ones_lower = jnp.where(causal, 1.0, 0.0).astype(jnp.bfloat16)
    low = lax.broadcasted_iota(jnp.int32, (CHUNK, 2 * HEAD), 1) < HEAD

    work = []
    for chunk in range(chunks):
        rows = pl.ds(chunk * CHUNK, CHUNK)
        recept = r_ref[rows, :].astype(jnp.float32)
        keyvec = k_ref[rows, :].astype(jnp.float32)
        logdec = -EXP_HALF * sigmoid(d_ref[rows, :].astype(jnp.float32))
        first, second = split(logdec)
        third = (logdec - first.astype(jnp.float32) - second.astype(jnp.float32)).astype(jnp.bfloat16)
        cum_in = dot(ones_lower, first, NN) + (
            dot(ones_lower, second, NN) + dot(ones_lower, third, NN)
        )
        cum_end = cum_in[CHUNK - 1 :, :]
        squares = keyvec * keyvec
        norms = jnp.where(
            low,
            jnp.sum(squares[:, :HEAD], axis=1, keepdims=True),
            jnp.sum(squares[:, HEAD:], axis=1, keepdims=True),
        )
        unit_key = keyvec * lax.rsqrt(1.0 + norms)
        correction = unit_key * sigmoid(a_ref[rows, :].astype(jnp.float32))
        growth = jnp.exp(-cum_in)
        tail = jnp.exp(cum_end - cum_in)
        r_scaled = recept * jnp.exp(cum_in)
        u_scaled = unit_key * jnp.exp(cum_in - logdec)
        queries = split(jnp.concatenate([u_scaled, r_scaled], axis=0))
        sources = split(jnp.concatenate([keyvec * growth, correction * growth], axis=0))
        tails = split(jnp.concatenate([keyvec * tail, -(correction * tail)], axis=0))
        keep = jnp.broadcast_to(jnp.exp(cum_end), (2 * HEAD, 2 * HEAD)).T
        values = v_ref[rows, :]
        for head in range(2):
            lanes = slice(head * HEAD, (head + 1) * HEAD)
            query = tuple(q[:, lanes] for q in queries)
            source = tuple(s[:, lanes] for s in sources)
            scores = dot3(query, source, NT)
            work.append(
                dict(
                    head=head,
                    chunk=chunk,
                    query=query,
                    tail=tuple(t[:, lanes] for t in tails),
                    keep=keep[lanes, :],
                    value=jnp.concatenate(
                        [values[:, lanes], jnp.zeros((CHUNK, HEAD), jnp.bfloat16)], axis=1
                    ),
                    key_both=split(
                        jnp.concatenate(
                            [
                                jnp.where(strict, scores[:CHUNK, :CHUNK], 0.0),
                                jnp.where(causal, scores[CHUNK:, :CHUNK], 0.0),
                            ],
                            axis=0,
                        )
                    ),
                    pull=jnp.where(strict, scores[:CHUNK, CHUNK:], 0.0),
                    corr_read=split(jnp.where(causal, scores[CHUNK:, CHUNK:], 0.0)),
                )
            )
    for item in work:
        item["inverse"] = eye - jnp.where(row // 2 == col // 2, item["pull"], 0.0)
        item["from_values"] = dot2(item["key_both"], item["value"])
    size = 2
    while size < CHUNK:
        joined = (row // (2 * size) == col // (2 * size)) & (row // size != col // size)
        halves = []
        for item in work:
            inverse = split(item["inverse"])
            between = split(jnp.where(joined, item["pull"], 0.0))
            halves.append((inverse, dot3(between, inverse)))
        for item, (inverse, half) in zip(work, halves):
            item["inverse"] = item["inverse"] - dot3(inverse, split(half))
        size *= 2
    key_row = lax.broadcasted_iota(jnp.int32, (HEAD, 2 * HEAD), 0)
    lane = lax.broadcasted_iota(jnp.int32, (HEAD, 2 * HEAD), 1)
    start = jnp.where(lane == key_row + HEAD, 1.0, 0.0)
    states = [start, start]
    for item in work:
        head = item["head"]
        state = states[head]
        from_start = dot3(item["query"], split(state)) + item["from_values"]
        pulled = dot3(split(item["inverse"]), split(from_start[:CHUNK]))
        pulled_parts = split(pulled)
        out_ref[pl.ds(item["chunk"] * CHUNK, CHUNK), pl.ds(head * 2 * HEAD, 2 * HEAD)] = (
            from_start[CHUNK:] - dot3(item["corr_read"], pulled_parts)
        )
        key_tail = tuple(t[:CHUNK] for t in item["tail"])
        corr_tail = tuple(t[CHUNK:] for t in item["tail"])
        states[head] = (
            item["keep"] * state
            + dot2(key_tail, item["value"], TN)
            + dot3(corr_tail, pulled_parts, TN)
        )
    for head in range(2):
        state_ref[pl.ds(head * HEAD, HEAD), :] = states[head].astype(jnp.bfloat16)


def read_kernel(place_ref, read_ref, maps_ref, gate_ref, gain_ref, out_ref):
    def one(step, carried):
        following = []
        for head in range(2):
            both = maps_ref[step, pl.ds(head * HEAD, HEAD), :]
            parts = split(carried[head])
            step_map = both[:, HEAD:]
            following.append(
                both[:, :HEAD].astype(jnp.float32)
                + dot(step_map, parts[0], NN)
                + dot(step_map, parts[1], NN)
            )
        return tuple(following)

    zero = jnp.zeros((HEAD, HEAD), jnp.float32)
    incoming = lax.fori_loop(0, place_ref[0], one, (zero, zero))
    scaled = []
    for head in range(2):
        both = read_ref[:, pl.ds(head * 2 * HEAD, 2 * HEAD)]
        state_read = both[:, :HEAD] + dot3(split(both[:, HEAD:]), split(incoming[head]))
        centred = state_read - jnp.mean(state_read, axis=1, keepdims=True)
        variance = jnp.mean(centred * centred, axis=1, keepdims=True)
        scaled.append(centred * lax.rsqrt(variance + EPS_GROUP))
    gated = (
        jnp.concatenate(scaled, axis=1)
        * gain_ref[...]
        * sigmoid(gate_ref[...].astype(jnp.float32))
    )
    out_ref[...] = gated.astype(jnp.bfloat16)


def time_mix(
    receptance, key_vectors, value_vectors, decay_logits, rate_logits, gate_logits, group_gain
):
    tokens_here, channels = receptance.shape
    pairs = channels // (2 * HEAD)
    wide = pl.BlockSpec((tokens_here, 2 * HEAD), lambda i: (0, i))
    double = pl.BlockSpec((tokens_here, 4 * HEAD), lambda i: (0, i))
    reads, states = pl.pallas_call(
        mix_kernel,
        grid=(pairs,),
        in_specs=[wide] * 5,
        out_specs=[double, pl.BlockSpec((2 * HEAD, 2 * HEAD), lambda i: (i, 0))],
        out_shape=[
            jax.ShapeDtypeStruct((tokens_here, 2 * channels), jnp.float32),
            jax.ShapeDtypeStruct((channels, 2 * HEAD), jnp.bfloat16),
        ],
        name="mix",
    )(receptance, key_vectors, value_vectors, decay_logits, rate_logits)
    maps = lax.all_gather(states, "sp")
    place = lax.axis_index("sp").astype(jnp.int32).reshape(1)
    return pl.pallas_call(
        read_kernel,
        grid=(pairs,),
        in_specs=[
            pl.BlockSpec(memory_space=pltpu.SMEM),
            double,
            pl.BlockSpec((maps.shape[0], 2 * HEAD, 2 * HEAD), lambda i: (0, i, 0)),
            wide,
            pl.BlockSpec((1, 2 * HEAD), lambda i: (0, i)),
        ],
        out_specs=wide,
        out_shape=jax.ShapeDtypeStruct((tokens_here, channels), jnp.bfloat16),
        name="read",
    )(place, reads, maps, gate_logits, group_gain.reshape(1, channels))


def exchange(x, axis, shape, source, target, collective_id, name):
    def kernel(x_ref, out_ref, stage, send_sem, recv_sem, local_sem):
        n = lax.axis_size(axis)
        me = lax.axis_index(axis)
        peers = [lax.rem(me + step, n) for step in range(1, n)]
        barrier = pltpu.get_barrier_semaphore()
        for peer in peers:
            pl.semaphore_signal(
                barrier, inc=1, device_id={axis: peer}, device_id_type=pl.DeviceIdType.MESH
            )
        pl.semaphore_wait(barrier, n - 1)
        copies = []
        for step, peer in enumerate(peers):
            copy = pltpu.make_async_remote_copy(
                src_ref=source(x_ref, peer),
                dst_ref=target(out_ref, me),
                send_sem=send_sem.at[step],
                recv_sem=recv_sem.at[step],
                device_id={axis: peer},
                device_id_type=pl.DeviceIdType.MESH,
            )
            copy.start()
            copies.append(copy)
        own = pltpu.make_async_copy(source(x_ref, me), stage, local_sem)
        own.start()
        own.wait()
        own = pltpu.make_async_copy(stage, target(out_ref, me), local_sem)
        own.start()
        own.wait()
        for copy in copies:
            copy.wait()

    n = lax.axis_size(axis)
    return pl.pallas_call(
        kernel,
        in_specs=[pl.BlockSpec(memory_space=pl.ANY)],
        out_specs=pl.BlockSpec(memory_space=pl.ANY),
        out_shape=jax.ShapeDtypeStruct(shape, x.dtype),
        scratch_shapes=[
            pltpu.VMEM(x.shape[-2:], x.dtype),
            pltpu.SemaphoreType.DMA((n - 1,)),
            pltpu.SemaphoreType.DMA((n - 1,)),
            pltpu.SemaphoreType.DMA,
        ],
        compiler_params=pltpu.CompilerParams(collective_id=collective_id, has_side_effects=True),
        name=name,
    )(x)


def gather_columns(x, axis, collective_id):
    rows, columns = x.shape
    return exchange(
        x,
        axis,
        (rows, lax.axis_size(axis) * columns),
        lambda ref, peer: ref,
        lambda ref, me: ref.at[:, pl.ds(pl.multiple_of(me * columns, columns), columns)],
        collective_id,
        "gather_columns",
    )


def gather_rows(x, axis, collective_id):
    rows, columns = x.shape
    return exchange(
        x,
        axis,
        (lax.axis_size(axis) * rows, columns),
        lambda ref, peer: ref,
        lambda ref, me: ref.at[pl.ds(pl.multiple_of(me * rows, rows), rows), :],
        collective_id,
        "gather_rows",
    )


def swap_blocks(x, axis, collective_id):
    return exchange(
        x, axis, x.shape, lambda ref, peer: ref.at[peer], lambda ref, me: ref.at[me],
        collective_id, "swap_blocks",
    )


MESH = pl.DeviceIdType.MESH
GROUPS = 4


def pack_left(a):
    hi, lo = split(a)
    return jnp.concatenate([hi, lo], axis=1)


def pack_right(b):
    both = jnp.concatenate(split(b), axis=1)
    return jnp.concatenate([both, both], axis=0)


def dot_packed(left, right):
    out = dot(left, right, NN)
    n = out.shape[1] // 2
    return out[:, :n] + out[:, n:]


def three(a, axis, second):
    hi, lo = split(a)
    return jnp.concatenate([hi, hi, lo] if second else [hi, lo, hi], axis=axis)


def lower_rows(a, size):
    starts = range(size, a.shape[0], 2 * size)
    return jnp.concatenate([a[at : at + size] for at in starts], axis=0)


def join_rows(a, lower, size):
    parts = []
    for i, at in enumerate(range(0, a.shape[0], 2 * size)):
        parts += [a[at : at + size], lower[i * size : (i + 1) * size]]
    return jnp.concatenate(parts, axis=0)


def spread_rows(lower, size):
    parts = []
    for at in range(0, lower.shape[0], size):
        parts += [jnp.zeros((size, lower.shape[1]), lower.dtype), lower[at : at + size]]
    return jnp.concatenate(parts, axis=0)


def mix_heads(recept_in, key_in, values_in, decay_in, rate_in, write_read, write_state):
    tokens, width = recept_in.shape
    chunks = tokens // CHUNK
    pairs = width // (2 * HEAD)
    row = lax.broadcasted_iota(jnp.int32, (CHUNK, CHUNK), 0)
    col = lax.broadcasted_iota(jnp.int32, (CHUNK, CHUNK), 1)
    strict = col < row
    causal = col <= row
    eye = jnp.where(col == row, 1.0, 0.0)
    ones_lower = jnp.where(causal, 1.0, 0.0).astype(jnp.bfloat16)
    ones_twice = jnp.concatenate([ones_lower, ones_lower], axis=1)
    low = lax.broadcasted_iota(jnp.int32, (CHUNK, 2 * HEAD), 1) < HEAD
    nothing = jnp.zeros((CHUNK, 2 * HEAD), jnp.bfloat16)

    work = []
    for chunk in range(chunks):
        rows = slice(chunk * CHUNK, (chunk + 1) * CHUNK)
        for pair in range(pairs):
            lanes = slice(pair * 2 * HEAD, (pair + 1) * 2 * HEAD)
            recept = recept_in[rows, lanes].astype(jnp.float32)
            keyvec = key_in[rows, lanes].astype(jnp.float32)
            values = values_in[rows, lanes]
            logdec = -EXP_HALF * sigmoid(decay_in[rows, lanes].astype(jnp.float32))
            first, second = split(logdec)
            third = (logdec - first.astype(jnp.float32) - second.astype(jnp.float32)).astype(
                jnp.bfloat16
            )
            cum_in = dot_packed(
                ones_twice,
                jnp.concatenate(
                    [
                        jnp.concatenate([first, third], axis=1),
                        jnp.concatenate([second, nothing], axis=1),
                    ],
                    axis=0,
                ),
            )
            cum_end = cum_in[CHUNK - 1 :, :]
            squares = keyvec * keyvec
            norms = jnp.where(
                low,
                jnp.sum(squares[:, :HEAD], axis=1, keepdims=True),
                jnp.sum(squares[:, HEAD:], axis=1, keepdims=True),
            )
            unit_key = keyvec * lax.rsqrt(1.0 + norms)
            correction = unit_key * sigmoid(rate_in[rows, lanes].astype(jnp.float32))
            growth = jnp.exp(-cum_in)
            tail = jnp.exp(cum_end - cum_in)
            r_scaled = recept * jnp.exp(cum_in)
            u_scaled = unit_key * jnp.exp(cum_in - logdec)
            queries = jnp.concatenate([u_scaled, r_scaled], axis=0)
            sources = jnp.concatenate([keyvec * growth, correction * growth], axis=0)
            tails = jnp.concatenate([(keyvec * tail).T, -(correction * tail).T], axis=1)
            tail_hi, tail_lo = split(tails)
            keep = jnp.broadcast_to(jnp.exp(cum_end), (2 * HEAD, 2 * HEAD)).T
            for head in range(2):
                part = slice(head * HEAD, (head + 1) * HEAD)
                query = three(queries[:, part], 1, False)
                scores = dot(query, three(sources[:, part], 1, True), NT)
                value = jnp.concatenate(
                    [values[:, part], jnp.zeros((CHUNK, HEAD), jnp.bfloat16)], axis=1
                )
                work.append(
                    dict(
                        head=2 * pair + head,
                        chunk=chunk,
                        query=query,
                        tail=jnp.concatenate([tail_hi[part, :], tail_lo[part, :]], axis=0),
                        keep=keep[part, :],
                        value=value,
                        key_both=pack_left(
                            jnp.concatenate(
                                [
                                    jnp.where(strict, scores[:CHUNK, :CHUNK], 0.0),
                                    jnp.where(causal, scores[CHUNK:, :CHUNK], 0.0),
                                ],
                                axis=0,
                            )
                        ),
                        pull=jnp.where(strict, scores[:CHUNK, CHUNK:], 0.0),
                        corr_read=pack_left(jnp.where(causal, scores[CHUNK:, CHUNK:], 0.0)),
                    )
                )
    for item in work:
        item["inverse"] = eye - jnp.where(row // 2 == col // 2, item["pull"], 0.0)
        value = item["value"]
        item["from_values"] = dot(
            item["key_both"], jnp.concatenate([value, value], axis=0), NN
        )
    size = 2
    while size < CHUNK:
        joined = (row // (2 * size) == col // (2 * size)) & (row // size != col // size)
        halves = []
        if size < 8:
            for item in work:
                between = pack_left(jnp.where(joined, item["pull"], 0.0))
                halves.append(dot_packed(between, pack_right(item["inverse"])))
            for item, half in zip(work, halves):
                item["inverse"] = item["inverse"] - dot_packed(
                    pack_left(item["inverse"]), pack_right(half)
                )
        else:
            for item in work:
                between = pack_left(lower_rows(jnp.where(joined, item["pull"], 0.0), size))
                halves.append(dot_packed(between, pack_right(item["inverse"])))
            for item, half in zip(work, halves):
                inverse = item["inverse"]
                below = lower_rows(inverse, size)
                update = dot_packed(pack_left(below), pack_right(spread_rows(half, size)))
                item["inverse"] = join_rows(inverse, below - update, size)
        size *= 2
    key_row = lax.broadcasted_iota(jnp.int32, (HEAD, 2 * HEAD), 0)
    lane = lax.broadcasted_iota(jnp.int32, (HEAD, 2 * HEAD), 1)
    start = jnp.where(lane == key_row + HEAD, 1.0, 0.0)
    states = [start] * (2 * pairs)
    for chunk in range(chunks):
        items = [item for item in work if item["chunk"] == chunk]
        froms = [
            dot(item["query"], three(states[item["head"]], 0, True), NN) + item["from_values"]
            for item in items
        ]
        pulls = [
            dot_packed(pack_left(item["inverse"]), pack_right(value[:CHUNK]))
            for item, value in zip(items, froms)
        ]
        for item, value, pulled in zip(items, froms, pulls):
            head = item["head"]
            write_read(
                chunk, head, value[CHUNK:] - dot_packed(item["corr_read"], pack_right(pulled))
            )
            hi, lo = split(pulled)
            right = jnp.concatenate(
                [
                    jnp.concatenate([item["value"], hi], axis=0),
                    jnp.concatenate([nothing, lo], axis=0),
                ],
                axis=1,
            )
            out = dot(item["tail"], right, NN)
            states[head] = (
                item["keep"] * states[head]
                + (out[:HEAD, : 2 * HEAD] + out[HEAD:, : 2 * HEAD])
                + out[:HEAD, 2 * HEAD :]
            )
    for head in range(2 * pairs):
        write_state(head, states[head].astype(jnp.bfloat16))


def mixer_kernel(
    r_ref,
    k_ref,
    v_ref,
    d_ref,
    a_ref,
    gate_ref,
    gain_ref,
    residual_ref,
    norm_ref,
    mixer_hbm,
    normed_ref,
    midway_ref,
    mixer_w,
    reads,
    maps_own,
    maps_in,
    joint,
    joint_in,
    carry_out,
    carry_in,
    carried,
    gathered,
    acc,
    sums,
    load_sem,
    swap_send,
    swap_recv,
    chain_send,
    chain_recv,
    joint_send,
    joint_recv,
    gather_send,
    gather_recv,
    sum_send,
    sum_recv,
):
    tokens, features = residual_ref.shape
    steps, _, wide = reads.shape
    width = wide // 2
    heads = width // HEAD
    tps = lax.axis_size("tp")
    chips = lax.axis_size("sp") // 2
    sp = lax.axis_index("sp")
    tp = lax.axis_index("tp")
    z, core = sp // 2, sp % 2
    partner = {"sp": z * 2 + (1 - core)}
    y, x = tp // 2, tp % 2
    x_peer = y * 2 + (1 - x)
    y_peer = (1 - y) * 2 + x
    peers = [{"tp": x_peer}, {"tp": y_peer}, {"tp": (1 - y) * 2 + (1 - x)}]

    def load(step, block):
        return pltpu.make_async_copy(
            mixer_hbm.at[pl.ds(pl.multiple_of(block * steps * width + step * width, width), width), :],
            mixer_w.at[step, pl.ds(block * width, width), :],
            load_sem.at[step, block],
        )

    def load_all(step, carry):
        for block in range(tps):
            load(step, block).start()
        return carry

    lax.fori_loop(0, steps, load_all, 0)

    barrier = pltpu.get_barrier_semaphore()
    friends = [partner] + peers
    friends += [{"sp": ((z + shift) % chips) * 2 + core} for shift in range(1, chips)]
    for friend in friends:
        pl.semaphore_signal(barrier, inc=1, device_id=friend, device_id_type=MESH)
    acc[...] = residual_ref[...].astype(jnp.float32)
    pl.semaphore_wait(barrier, len(friends))

    def remote(source, target, send, recv, device):
        return pltpu.make_async_remote_copy(
            src_ref=source, dst_ref=target, send_sem=send, recv_sem=recv,
            device_id=device, device_id_type=MESH,
        )

    def swap(j):
        return remote(maps_own.at[j], maps_in.at[j], swap_send.at[j], swap_recv.at[j], partner)

    def chain(j, hop, target):
        return remote(
            carry_out.at[j], carry_in.at[j], chain_send.at[hop, j], chain_recv.at[j],
            {"sp": target * 2 + core},
        )

    def hand_joint(j):
        return remote(
            joint.at[j], joint_in.at[j], joint_send.at[j], joint_recv.at[j],
            {"sp": (chips - 1) * 2 + core},
        )

    def columns(owner):
        return pl.ds(pl.multiple_of(owner * width, width), width)

    def gather(j):
        own = gathered.at[j, :, columns(tp)]
        return [
            remote(own, own, gather_send.at[i, j], gather_recv.at[i, j], peers[i]) for i in range(2)
        ]

    def relay(j):
        low = gathered.at[j, pl.ds(0, tokens // 2), columns(x_peer)]
        high = gathered.at[j, pl.ds(tokens // 2, tokens // 2), columns(y_peer)]
        return [
            remote(low, low, gather_send.at[2, j], gather_recv.at[2, j], peers[1]),
            remote(high, high, gather_send.at[3, j], gather_recv.at[3, j], peers[0]),
        ]

    def mix(i):
        lanes = pl.ds(pl.multiple_of(i * width, width), width)

        def write_read(chunk, head, value):
            reads[i, pl.ds(chunk * CHUNK, CHUNK), pl.ds(head * 2 * HEAD, 2 * HEAD)] = value

        def write_state(head, value):
            maps_own[i, pl.ds(head * HEAD, HEAD), :] = value

        mix_heads(
            r_ref[:, lanes], k_ref[:, lanes], v_ref[:, lanes], d_ref[:, lanes], a_ref[:, lanes],
            write_read, write_state,
        )
        swap(i).start()

    half_lane = lax.broadcasted_iota(jnp.int32, (HEAD, 2 * HEAD), 1) < HEAD

    def join(j):
        swap(j).wait_recv()
        for head in range(heads):
            part = pl.ds(head * HEAD, HEAD)
            own, other = maps_own[j, part, :], maps_in[j, part, :]
            first = jnp.where(core == 0, own, other)
            second = jnp.where(core == 0, other, own)
            both = dot(second[:, HEAD:], first, NN)
            joint[j, part, :] = both + jnp.where(half_lane, second.astype(jnp.float32), 0.0)

        @pl.when(z == 0)
        def _():
            carry_out[j] = jnp.concatenate(
                [joint[j, pl.ds(head * HEAD, HEAD), :][:, :HEAD] for head in range(heads)], axis=1
            ).astype(jnp.bfloat16)
            carried[j] = jnp.zeros((HEAD, width), jnp.bfloat16)
            chain(j, 0, 1).start()

        @pl.when(z == 2)
        def _():
            hand_joint(j).start()

    def advance(maps, j):
        following = []
        for head in range(heads):
            both = maps[j, pl.ds(head * HEAD, HEAD), :]
            value = carry_in[j, :, pl.ds(head * HEAD, HEAD)]
            following.append(both[:, :HEAD] + dot2(split(both[:, HEAD:]), value))
        return jnp.concatenate(following, axis=1).astype(jnp.bfloat16)

    def hop(j):
        chain(j, 0, 1).wait_recv()
        carried[j] = carry_in[j]
        carry_out[j] = advance(joint, j)
        chain(j, 0, 2).start()
        chain(j, 1, 3).start()

    def finish(j):
        @pl.when(z >= 2)
        def _():
            chain(j, 0, 1).wait_recv()

        @pl.when(z == 2)
        def _():
            carried[j] = carry_in[j]

        @pl.when(z == 3)
        def _():
            hand_joint(j).wait_recv()
            carried[j] = advance(joint_in, j)

        nothing = jnp.zeros((HEAD, HEAD), jnp.bfloat16)
        unit = jnp.where(
            lax.broadcasted_iota(jnp.int32, (HEAD, HEAD), 0)
            == lax.broadcasted_iota(jnp.int32, (HEAD, HEAD), 1),
            1.0,
            0.0,
        ).astype(jnp.bfloat16)
        state_parts = []
        for head in range(heads):
            value = carried[j, :, pl.ds(head * HEAD, HEAD)]
            other = maps_in[j, pl.ds(head * HEAD, HEAD), :]
            passed = other[:, :HEAD].astype(jnp.float32) + dot(other[:, HEAD:], value, NN)
            state_parts.append(split(jnp.where(core == 0, value.astype(jnp.float32), passed)))
        head_of = [
            lax.broadcasted_iota(jnp.int32, (4 * HEAD, 2 * HEAD), axis) // HEAD % 2
            for axis in range(2)
        ]
        average = jnp.where(head_of[0] == head_of[1], 1.0 / HEAD, 0.0).astype(jnp.bfloat16)
        for pair in range(heads // 2):
            here = [reads[j, :, pl.ds((2 * pair + i) * 2 * HEAD, 2 * HEAD)] for i in range(2)]
            hi, lo = split(jnp.concatenate(here, axis=1))
            (first_hi, first_lo), (second_hi, second_lo) = state_parts[2 * pair : 2 * pair + 2]
            wide_rows = [
                [unit, nothing, nothing, nothing],
                [first_hi, nothing, first_lo, nothing],
                [nothing, unit, nothing, nothing],
                [nothing, second_hi, nothing, second_lo],
            ]
            right = jnp.concatenate(
                [jnp.concatenate(blocks, axis=1) for blocks in wide_rows], axis=0
            )
            state_read = dot_packed(hi, right) + dot(lo, right[:, : 2 * HEAD], NN)
            centred = state_read - dot(pack_left(state_read), average, NN)
            variance = dot(pack_left(centred * centred), average, NN)
            lanes = pl.ds(pl.multiple_of(j * width + pair * 2 * HEAD, 2 * HEAD), 2 * HEAD)
            gated = (
                centred
                * lax.rsqrt(variance + EPS_GROUP)
                * gain_ref[:, lanes]
                * sigmoid(gate_ref[:, lanes].astype(jnp.float32))
            )
            own_lanes = pl.ds(pl.multiple_of(tp * width + pair * 2 * HEAD, 2 * HEAD), 2 * HEAD)
            gathered[j, :, own_lanes] = gated.astype(jnp.bfloat16)
        for copy in gather(j):
            copy.start()

    def pass_on(j):
        for copy, after in zip(gather(j), relay(j)):
            copy.wait_recv()
            after.start()

    def project(j):
        for block in range(tps):
            load(j, block).wait()
        for copy in relay(j):
            copy.wait_recv()
        acc[...] += dot(gathered[j], mixer_w[j], NN)

    def within(j):
        return jnp.logical_and(j >= 0, j < steps)

    def step(t, carry):
        @pl.when(jnp.logical_and(z == 1, within(t - 2)))
        def _():
            hop(t - 2)

        @pl.when(within(t))
        def _():
            mix(t)

        @pl.when(within(t - 1))
        def _():
            join(t - 1)

        @pl.when(jnp.logical_and(z == 0, within(t - 1)))
        def _():
            finish(t - 1)

        @pl.when(jnp.logical_and(z > 0, within(t - 2)))
        def _():
            finish(t - 2)

        @pl.when(within(t - 3))
        def _():
            pass_on(t - 3)

        @pl.when(within(t - 4))
        def _():
            project(t - 4)

        return carry

    lax.fori_loop(0, steps + 4, step, 0)

    midway = acc[...].astype(jnp.bfloat16)
    midway_ref[...] = midway
    midway_f = midway.astype(jnp.float32)
    squares = jnp.sum(midway_f * midway_f, axis=1, keepdims=True)
    sums[0] = jnp.broadcast_to(squares, (tokens, 128)).T[:8, :]
    copies = [
        remote(sums.at[0], sums.at[i + 1], sum_send.at[i], sum_recv.at[i], peer)
        for i, peer in enumerate(peers)
    ]
    for copy in copies:
        copy.start()
    scaled = midway_f * norm_ref[...]
    for copy in copies:
        copy.wait_recv()
    total = sums[0]
    for i in range(1, tps):
        total = total + sums[i]
    total = jnp.concatenate([total] * (128 // 8), axis=0).T[:, :1]
    normed_ref[...] = (scaled * lax.rsqrt(total / D + EPS_NORM)).astype(jnp.bfloat16)

    for copy in copies:
        copy.wait_send()

    def drain(j, carry):
        swap(j).wait_send()

        @pl.when(z < 2)
        def _():
            chain(j, 0, 1).wait_send()

        @pl.when(z == 1)
        def _():
            chain(j, 1, 1).wait_send()

        @pl.when(z == 2)
        def _():
            hand_joint(j).wait_send()

        for copy in gather(j) + relay(j):
            copy.wait_send()
        return carry

    lax.fori_loop(0, steps, drain, 0)


HEADS_PER_STEP = 4


def mixed_tokens(
    receptance, key_vectors, value_vectors, decay_logits, rate_logits, gate_logits, group_gain,
    residual, mixer_out, norm_gain,
):
    tokens, channels = receptance.shape
    features = residual.shape[1]
    tps = lax.axis_size("tp")
    width = HEADS_PER_STEP * HEAD
    steps = channels // width
    bf = jnp.bfloat16
    f32 = jnp.float32
    whole = pl.BlockSpec(memory_space=pltpu.VMEM)
    dma = pltpu.SemaphoreType.DMA
    return pl.pallas_call(
        mixer_kernel,
        in_specs=[whole] * 9 + [pl.BlockSpec(memory_space=pl.ANY)],
        out_specs=[whole, whole],
        out_shape=[jax.ShapeDtypeStruct((tokens, features), bf)] * 2,
        scratch_shapes=[
            pltpu.VMEM((steps, tps * width, features), bf),
            pltpu.VMEM((steps, tokens, 2 * width), f32),
            pltpu.VMEM((steps, width, 2 * HEAD), bf),
            pltpu.VMEM((steps, width, 2 * HEAD), bf),
            pltpu.VMEM((steps, width, 2 * HEAD), f32),
            pltpu.VMEM((steps, width, 2 * HEAD), f32),
            pltpu.VMEM((steps, HEAD, width), bf),
            pltpu.VMEM((steps, HEAD, width), bf),
            pltpu.VMEM((steps, HEAD, width), bf),
            pltpu.VMEM((steps, tokens, tps * width), bf),
            pltpu.VMEM((tokens, features), f32),
            pltpu.VMEM((tps, 8, tokens), f32),
            dma((steps, tps)),
            dma((steps,)),
            dma((steps,)),
            dma((2, steps)),
            dma((steps,)),
            dma((steps,)),
            dma((steps,)),
            dma((4, steps)),
            dma((4, steps)),
            dma((tps - 1,)),
            dma((tps - 1,)),
        ],
        compiler_params=pltpu.CompilerParams(
            collective_id=5, has_side_effects=True, vmem_limit_bytes=56 * 1024 * 1024
        ),
        name="mixer",
    )(
        receptance, key_vectors, value_vectors, decay_logits, rate_logits, gate_logits,
        group_gain.reshape(1, channels), residual, norm_gain.reshape(1, features), mixer_out,
    )


LAG = 1


def expert_kernel(
    normed_hbm,
    midway_hbm,
    ids_ref,
    weight_ref,
    gate_hbm,
    up_hbm,
    down_hbm,
    out_ref,
    normed_ref,
    midway_ref,
    gate_w,
    up_w,
    down_w,
    select,
    outgoing,
    factors,
    aux_out,
    aux_in,
    rows_in,
    part_a,
    part_b,
    first_a,
    first_b,
    pass_a,
    pass_b,
    second_a,
    second_b,
    hidden_a,
    hidden_b,
    own_res,
    pair_out,
    pair_in,
    back_out,
    back_in,
    load_sem,
    disp_send,
    disp_recv,
    aux_send,
    aux_recv,
    fwd_send,
    fwd_recv,
    tp_send,
    tp_recv,
    pair_send,
    pair_recv,
    back_send,
    back_recv,
):
    tokens = normed_ref.shape[0]
    size = outgoing.shape[1]
    slots = 2 * size
    quarter = size // 4
    half = size // 2
    width = hidden_a.shape[2]
    peers = GROUPS
    units = 2 * peers
    blocks = 2 * units
    sp = lax.axis_index("sp")
    tp = lax.axis_index("tp")
    z, core = sp // 2, sp % 2
    y, x = tp // 2, tp % 2
    x_peer = y * 2 + (1 - x)
    y_peer = (1 - y) * 2 + x

    def chip(turn):
        return 2 * ((z // 2 + turn // 2) % 2) + (z % 2 + turn % 2) % 2

    def turn_of(q):
        return (q + 6) // 8 + (q + 5) // 8 + (q + 3) // 8 - 2 * ((q + 1) // 8)

    def half_of(q):
        return (q + 7) // 8 - (q + 6) // 8 + (q + 4) // 8 - (q + 3) // 8 + (q + 2) // 8

    loads = [
        pltpu.make_async_copy(source.at[0], target, load_sem.at[i])
        for i, (source, target) in enumerate(((gate_hbm, gate_w), (up_hbm, up_w), (down_hbm, down_w)))
    ]
    load_rows = pltpu.make_async_copy(normed_hbm, normed_ref, load_sem.at[3])
    load_rows.start()
    loads.append(pltpu.make_async_copy(midway_hbm, midway_ref, load_sem.at[4]))
    for load in loads:
        load.start()

    partner = {"sp": z * 2 + (1 - core)}
    barrier = pltpu.get_barrier_semaphore()
    friends = [partner, {"tp": x_peer}, {"tp": y_peer}]
    friends += [{"sp": chip(turn) * 2 + core} for turn in range(1, peers)]
    for friend in friends:
        pl.semaphore_signal(barrier, inc=1, device_id=friend, device_id_type=MESH)

    def remote(source, target, send, recv, device):
        return pltpu.make_async_remote_copy(
            src_ref=source, dst_ref=target, send_sem=send, recv_sem=recv,
            device_id=device, device_id_type=MESH,
        )

    def dispatch(q):
        return remote(
            outgoing.at[q], rows_in.at[2 * q], disp_send.at[q], disp_recv.at[q],
            {"sp": chip(turn_of(q)) * 2 + core},
        )

    def dispatch_aux(turn):
        return remote(
            aux_out.at[turn], aux_in.at[turn], aux_send.at[turn], aux_recv.at[turn],
            {"sp": chip(turn) * 2 + core},
        )

    def forward(q):
        return remote(rows_in.at[2 * q], rows_in.at[2 * q + 1], fwd_send.at[q], fwd_recv.at[q], partner)

    def over_tp(kind, k, source, target, device):
        return remote(source, target, tp_send.at[kind, k], tp_recv.at[kind, k], {"tp": device})

    def rows(start, size):
        return pl.ds(pl.multiple_of(start, quarter), size)

    def sum_first(k):
        return (
            over_tp(0, k, part_a.at[k, rows(half * (1 - x), half)], first_a.at[k], x_peer),
            over_tp(1, k, part_b.at[k, rows(half * (1 - y), half)], first_b.at[k], y_peer),
        )

    def sum_second(k):
        return (
            over_tp(2, k, pass_a.at[k], second_a.at[k], y_peer),
            over_tp(3, k, pass_b.at[k], second_b.at[k], x_peer),
        )

    def spread_first(k):
        own_a = hidden_a.at[k, rows(half * x + quarter * y, quarter)]
        own_b = hidden_b.at[k, rows(half * y + quarter * x, quarter)]
        return (over_tp(4, k, own_a, own_a, y_peer), over_tp(5, k, own_b, own_b, x_peer))

    def spread_second(k):
        own_a = hidden_a.at[k, rows(half * x, half)]
        own_b = hidden_b.at[k, rows(half * y, half)]
        return (over_tp(6, k, own_a, own_a, x_peer), over_tp(7, k, own_b, own_b, y_peer))

    def pair(q):
        return remote(pair_out.at[q], pair_in.at[q], pair_send.at[q], pair_recv.at[q], partner)

    def back_rows(q):
        return pl.ds(pl.multiple_of(turn_of(q) * slots + half_of(q) * size, size), size)

    def give_back(q):
        return remote(
            back_out.at[q], back_in.at[back_rows(q), :], back_send.at[q], back_recv.at[q],
            {"sp": chip(turn_of(q)) * 2 + core},
        )

    def as_columns(few_rows):
        return jnp.concatenate([few_rows] * (slots // 8), axis=0).T

    def few_rows():
        few = jnp.concatenate(
            [ids_ref[...].astype(jnp.float32), weight_ref[...], jnp.zeros((4, tokens), jnp.float32)],
            axis=0,
        )
        return jnp.concatenate([few] * (128 // 8), axis=0).T

    ids = few_rows()[:, :2].astype(jnp.int32)
    lane = lax.broadcasted_iota(jnp.int32, (tokens, 128), 1)
    slot_lane = lax.broadcasted_iota(jnp.int32, (tokens, slots), 1).astype(jnp.float32)
    earlier = jnp.where(
        lax.broadcasted_iota(jnp.int32, (tokens, tokens), 1)
        < lax.broadcasted_iota(jnp.int32, (tokens, tokens), 0),
        1.0,
        0.0,
    ).astype(jnp.bfloat16)
    group_of = [chip(turn) for turn in range(peers)]
    member = [
        jnp.logical_and(ids[:, :1] >= 2 * group, ids[:, :1] < 2 * group + 2) for group in group_of
    ]
    members = jnp.zeros((tokens, 128), jnp.float32)
    for turn in range(peers):
        members = jnp.where(jnp.logical_and(lane == turn, member[turn]), 1.0, members)
    ranks = dot(earlier, members.astype(jnp.bfloat16), NN)
    load_rows.wait()
    normed = normed_ref[...]
    pl.semaphore_wait(barrier, len(friends))
    for turn in range(peers):
        chosen = jnp.where(
            jnp.logical_and(slot_lane == ranks[:, turn : turn + 1], member[turn]), 1.0, 0.0
        ).astype(jnp.bfloat16)
        select[:, turn * slots : (turn + 1) * slots] = chosen
        picked = dot(chosen, normed, TN).astype(jnp.bfloat16)
        for part in range(2):
            piece = picked[part * size : (part + 1) * size]
            if turn == 0:
                rows_in[2 * part] = piece
                forward(part).start()
            else:
                q = {(1, 0): 2, (2, 0): 3, (2, 1): 4, (3, 0): 5, (3, 1): 6, (1, 1): 7}[turn, part]
                outgoing[q] = piece
                if q < 7:
                    dispatch(q).start()
    dispatch(7).start()
    for load in loads:
        load.wait()

    def weigh():
        few = few_rows()
        lane_of = lax.broadcasted_iota(jnp.int32, (tokens, 128), 1)
        ids, weights = few[:, :2].astype(jnp.int32), few[:, 2:4]
        for turn in range(peers):
            parts = jnp.zeros((tokens, 128), jnp.float32)
            for expert in range(2):
                name = 2 * group_of[turn] + expert
                value = jnp.where(ids[:, :1] == name, weights[:, :1], 0.0) + jnp.where(
                    ids[:, 1:2] == name, weights[:, 1:2], 0.0
                )
                for piece in range(3):
                    term = value.astype(jnp.bfloat16).astype(jnp.float32)
                    parts = jnp.where(lane_of == 3 * expert + piece, term, parts)
                    value = value - term
            by_slot = dot(
                parts.astype(jnp.bfloat16), select[:, turn * slots : (turn + 1) * slots], TN
            )
            weight_rows = jnp.concatenate(
                [
                    by_slot[0:1] + by_slot[1:2] + by_slot[2:3],
                    by_slot[3:4] + by_slot[4:5] + by_slot[5:6],
                    jnp.zeros((6, slots), jnp.float32),
                ],
                axis=0,
            )
            if turn == 0:
                factors[0] = as_columns(weight_rows)
            else:
                aux_out[turn] = weight_rows
                dispatch_aux(turn).start()

    def step(t, carry):
        @pl.when(t < blocks)
        def _():
            k = t
            q = k // 2

            @pl.when(jnp.logical_and(k % 2 == 0, q > 1))
            def _():
                dispatch(q).wait_recv()
                forward(q).start()

            @pl.when(k % 2 == 1)
            def _():
                forward(q).wait_recv()

            block = rows_in[k]
            for part, columns in ((part_a, pl.ds(0, width)), (part_b, pl.ds(width, width))):
                part[k, :, :width] = dot(block, gate_w[:, columns], NN).astype(jnp.bfloat16)
                part[k, :, width:] = dot(block, up_w[:, columns], NN).astype(jnp.bfloat16)
            for copy in sum_first(k):
                copy.start()

        @pl.when(t == 1)
        def _():
            weigh()

        @pl.when(jnp.logical_and(t >= LAG, t < blocks + LAG))
        def _():
            k = t - LAG
            copies = sum_first(k)
            nexts = sum_second(k)
            copies[0].wait_recv()
            pass_a[k] = (
                part_a[k, rows(half * x + quarter * (1 - y), quarter)].astype(jnp.float32)
                + first_a[k, rows(quarter * (1 - y), quarter)].astype(jnp.float32)
            ).astype(jnp.bfloat16)
            nexts[0].start()
            copies[1].wait_recv()
            pass_b[k] = (
                part_b[k, rows(half * y + quarter * (1 - x), quarter)].astype(jnp.float32)
                + first_b[k, rows(quarter * (1 - x), quarter)].astype(jnp.float32)
            ).astype(jnp.bfloat16)
            nexts[1].start()

        @pl.when(jnp.logical_and(t >= 2 * LAG, t < blocks + 2 * LAG))
        def _():
            k = t - 2 * LAG
            copies = sum_second(k)
            nexts = spread_first(k)
            for i, (part, first, second, hidden, major, minor) in enumerate(
                (
                    (part_a, first_a, second_a, hidden_a, x, y),
                    (part_b, first_b, second_b, hidden_b, y, x),
                )
            ):
                copies[i].wait_recv()
                mine = rows(half * major + quarter * minor, quarter)
                total = (
                    part[k, mine].astype(jnp.float32)
                    + first[k, rows(quarter * minor, quarter)].astype(jnp.float32)
                    + second[k].astype(jnp.float32)
                )
                gate, up = total[:, :width], total[:, width:]
                hidden[k, mine] = (gate * sigmoid(gate) * up).astype(jnp.bfloat16)
                nexts[i].start()

        @pl.when(jnp.logical_and(t >= 3 * LAG, t < blocks + 3 * LAG))
        def _():
            k = t - 3 * LAG
            for copy, follow in zip(spread_first(k), spread_second(k)):
                copy.wait_recv()
                follow.start()

        @pl.when(jnp.logical_and(t >= 4 * LAG, t < blocks + 4 * LAG))
        def _():
            k = t - 4 * LAG
            q = k // 2
            for copy in spread_second(k):
                copy.wait_recv()
            result = dot(hidden_a[k], down_w[:width, :], NN) + dot(hidden_b[k], down_w[width:, :], NN)

            @pl.when(k % 2 == 0)
            def _():
                own_res[q] = result

            @pl.when(k % 2 == 1)
            def _():
                pair_out[q] = result.astype(jnp.bfloat16)
                pair(q).start()

        last = t - 5 * LAG - 1

        @pl.when(jnp.logical_and(last >= 0, last % 2 == 0))
        def _():
            q = last // 2

            @pl.when(q == 2)
            def _():
                for turn in range(1, peers):
                    dispatch_aux(turn).wait_recv()
                    factors[turn] = as_columns(aux_in[turn])

            pair(q).wait_recv()
            columns = factors[turn_of(q), pl.ds(pl.multiple_of(half_of(q) * size, size), size), :]
            low, high = columns[:, 0:1], columns[:, 1:2]
            mine = jnp.where(core == 0, low, high)
            other = jnp.where(core == 0, high, low)
            both = (own_res[q] * mine + pair_in[q].astype(jnp.float32) * other).astype(jnp.bfloat16)

            @pl.when(q < 2)
            def _():
                back_in[back_rows(q), :] = both

            @pl.when(q >= 2)
            def _():
                back_out[q] = both
                give_back(q).start()

        return carry

    lax.fori_loop(0, blocks + 5 * LAG, step, 0)
    for q in range(2, units):
        give_back(q).wait_recv()
    total = midway_ref[...].astype(jnp.float32) + dot(select[...], back_in[...], NN)
    out_ref[...] = total.astype(jnp.bfloat16)

    for q in range(units):
        forward(q).wait_send()
        pair(q).wait_send()
        if q > 1:
            dispatch(q).wait_send()
            give_back(q).wait_send()
    for turn in range(1, peers):
        dispatch_aux(turn).wait_send()

    def drain(k, carry):
        for copies in (sum_first(k), sum_second(k), spread_first(k), spread_second(k)):
            for copy in copies:
                copy.wait_send()
        return carry

    lax.fori_loop(0, blocks, drain, 0)


def routed_experts(normed, midway, expert_ids, route_weight, expert_gate, expert_up, expert_down):
    tokens, features = normed.shape
    hidden = expert_gate.shape[2]
    half = hidden // 2
    slots = tokens // 2
    size = slots // 2
    quarter = size // 4
    peers = GROUPS
    units = 2 * peers
    blocks = 2 * units
    bf = jnp.bfloat16
    whole = pl.BlockSpec(memory_space=pltpu.VMEM)
    far = pl.BlockSpec(memory_space=pltpu.HBM)
    dma = pltpu.SemaphoreType.DMA
    return pl.pallas_call(
        expert_kernel,
        in_specs=[far] * 2 + [whole] * 2 + [far] * 3,
        out_specs=whole,
        out_shape=jax.ShapeDtypeStruct((tokens, features), bf),
        scratch_shapes=[
            pltpu.VMEM((tokens, features), bf),
            pltpu.VMEM((tokens, features), bf),
            pltpu.VMEM((features, hidden), bf),
            pltpu.VMEM((features, hidden), bf),
            pltpu.VMEM((hidden, features), bf),
            pltpu.VMEM((tokens, peers * slots), bf),
            pltpu.VMEM((units, size, features), bf),
            pltpu.VMEM((peers, slots, slots), jnp.float32),
            pltpu.VMEM((peers, 8, slots), jnp.float32),
            pltpu.VMEM((peers, 8, slots), jnp.float32),
            pltpu.VMEM((blocks, size, features), bf),
            pltpu.VMEM((blocks, size, hidden), bf),
            pltpu.VMEM((blocks, size, hidden), bf),
            pltpu.VMEM((blocks, size // 2, hidden), bf),
            pltpu.VMEM((blocks, size // 2, hidden), bf),
            pltpu.VMEM((blocks, quarter, hidden), bf),
            pltpu.VMEM((blocks, quarter, hidden), bf),
            pltpu.VMEM((blocks, quarter, hidden), bf),
            pltpu.VMEM((blocks, quarter, hidden), bf),
            pltpu.VMEM((blocks, size, half), bf),
            pltpu.VMEM((blocks, size, half), bf),
            pltpu.VMEM((units, size, features), jnp.float32),
            pltpu.VMEM((units, size, features), bf),
            pltpu.VMEM((units, size, features), bf),
            pltpu.VMEM((units, size, features), bf),
            pltpu.VMEM((peers * slots, features), bf),
            dma((5,)),
            dma((units,)),
            dma((units,)),
            dma((peers,)),
            dma((peers,)),
            dma((units,)),
            dma((units,)),
            dma((8, blocks)),
            dma((8, blocks)),
            dma((units,)),
            dma((units,)),
            dma((units,)),
            dma((units,)),
        ],
        compiler_params=pltpu.CompilerParams(
            collective_id=4, has_side_effects=True, vmem_limit_bytes=66_900_000
        ),
        name="experts",
    )(normed, midway, expert_ids.T, route_weight.T, expert_gate, expert_up, expert_down)


def local(
    receptance,
    key_vectors,
    value_vectors,
    decay_logits,
    rate_logits,
    gate_logits,
    group_gain,
    residual,
    mixer_out,
    norm_gain,
    expert_ids,
    route_weight,
    expert_gate,
    expert_up,
    expert_down,
):
    paired_cores = lax.axis_size("sp") == 2 * GROUPS and lax.axis_size("tp") == 4
    if paired_cores and expert_gate.shape[0] == 1:
        normed, midway = mixed_tokens(
            receptance, key_vectors, value_vectors, decay_logits, rate_logits, gate_logits,
            group_gain, residual, mixer_out, norm_gain,
        )
        return routed_experts(
            normed, midway, expert_ids, route_weight, expert_gate, expert_up, expert_down
        )
    mixed_rows = time_mix(
        receptance, key_vectors, value_vectors, decay_logits, rate_logits, gate_logits, group_gain
    )
    tokens_here, features = residual.shape
    projected = jnp.dot(
        gather_columns(mixed_rows, "tp", 0),
        mixer_out,
        preferred_element_type=jnp.float32,
    )
    midway = (residual.astype(jnp.float32) + projected).astype(jnp.bfloat16)
    midway_f = midway.astype(jnp.float32)
    squares = lax.psum(jnp.sum(midway_f * midway_f, axis=1), "tp")
    inv_rms = lax.rsqrt(squares / D + EPS_NORM)
    normed = (midway_f * norm_gain[None, :] * inv_rms[:, None]).astype(jnp.bfloat16)
    routes = expert_ids.shape[1]
    experts_all = lax.axis_size("sp") * expert_gate.shape[0]
    capacity = 2 * tokens_here * routes // experts_all
    flat_ids = expert_ids.reshape(-1)
    onehot = (flat_ids[:, None] == jnp.arange(experts_all, dtype=jnp.int32)[None, :]).astype(
        jnp.int32
    )
    earlier_count = jnp.sum((jnp.cumsum(onehot, axis=0) - onehot) * onehot, axis=1)
    slot_of = flat_ids * capacity + earlier_count
    owner_token = jnp.arange(tokens_here * routes, dtype=jnp.int32) // routes
    slot_table = (
        jnp.full((experts_all * capacity,), tokens_here, jnp.int32).at[slot_of].set(owner_token)
    )
    padded = jnp.concatenate([normed, jnp.zeros((1, features), jnp.bfloat16)], axis=0)
    outgoing = padded[slot_table].reshape(experts_all, capacity, features)
    arrived = swap_blocks(outgoing, "sp", 2)
    arrived_rows = arrived.reshape(-1, features)
    paired = jnp.concatenate([expert_gate[0], expert_up[0]], axis=1)
    gate_up = lax.psum_scatter(
        jnp.dot(arrived_rows, paired, preferred_element_type=jnp.float32).astype(jnp.bfloat16),
        "tp",
        scatter_dimension=0,
        tiled=True,
    ).astype(jnp.float32)
    half_width = paired.shape[1] // 2
    hidden = (jax.nn.silu(gate_up[:, :half_width]) * gate_up[:, half_width:]).astype(jnp.bfloat16)
    expert_res = jnp.dot(
        gather_rows(hidden, "tp", 1),
        expert_down[0],
        preferred_element_type=jnp.float32,
    )
    returned = swap_blocks(
        expert_res.astype(jnp.bfloat16).reshape(-1, capacity, features), "sp", 3
    )
    picked = (
        returned.reshape(-1, features)[slot_of]
        .astype(jnp.float32)
        .reshape(tokens_here, routes, features)
    )
    routed_sum = jnp.sum(picked * route_weight[:, :, None], axis=1)
    return (midway_f + routed_sum).astype(jnp.bfloat16)


def solution(mesh):
    placed = (
        P("sp", "tp"),
        P("sp", "tp"),
        P("sp", "tp"),
        P("sp", "tp"),
        P("sp", "tp"),
        P("sp", "tp"),
        P("tp"),
        P("sp", "tp"),
        P(None, "tp"),
        P("tp"),
        P("sp", None),
        P("sp", None),
        P("sp", "tp", None),
        P("sp", "tp", None),
        P("sp", None, "tp"),
    )
    return jax.shard_map(
        local, mesh=mesh, in_specs=placed, out_specs=P("sp", "tp"), check_vma=False
    )
```

```python
import jax
import jax.numpy as jnp
from jax import lax
from jax.experimental import pallas as pl
from jax.experimental.pallas import tpu as pltpu
from jax.sharding import PartitionSpec as P

D = 4096
HEAD = 64
CHUNK = 128
EXP_HALF = 0.6065306597126334


EPS_GROUP = 0.00064
EPS_NORM = 1e-06


def split(x):
    hi = x.astype(jnp.bfloat16)
    lo = (x - hi.astype(jnp.float32)).astype(jnp.bfloat16)
    return hi, lo


def dot(a, b, dims):
    return lax.dot_general(a, b, (dims, ((), ())), preferred_element_type=jnp.float32)


NN = ((1,), (0,))
NT = ((1,), (1,))
TN = ((0,), (0,))


def dot3(a, b, dims=NN):
    return dot(a[0], b[0], dims) + (dot(a[0], b[1], dims) + dot(a[1], b[0], dims))


def dot2(a, b, dims=NN):
    return dot(a[0], b, dims) + dot(a[1], b, dims)


def sigmoid(x):
    return 1.0 / (1.0 + jnp.exp(-x))


def mix_kernel(r_ref, k_ref, v_ref, d_ref, a_ref, out_ref, state_ref):
    tokens = r_ref.shape[0]
    chunks = tokens // CHUNK
    row = lax.broadcasted_iota(jnp.int32, (CHUNK, CHUNK), 0)
    col = lax.broadcasted_iota(jnp.int32, (CHUNK, CHUNK), 1)
    strict = col < row
    causal = col <= row
    eye = jnp.where(col == row, 1.0, 0.0)
    ones_lower = jnp.where(causal, 1.0, 0.0).astype(jnp.bfloat16)
    low = lax.broadcasted_iota(jnp.int32, (CHUNK, 2 * HEAD), 1) < HEAD

    work = []
    for chunk in range(chunks):
        rows = pl.ds(chunk * CHUNK, CHUNK)
        recept = r_ref[rows, :].astype(jnp.float32)
        keyvec = k_ref[rows, :].astype(jnp.float32)
        logdec = -EXP_HALF * sigmoid(d_ref[rows, :].astype(jnp.float32))
        first, second = split(logdec)
        third = (logdec - first.astype(jnp.float32) - second.astype(jnp.float32)).astype(jnp.bfloat16)
        cum_in = dot(ones_lower, first, NN) + (
            dot(ones_lower, second, NN) + dot(ones_lower, third, NN)
        )
        cum_end = cum_in[CHUNK - 1 :, :]
        squares = keyvec * keyvec
        norms = jnp.where(
            low,
            jnp.sum(squares[:, :HEAD], axis=1, keepdims=True),
            jnp.sum(squares[:, HEAD:], axis=1, keepdims=True),
        )
        unit_key = keyvec * lax.rsqrt(1.0 + norms)
        correction = unit_key * sigmoid(a_ref[rows, :].astype(jnp.float32))
        growth = jnp.exp(-cum_in)
        tail = jnp.exp(cum_end - cum_in)
        r_scaled = recept * jnp.exp(cum_in)
        u_scaled = unit_key * jnp.exp(cum_in - logdec)
        queries = split(jnp.concatenate([u_scaled, r_scaled], axis=0))
        sources = split(jnp.concatenate([keyvec * growth, correction * growth], axis=0))
        tails = split(jnp.concatenate([keyvec * tail, -(correction * tail)], axis=0))
        keep = jnp.broadcast_to(jnp.exp(cum_end), (2 * HEAD, 2 * HEAD)).T
        values = v_ref[rows, :]
        for head in range(2):
            lanes = slice(head * HEAD, (head + 1) * HEAD)
            query = tuple(q[:, lanes] for q in queries)
            source = tuple(s[:, lanes] for s in sources)
            scores = dot3(query, source, NT)
            work.append(
                dict(
                    head=head,
                    chunk=chunk,
                    query=query,
                    tail=tuple(t[:, lanes] for t in tails),
                    keep=keep[lanes, :],
                    value=jnp.concatenate(
                        [values[:, lanes], jnp.zeros((CHUNK, HEAD), jnp.bfloat16)], axis=1
                    ),
                    key_both=split(
                        jnp.concatenate(
                            [
                                jnp.where(strict, scores[:CHUNK, :CHUNK], 0.0),
                                jnp.where(causal, scores[CHUNK:, :CHUNK], 0.0),
                            ],
                            axis=0,
                        )
                    ),
                    pull=jnp.where(strict, scores[:CHUNK, CHUNK:], 0.0),
                    corr_read=split(jnp.where(causal, scores[CHUNK:, CHUNK:], 0.0)),
                )
            )
    for item in work:
        item["inverse"] = eye - jnp.where(row // 2 == col // 2, item["pull"], 0.0)
        item["from_values"] = dot2(item["key_both"], item["value"])
    size = 2
    while size < CHUNK:
        joined = (row // (2 * size) == col // (2 * size)) & (row // size != col // size)
        halves = []
        for item in work:
            inverse = split(item["inverse"])
            between = split(jnp.where(joined, item["pull"], 0.0))
            halves.append((inverse, dot3(between, inverse)))
        for item, (inverse, half) in zip(work, halves):
            item["inverse"] = item["inverse"] - dot3(inverse, split(half))
        size *= 2
    key_row = lax.broadcasted_iota(jnp.int32, (HEAD, 2 * HEAD), 0)
    lane = lax.broadcasted_iota(jnp.int32, (HEAD, 2 * HEAD), 1)
    start = jnp.where(lane == key_row + HEAD, 1.0, 0.0)
    states = [start, start]
    for item in work:
        head = item["head"]
        state = states[head]
        from_start = dot3(item["query"], split(state)) + item["from_values"]
        pulled = dot3(split(item["inverse"]), split(from_start[:CHUNK]))
        pulled_parts = split(pulled)
        out_ref[pl.ds(item["chunk"] * CHUNK, CHUNK), pl.ds(head * 2 * HEAD, 2 * HEAD)] = (
            from_start[CHUNK:] - dot3(item["corr_read"], pulled_parts)
        )
        key_tail = tuple(t[:CHUNK] for t in item["tail"])
        corr_tail = tuple(t[CHUNK:] for t in item["tail"])
        states[head] = (
            item["keep"] * state
            + dot2(key_tail, item["value"], TN)
            + dot3(corr_tail, pulled_parts, TN)
        )
    for head in range(2):
        state_ref[pl.ds(head * HEAD, HEAD), :] = states[head].astype(jnp.bfloat16)


def read_kernel(place_ref, read_ref, maps_ref, gate_ref, gain_ref, out_ref):
    def one(step, carried):
        following = []
        for head in range(2):
            both = maps_ref[step, pl.ds(head * HEAD, HEAD), :]
            parts = split(carried[head])
            step_map = both[:, HEAD:]
            following.append(
                both[:, :HEAD].astype(jnp.float32)
                + dot(step_map, parts[0], NN)
                + dot(step_map, parts[1], NN)
            )
        return tuple(following)

    zero = jnp.zeros((HEAD, HEAD), jnp.float32)
    incoming = lax.fori_loop(0, place_ref[0], one, (zero, zero))
    scaled = []
    for head in range(2):
        both = read_ref[:, pl.ds(head * 2 * HEAD, 2 * HEAD)]
        state_read = both[:, :HEAD] + dot3(split(both[:, HEAD:]), split(incoming[head]))
        centred = state_read - jnp.mean(state_read, axis=1, keepdims=True)
        variance = jnp.mean(centred * centred, axis=1, keepdims=True)
        scaled.append(centred * lax.rsqrt(variance + EPS_GROUP))
    gated = (
        jnp.concatenate(scaled, axis=1)
        * gain_ref[...]
        * sigmoid(gate_ref[...].astype(jnp.float32))
    )
    out_ref[...] = gated.astype(jnp.bfloat16)


def time_mix(
    receptance, key_vectors, value_vectors, decay_logits, rate_logits, gate_logits, group_gain
):
    tokens_here, channels = receptance.shape
    pairs = channels // (2 * HEAD)
    wide = pl.BlockSpec((tokens_here, 2 * HEAD), lambda i: (0, i))
    double = pl.BlockSpec((tokens_here, 4 * HEAD), lambda i: (0, i))
    reads, states = pl.pallas_call(
        mix_kernel,
        grid=(pairs,),
        in_specs=[wide] * 5,
        out_specs=[double, pl.BlockSpec((2 * HEAD, 2 * HEAD), lambda i: (i, 0))],
        out_shape=[
            jax.ShapeDtypeStruct((tokens_here, 2 * channels), jnp.float32),
            jax.ShapeDtypeStruct((channels, 2 * HEAD), jnp.bfloat16),
        ],
        name="mix",
    )(receptance, key_vectors, value_vectors, decay_logits, rate_logits)
    maps = lax.all_gather(states, "sp")
    place = lax.axis_index("sp").astype(jnp.int32).reshape(1)
    return pl.pallas_call(
        read_kernel,
        grid=(pairs,),
        in_specs=[
            pl.BlockSpec(memory_space=pltpu.SMEM),
            double,
            pl.BlockSpec((maps.shape[0], 2 * HEAD, 2 * HEAD), lambda i: (0, i, 0)),
            wide,
            pl.BlockSpec((1, 2 * HEAD), lambda i: (0, i)),
        ],
        out_specs=wide,
        out_shape=jax.ShapeDtypeStruct((tokens_here, channels), jnp.bfloat16),
        name="read",
    )(place, reads, maps, gate_logits, group_gain.reshape(1, channels))


def exchange(x, axis, shape, source, target, collective_id, name):
    def kernel(x_ref, out_ref, stage, send_sem, recv_sem, local_sem):
        n = lax.axis_size(axis)
        me = lax.axis_index(axis)
        peers = [lax.rem(me + step, n) for step in range(1, n)]
        barrier = pltpu.get_barrier_semaphore()
        for peer in peers:
            pl.semaphore_signal(
                barrier, inc=1, device_id={axis: peer}, device_id_type=pl.DeviceIdType.MESH
            )
        pl.semaphore_wait(barrier, n - 1)
        copies = []
        for step, peer in enumerate(peers):
            copy = pltpu.make_async_remote_copy(
                src_ref=source(x_ref, peer),
                dst_ref=target(out_ref, me),
                send_sem=send_sem.at[step],
                recv_sem=recv_sem.at[step],
                device_id={axis: peer},
                device_id_type=pl.DeviceIdType.MESH,
            )
            copy.start()
            copies.append(copy)
        own = pltpu.make_async_copy(source(x_ref, me), stage, local_sem)
        own.start()
        own.wait()
        own = pltpu.make_async_copy(stage, target(out_ref, me), local_sem)
        own.start()
        own.wait()
        for copy in copies:
            copy.wait()

    n = lax.axis_size(axis)
    return pl.pallas_call(
        kernel,
        in_specs=[pl.BlockSpec(memory_space=pl.ANY)],
        out_specs=pl.BlockSpec(memory_space=pl.ANY),
        out_shape=jax.ShapeDtypeStruct(shape, x.dtype),
        scratch_shapes=[
            pltpu.VMEM(x.shape[-2:], x.dtype),
            pltpu.SemaphoreType.DMA((n - 1,)),
            pltpu.SemaphoreType.DMA((n - 1,)),
            pltpu.SemaphoreType.DMA,
        ],
        compiler_params=pltpu.CompilerParams(collective_id=collective_id, has_side_effects=True),
        name=name,
    )(x)


def gather_columns(x, axis, collective_id):
    rows, columns = x.shape
    return exchange(
        x,
        axis,
        (rows, lax.axis_size(axis) * columns),
        lambda ref, peer: ref,
        lambda ref, me: ref.at[:, pl.ds(pl.multiple_of(me * columns, columns), columns)],
        collective_id,
        "gather_columns",
    )


def gather_rows(x, axis, collective_id):
    rows, columns = x.shape
    return exchange(
        x,
        axis,
        (lax.axis_size(axis) * rows, columns),
        lambda ref, peer: ref,
        lambda ref, me: ref.at[pl.ds(pl.multiple_of(me * rows, rows), rows), :],
        collective_id,
        "gather_rows",
    )


def swap_blocks(x, axis, collective_id):
    return exchange(
        x, axis, x.shape, lambda ref, peer: ref.at[peer], lambda ref, me: ref.at[me],
        collective_id, "swap_blocks",
    )


MESH = pl.DeviceIdType.MESH
GROUPS = 4


def pack_left(a):
    hi, lo = split(a)
    return jnp.concatenate([hi, lo], axis=1)


def pack_right(b):
    both = jnp.concatenate(split(b), axis=1)
    return jnp.concatenate([both, both], axis=0)


def dot_packed(left, right):
    out = dot(left, right, NN)
    n = out.shape[1] // 2
    return out[:, :n] + out[:, n:]


def three(a, axis, second):
    hi, lo = split(a)
    return jnp.concatenate([hi, hi, lo] if second else [hi, lo, hi], axis=axis)


def lower_rows(a, size):
    starts = range(size, a.shape[0], 2 * size)
    return jnp.concatenate([a[at : at + size] for at in starts], axis=0)


def join_rows(a, lower, size):
    parts = []
    for i, at in enumerate(range(0, a.shape[0], 2 * size)):
        parts += [a[at : at + size], lower[i * size : (i + 1) * size]]
    return jnp.concatenate(parts, axis=0)


def spread_rows(lower, size):
    parts = []
    for at in range(0, lower.shape[0], size):
        parts += [jnp.zeros((size, lower.shape[1]), lower.dtype), lower[at : at + size]]
    return jnp.concatenate(parts, axis=0)


def mix_heads(recept_in, key_in, values_in, decay_in, rate_in, write_read, write_state):
    tokens, width = recept_in.shape
    chunks = tokens // CHUNK
    pairs = width // (2 * HEAD)
    row = lax.broadcasted_iota(jnp.int32, (CHUNK, CHUNK), 0)
    col = lax.broadcasted_iota(jnp.int32, (CHUNK, CHUNK), 1)
    strict = col < row
    causal = col <= row
    eye = jnp.where(col == row, 1.0, 0.0)
    ones_lower = jnp.where(causal, 1.0, 0.0).astype(jnp.bfloat16)
    ones_twice = jnp.concatenate([ones_lower, ones_lower], axis=1)
    low = lax.broadcasted_iota(jnp.int32, (CHUNK, 2 * HEAD), 1) < HEAD
    nothing = jnp.zeros((CHUNK, 2 * HEAD), jnp.bfloat16)

    work = []
    for chunk in range(chunks):
        rows = slice(chunk * CHUNK, (chunk + 1) * CHUNK)
        for pair in range(pairs):
            lanes = slice(pair * 2 * HEAD, (pair + 1) * 2 * HEAD)
            recept = recept_in[rows, lanes].astype(jnp.float32)
            keyvec = key_in[rows, lanes].astype(jnp.float32)
            values = values_in[rows, lanes]
            logdec = -EXP_HALF * sigmoid(decay_in[rows, lanes].astype(jnp.float32))
            first, second = split(logdec)
            third = (logdec - first.astype(jnp.float32) - second.astype(jnp.float32)).astype(
                jnp.bfloat16
            )
            cum_in = dot_packed(
                ones_twice,
                jnp.concatenate(
                    [
                        jnp.concatenate([first, third], axis=1),
                        jnp.concatenate([second, nothing], axis=1),
                    ],
                    axis=0,
                ),
            )
            cum_end = cum_in[CHUNK - 1 :, :]
            squares = keyvec * keyvec
            norms = jnp.where(
                low,
                jnp.sum(squares[:, :HEAD], axis=1, keepdims=True),
                jnp.sum(squares[:, HEAD:], axis=1, keepdims=True),
            )
            unit_key = keyvec * lax.rsqrt(1.0 + norms)
            correction = unit_key * sigmoid(rate_in[rows, lanes].astype(jnp.float32))
            growth = jnp.exp(-cum_in)
            tail = jnp.exp(cum_end - cum_in)
            r_scaled = recept * jnp.exp(cum_in)
            u_scaled = unit_key * jnp.exp(cum_in - logdec)
            queries = jnp.concatenate([u_scaled, r_scaled], axis=0)
            sources = jnp.concatenate([keyvec * growth, correction * growth], axis=0)
            tails = jnp.concatenate([(keyvec * tail).T, -(correction * tail).T], axis=1)
            tail_hi, tail_lo = split(tails)
            keep = jnp.broadcast_to(jnp.exp(cum_end), (2 * HEAD, 2 * HEAD)).T
            for head in range(2):
                part = slice(head * HEAD, (head + 1) * HEAD)
                query = three(queries[:, part], 1, False)
                scores = dot(query, three(sources[:, part], 1, True), NT)
                value = jnp.concatenate(
                    [values[:, part], jnp.zeros((CHUNK, HEAD), jnp.bfloat16)], axis=1
                )
                work.append(
                    dict(
                        head=2 * pair + head,
                        chunk=chunk,
                        query=query,
                        tail=jnp.concatenate([tail_hi[part, :], tail_lo[part, :]], axis=0),
                        keep=keep[part, :],
                        value=value,
                        key_both=pack_left(
                            jnp.concatenate(
                                [
                                    jnp.where(strict, scores[:CHUNK, :CHUNK], 0.0),
                                    jnp.where(causal, scores[CHUNK:, :CHUNK], 0.0),
                                ],
                                axis=0,
                            )
                        ),
                        pull=jnp.where(strict, scores[:CHUNK, CHUNK:], 0.0),
                        corr_read=pack_left(jnp.where(causal, scores[CHUNK:, CHUNK:], 0.0)),
                    )
                )
    for item in work:
        item["inverse"] = eye - jnp.where(row // 2 == col // 2, item["pull"], 0.0)
        value = item["value"]
        item["from_values"] = dot(
            item["key_both"], jnp.concatenate([value, value], axis=0), NN
        )
    size = 2
    while size < CHUNK:
        joined = (row // (2 * size) == col // (2 * size)) & (row // size != col // size)
        halves = []
        if size < 8:
            for item in work:
                between = pack_left(jnp.where(joined, item["pull"], 0.0))
                halves.append(dot_packed(between, pack_right(item["inverse"])))
            for item, half in zip(work, halves):
                item["inverse"] = item["inverse"] - dot_packed(
                    pack_left(item["inverse"]), pack_right(half)
                )
        else:
            for item in work:
                between = pack_left(lower_rows(jnp.where(joined, item["pull"], 0.0), size))
                halves.append(dot_packed(between, pack_right(item["inverse"])))
            for item, half in zip(work, halves):
                inverse = item["inverse"]
                below = lower_rows(inverse, size)
                update = dot_packed(pack_left(below), pack_right(spread_rows(half, size)))
                item["inverse"] = join_rows(inverse, below - update, size)
        size *= 2
    key_row = lax.broadcasted_iota(jnp.int32, (HEAD, 2 * HEAD), 0)
    lane = lax.broadcasted_iota(jnp.int32, (HEAD, 2 * HEAD), 1)
    start = jnp.where(lane == key_row + HEAD, 1.0, 0.0)
    states = [start] * (2 * pairs)
    for chunk in range(chunks):
        items = [item for item in work if item["chunk"] == chunk]
        froms = [
            dot(item["query"], three(states[item["head"]], 0, True), NN) + item["from_values"]
            for item in items
        ]
        pulls = [
            dot_packed(pack_left(item["inverse"]), pack_right(value[:CHUNK]))
            for item, value in zip(items, froms)
        ]
        for item, value, pulled in zip(items, froms, pulls):
            head = item["head"]
            write_read(
                chunk, head, value[CHUNK:] - dot_packed(item["corr_read"], pack_right(pulled))
            )
            hi, lo = split(pulled)
            right = jnp.concatenate(
                [
                    jnp.concatenate([item["value"], hi], axis=0),
                    jnp.concatenate([nothing, lo], axis=0),
                ],
                axis=1,
            )
            out = dot(item["tail"], right, NN)
            states[head] = (
                item["keep"] * states[head]
                + (out[:HEAD, : 2 * HEAD] + out[HEAD:, : 2 * HEAD])
                + out[:HEAD, 2 * HEAD :]
            )
    for head in range(2 * pairs):
        write_state(head, states[head].astype(jnp.bfloat16))


def mixer_kernel(
    r_ref,
    k_ref,
    v_ref,
    d_ref,
    a_ref,
    gate_ref,
    gain_ref,
    residual_ref,
    norm_ref,
    mixer_hbm,
    normed_ref,
    midway_ref,
    mixer_w,
    reads,
    maps_own,
    maps_in,
    joint,
    joint_in,
    carry_out,
    carry_in,
    carried,
    gathered,
    acc,
    sums,
    load_sem,
    swap_send,
    swap_recv,
    chain_send,
    chain_recv,
    joint_send,
    joint_recv,
    gather_send,
    gather_recv,
    sum_send,
    sum_recv,
):
    tokens, features = residual_ref.shape
    steps, _, wide = reads.shape
    width = wide // 2
    heads = width // HEAD
    tps = lax.axis_size("tp")
    chips = lax.axis_size("sp") // 2
    sp = lax.axis_index("sp")
    tp = lax.axis_index("tp")
    z, core = sp // 2, sp % 2
    partner = {"sp": z * 2 + (1 - core)}
    y, x = tp // 2, tp % 2
    x_peer = y * 2 + (1 - x)
    y_peer = (1 - y) * 2 + x
    peers = [{"tp": x_peer}, {"tp": y_peer}, {"tp": (1 - y) * 2 + (1 - x)}]

    def load(step, block):
        return pltpu.make_async_copy(
            mixer_hbm.at[pl.ds(pl.multiple_of(block * steps * width + step * width, width), width), :],
            mixer_w.at[step, pl.ds(block * width, width), :],
            load_sem.at[step, block],
        )

    def load_all(step, carry):
        for block in range(tps):
            load(step, block).start()
        return carry

    lax.fori_loop(0, steps, load_all, 0)

    barrier = pltpu.get_barrier_semaphore()
    friends = [partner] + peers
    friends += [{"sp": ((z + shift) % chips) * 2 + core} for shift in range(1, chips)]
    for friend in friends:
        pl.semaphore_signal(barrier, inc=1, device_id=friend, device_id_type=MESH)
    acc[...] = residual_ref[...].astype(jnp.float32)
    pl.semaphore_wait(barrier, len(friends))

    def remote(source, target, send, recv, device):
        return pltpu.make_async_remote_copy(
            src_ref=source, dst_ref=target, send_sem=send, recv_sem=recv,
            device_id=device, device_id_type=MESH,
        )

    def swap(j):
        return remote(maps_own.at[j], maps_in.at[j], swap_send.at[j], swap_recv.at[j], partner)

    def chain(j, hop, target):
        return remote(
            carry_out.at[j], carry_in.at[j], chain_send.at[hop, j], chain_recv.at[j],
            {"sp": target * 2 + core},
        )

    def hand_joint(j):
        return remote(
            joint.at[j], joint_in.at[j], joint_send.at[j], joint_recv.at[j],
            {"sp": (chips - 1) * 2 + core},
        )

    def columns(owner):
        return pl.ds(pl.multiple_of(owner * width, width), width)

    def gather(j):
        own = gathered.at[j, :, columns(tp)]
        return [
            remote(own, own, gather_send.at[i, j], gather_recv.at[i, j], peers[i]) for i in range(2)
        ]

    def relay(j):
        low = gathered.at[j, pl.ds(0, tokens // 2), columns(x_peer)]
        high = gathered.at[j, pl.ds(tokens // 2, tokens // 2), columns(y_peer)]
        return [
            remote(low, low, gather_send.at[2, j], gather_recv.at[2, j], peers[1]),
            remote(high, high, gather_send.at[3, j], gather_recv.at[3, j], peers[0]),
        ]

    def mix(i):
        lanes = pl.ds(pl.multiple_of(i * width, width), width)

        def write_read(chunk, head, value):
            reads[i, pl.ds(chunk * CHUNK, CHUNK), pl.ds(head * 2 * HEAD, 2 * HEAD)] = value

        def write_state(head, value):
            maps_own[i, pl.ds(head * HEAD, HEAD), :] = value

        mix_heads(
            r_ref[:, lanes], k_ref[:, lanes], v_ref[:, lanes], d_ref[:, lanes], a_ref[:, lanes],
            write_read, write_state,
        )
        swap(i).start()

    half_lane = lax.broadcasted_iota(jnp.int32, (HEAD, 2 * HEAD), 1) < HEAD

    def join(j):
        swap(j).wait_recv()
        for head in range(heads):
            part = pl.ds(head * HEAD, HEAD)
            own, other = maps_own[j, part, :], maps_in[j, part, :]
            first = jnp.where(core == 0, own, other)
            second = jnp.where(core == 0, other, own)
            both = dot(second[:, HEAD:], first, NN)
            joint[j, part, :] = both + jnp.where(half_lane, second.astype(jnp.float32), 0.0)

        @pl.when(z == 0)
        def _():
            carry_out[j] = jnp.concatenate(
                [joint[j, pl.ds(head * HEAD, HEAD), :][:, :HEAD] for head in range(heads)], axis=1
            ).astype(jnp.bfloat16)
            carried[j] = jnp.zeros((HEAD, width), jnp.bfloat16)
            chain(j, 0, 1).start()

        @pl.when(z == 2)
        def _():
            hand_joint(j).start()

    def advance(maps, j):
        following = []
        for head in range(heads):
            both = maps[j, pl.ds(head * HEAD, HEAD), :]
            value = carry_in[j, :, pl.ds(head * HEAD, HEAD)]
            following.append(both[:, :HEAD] + dot2(split(both[:, HEAD:]), value))
        return jnp.concatenate(following, axis=1).astype(jnp.bfloat16)

    def hop(j):
        chain(j, 0, 1).wait_recv()
        carried[j] = carry_in[j]
        carry_out[j] = advance(joint, j)
        chain(j, 0, 2).start()
        chain(j, 1, 3).start()

    def finish(j):
        @pl.when(z >= 2)
        def _():
            chain(j, 0, 1).wait_recv()

        @pl.when(z == 2)
        def _():
            carried[j] = carry_in[j]

        @pl.when(z == 3)
        def _():
            hand_joint(j).wait_recv()
            carried[j] = advance(joint_in, j)

        nothing = jnp.zeros((HEAD, HEAD), jnp.bfloat16)
        unit = jnp.where(
            lax.broadcasted_iota(jnp.int32, (HEAD, HEAD), 0)
            == lax.broadcasted_iota(jnp.int32, (HEAD, HEAD), 1),
            1.0,
            0.0,
        ).astype(jnp.bfloat16)
        state_parts = []
        for head in range(heads):
            value = carried[j, :, pl.ds(head * HEAD, HEAD)]
            other = maps_in[j, pl.ds(head * HEAD, HEAD), :]
            passed = other[:, :HEAD].astype(jnp.float32) + dot(other[:, HEAD:], value, NN)
            state_parts.append(split(jnp.where(core == 0, value.astype(jnp.float32), passed)))
        head_of = [
            lax.broadcasted_iota(jnp.int32, (4 * HEAD, 2 * HEAD), axis) // HEAD % 2
            for axis in range(2)
        ]
        average = jnp.where(head_of[0] == head_of[1], 1.0 / HEAD, 0.0).astype(jnp.bfloat16)
        for pair in range(heads // 2):
            here = [reads[j, :, pl.ds((2 * pair + i) * 2 * HEAD, 2 * HEAD)] for i in range(2)]
            hi, lo = split(jnp.concatenate(here, axis=1))
            (first_hi, first_lo), (second_hi, second_lo) = state_parts[2 * pair : 2 * pair + 2]
            wide_rows = [
                [unit, nothing, nothing, nothing],
                [first_hi, nothing, first_lo, nothing],
                [nothing, unit, nothing, nothing],
                [nothing, second_hi, nothing, second_lo],
            ]
            right = jnp.concatenate(
                [jnp.concatenate(blocks, axis=1) for blocks in wide_rows], axis=0
            )
            state_read = dot_packed(hi, right) + dot(lo, right[:, : 2 * HEAD], NN)
            centred = state_read - dot(pack_left(state_read), average, NN)
            variance = dot(pack_left(centred * centred), average, NN)
            lanes = pl.ds(pl.multiple_of(j * width + pair * 2 * HEAD, 2 * HEAD), 2 * HEAD)
            gated = (
                centred
                * lax.rsqrt(variance + EPS_GROUP)
                * gain_ref[:, lanes]
                * sigmoid(gate_ref[:, lanes].astype(jnp.float32))
            )
            own_lanes = pl.ds(pl.multiple_of(tp * width + pair * 2 * HEAD, 2 * HEAD), 2 * HEAD)
            gathered[j, :, own_lanes] = gated.astype(jnp.bfloat16)
        for copy in gather(j):
            copy.start()

    def pass_on(j):
        for copy, after in zip(gather(j), relay(j)):
            copy.wait_recv()
            after.start()

    def project(j):
        for block in range(tps):
            load(j, block).wait()
        for copy in relay(j):
            copy.wait_recv()
        acc[...] += dot(gathered[j], mixer_w[j], NN)

    def within(j):
        return jnp.logical_and(j >= 0, j < steps)

    def step(t, carry):
        @pl.when(jnp.logical_and(z == 1, within(t - 2)))
        def _():
            hop(t - 2)

        @pl.when(within(t))
        def _():
            mix(t)

        @pl.when(within(t - 1))
        def _():
            join(t - 1)

        @pl.when(jnp.logical_and(z == 0, within(t - 1)))
        def _():
            finish(t - 1)

        @pl.when(jnp.logical_and(z > 0, within(t - 2)))
        def _():
            finish(t - 2)

        @pl.when(within(t - 3))
        def _():
            pass_on(t - 3)

        @pl.when(within(t - 4))
        def _():
            project(t - 4)

        return carry

    lax.fori_loop(0, steps + 4, step, 0)

    midway = acc[...].astype(jnp.bfloat16)
    midway_ref[...] = midway
    midway_f = midway.astype(jnp.float32)
    squares = jnp.sum(midway_f * midway_f, axis=1, keepdims=True)
    sums[0] = jnp.broadcast_to(squares, (tokens, 128)).T[:8, :]
    copies = [
        remote(sums.at[0], sums.at[i + 1], sum_send.at[i], sum_recv.at[i], peer)
        for i, peer in enumerate(peers)
    ]
    for copy in copies:
        copy.start()
    scaled = midway_f * norm_ref[...]
    for copy in copies:
        copy.wait_recv()
    total = sums[0]
    for i in range(1, tps):
        total = total + sums[i]
    total = jnp.concatenate([total] * (128 // 8), axis=0).T[:, :1]
    normed_ref[...] = (scaled * lax.rsqrt(total / D + EPS_NORM)).astype(jnp.bfloat16)

    for copy in copies:
        copy.wait_send()

    def drain(j, carry):
        swap(j).wait_send()

        @pl.when(z < 2)
        def _():
            chain(j, 0, 1).wait_send()

        @pl.when(z == 1)
        def _():
            chain(j, 1, 1).wait_send()

        @pl.when(z == 2)
        def _():
            hand_joint(j).wait_send()

        for copy in gather(j) + relay(j):
            copy.wait_send()
        return carry

    lax.fori_loop(0, steps, drain, 0)


HEADS_PER_STEP = 4


def mixed_tokens(
    receptance, key_vectors, value_vectors, decay_logits, rate_logits, gate_logits, group_gain,
    residual, mixer_out, norm_gain,
):
    tokens, channels = receptance.shape
    features = residual.shape[1]
    tps = lax.axis_size("tp")
    width = HEADS_PER_STEP * HEAD
    steps = channels // width
    bf = jnp.bfloat16
    f32 = jnp.float32
    whole = pl.BlockSpec(memory_space=pltpu.VMEM)
    dma = pltpu.SemaphoreType.DMA
    return pl.pallas_call(
        mixer_kernel,
        in_specs=[whole] * 9 + [pl.BlockSpec(memory_space=pl.ANY)],
        out_specs=[whole, whole],
        out_shape=[jax.ShapeDtypeStruct((tokens, features), bf)] * 2,
        scratch_shapes=[
            pltpu.VMEM((steps, tps * width, features), bf),
            pltpu.VMEM((steps, tokens, 2 * width), f32),
            pltpu.VMEM((steps, width, 2 * HEAD), bf),
            pltpu.VMEM((steps, width, 2 * HEAD), bf),
            pltpu.VMEM((steps, width, 2 * HEAD), f32),
            pltpu.VMEM((steps, width, 2 * HEAD), f32),
            pltpu.VMEM((steps, HEAD, width), bf),
            pltpu.VMEM((steps, HEAD, width), bf),
            pltpu.VMEM((steps, HEAD, width), bf),
            pltpu.VMEM((steps, tokens, tps * width), bf),
            pltpu.VMEM((tokens, features), f32),
            pltpu.VMEM((tps, 8, tokens), f32),
            dma((steps, tps)),
            dma((steps,)),
            dma((steps,)),
            dma((2, steps)),
            dma((steps,)),
            dma((steps,)),
            dma((steps,)),
            dma((4, steps)),
            dma((4, steps)),
            dma((tps - 1,)),
            dma((tps - 1,)),
        ],
        compiler_params=pltpu.CompilerParams(
            collective_id=5, has_side_effects=True, vmem_limit_bytes=56 * 1024 * 1024
        ),
        name="mixer",
    )(
        receptance, key_vectors, value_vectors, decay_logits, rate_logits, gate_logits,
        group_gain.reshape(1, channels), residual, norm_gain.reshape(1, features), mixer_out,
    )


LAG = 1
LEAD = 1


def expert_kernel(
    normed_hbm,
    midway_hbm,
    ids_ref,
    weight_ref,
    gate_hbm,
    up_hbm,
    down_hbm,
    out_ref,
    normed_ref,
    midway_ref,
    gate_w,
    up_w,
    down_w,
    select,
    outgoing,
    factors,
    aux_out,
    aux_in,
    rows_in,
    part_a,
    part_b,
    first_a,
    first_b,
    pass_a,
    pass_b,
    second_a,
    second_b,
    hidden_a,
    hidden_b,
    own_res,
    pair_out,
    pair_in,
    back_out,
    back_in,
    load_sem,
    disp_send,
    disp_recv,
    aux_send,
    aux_recv,
    fwd_send,
    fwd_recv,
    tp_send,
    tp_recv,
    pair_send,
    pair_recv,
    back_send,
    back_recv,
):
    tokens = normed_ref.shape[0]
    size = outgoing.shape[1]
    slots = 2 * size
    quarter = size // 4
    half = size // 2
    width = hidden_a.shape[2]
    peers = GROUPS
    units = 2 * peers
    blocks = 2 * units
    sp = lax.axis_index("sp")
    tp = lax.axis_index("tp")
    z, core = sp // 2, sp % 2
    y, x = tp // 2, tp % 2
    x_peer = y * 2 + (1 - x)
    y_peer = (1 - y) * 2 + x

    def chip(turn):
        return 2 * ((z // 2 + turn // 2) % 2) + (z % 2 + turn % 2) % 2

    def turn_of(q):
        return (q + 6) // 8 + (q + 5) // 8 + (q + 3) // 8 - 2 * ((q + 1) // 8)

    def half_of(q):
        return (q + 7) // 8 - (q + 6) // 8 + (q + 4) // 8 - (q + 3) // 8 + (q + 2) // 8

    loads = [
        pltpu.make_async_copy(source.at[0], target, load_sem.at[i])
        for i, (source, target) in enumerate(((gate_hbm, gate_w), (up_hbm, up_w), (down_hbm, down_w)))
    ]
    load_rows = pltpu.make_async_copy(normed_hbm, normed_ref, load_sem.at[3])
    load_rows.start()
    loads.append(pltpu.make_async_copy(midway_hbm, midway_ref, load_sem.at[4]))
    for load in loads:
        load.start()

    partner = {"sp": z * 2 + (1 - core)}
    barrier = pltpu.get_barrier_semaphore()
    friends = [partner, {"tp": x_peer}, {"tp": y_peer}]
    friends += [{"sp": chip(turn) * 2 + core} for turn in range(1, peers)]
    for friend in friends:
        pl.semaphore_signal(barrier, inc=1, device_id=friend, device_id_type=MESH)

    def remote(source, target, send, recv, device):
        return pltpu.make_async_remote_copy(
            src_ref=source, dst_ref=target, send_sem=send, recv_sem=recv,
            device_id=device, device_id_type=MESH,
        )

    def dispatch(q):
        return remote(
            outgoing.at[q], rows_in.at[2 * q], disp_send.at[q], disp_recv.at[q],
            {"sp": chip(turn_of(q)) * 2 + core},
        )

    def dispatch_aux(turn):
        return remote(
            aux_out.at[turn], aux_in.at[turn], aux_send.at[turn], aux_recv.at[turn],
            {"sp": chip(turn) * 2 + core},
        )

    def forward(q):
        return remote(rows_in.at[2 * q], rows_in.at[2 * q + 1], fwd_send.at[q], fwd_recv.at[q], partner)

    def over_tp(kind, k, source, target, device):
        return remote(source, target, tp_send.at[kind, k], tp_recv.at[kind, k], {"tp": device})

    def rows(start, size):
        return pl.ds(pl.multiple_of(start, quarter), size)

    def sum_first(k):
        return (
            over_tp(0, k, part_a.at[k, rows(half * (1 - x), half)], first_a.at[k], x_peer),
            over_tp(1, k, part_b.at[k, rows(half * (1 - y), half)], first_b.at[k], y_peer),
        )

    def sum_second(k):
        return (
            over_tp(2, k, pass_a.at[k], second_a.at[k], y_peer),
            over_tp(3, k, pass_b.at[k], second_b.at[k], x_peer),
        )

    def spread_first(k):
        own_a = hidden_a.at[k, rows(half * x + quarter * y, quarter)]
        own_b = hidden_b.at[k, rows(half * y + quarter * x, quarter)]
        return (over_tp(4, k, own_a, own_a, y_peer), over_tp(5, k, own_b, own_b, x_peer))

    def spread_second(k):
        own_a = hidden_a.at[k, rows(half * x, half)]
        own_b = hidden_b.at[k, rows(half * y, half)]
        return (over_tp(6, k, own_a, own_a, x_peer), over_tp(7, k, own_b, own_b, y_peer))

    def pair(q):
        return remote(pair_out.at[q], pair_in.at[q], pair_send.at[q], pair_recv.at[q], partner)

    def back_rows(q):
        return pl.ds(pl.multiple_of(turn_of(q) * slots + half_of(q) * size, size), size)

    def give_back(q):
        return remote(
            back_out.at[q], back_in.at[back_rows(q), :], back_send.at[q], back_recv.at[q],
            {"sp": chip(turn_of(q)) * 2 + core},
        )

    def as_columns(few_rows):
        return jnp.concatenate([few_rows] * (slots // 8), axis=0).T

    def few_rows():
        few = jnp.concatenate(
            [ids_ref[...].astype(jnp.float32), weight_ref[...], jnp.zeros((4, tokens), jnp.float32)],
            axis=0,
        )
        return jnp.concatenate([few] * (128 // 8), axis=0).T

    ids = few_rows()[:, :2].astype(jnp.int32)
    lane = lax.broadcasted_iota(jnp.int32, (tokens, 128), 1)
    slot_lane = lax.broadcasted_iota(jnp.int32, (tokens, slots), 1).astype(jnp.float32)
    earlier = jnp.where(
        lax.broadcasted_iota(jnp.int32, (tokens, tokens), 1)
        < lax.broadcasted_iota(jnp.int32, (tokens, tokens), 0),
        1.0,
        0.0,
    ).astype(jnp.bfloat16)
    group_of = [chip(turn) for turn in range(peers)]
    member = [
        jnp.logical_and(ids[:, :1] >= 2 * group, ids[:, :1] < 2 * group + 2) for group in group_of
    ]
    members = jnp.zeros((tokens, 128), jnp.float32)
    for turn in range(peers):
        members = jnp.where(jnp.logical_and(lane == turn, member[turn]), 1.0, members)
    ranks = dot(earlier, members.astype(jnp.bfloat16), NN)
    load_rows.wait()
    normed = normed_ref[...]
    pl.semaphore_wait(barrier, len(friends))
    for turn in range(peers):
        chosen = jnp.where(
            jnp.logical_and(slot_lane == ranks[:, turn : turn + 1], member[turn]), 1.0, 0.0
        ).astype(jnp.bfloat16)
        select[:, turn * slots : (turn + 1) * slots] = chosen
        picked = dot(chosen, normed, TN).astype(jnp.bfloat16)
        for part in range(2):
            piece = picked[part * size : (part + 1) * size]
            if turn == 0:
                rows_in[2 * part] = piece
                forward(part).start()
            else:
                q = {(1, 0): 2, (2, 0): 3, (2, 1): 4, (3, 0): 5, (3, 1): 6, (1, 1): 7}[turn, part]
                outgoing[q] = piece
                if q < 7:
                    dispatch(q).start()
    dispatch(7).start()
    for load in loads:
        load.wait()

    def weigh():
        few = few_rows()
        lane_of = lax.broadcasted_iota(jnp.int32, (tokens, 128), 1)
        ids, weights = few[:, :2].astype(jnp.int32), few[:, 2:4]
        for turn in range(peers):
            parts = jnp.zeros((tokens, 128), jnp.float32)
            for expert in range(2):
                name = 2 * group_of[turn] + expert
                value = jnp.where(ids[:, :1] == name, weights[:, :1], 0.0) + jnp.where(
                    ids[:, 1:2] == name, weights[:, 1:2], 0.0
                )
                for piece in range(3):
                    term = value.astype(jnp.bfloat16).astype(jnp.float32)
                    parts = jnp.where(lane_of == 3 * expert + piece, term, parts)
                    value = value - term
            by_slot = dot(
                parts.astype(jnp.bfloat16), select[:, turn * slots : (turn + 1) * slots], TN
            )
            weight_rows = jnp.concatenate(
                [
                    by_slot[0:1] + by_slot[1:2] + by_slot[2:3],
                    by_slot[3:4] + by_slot[4:5] + by_slot[5:6],
                    jnp.zeros((6, slots), jnp.float32),
                ],
                axis=0,
            )
            if turn == 0:
                factors[0] = as_columns(weight_rows)
            else:
                aux_out[turn] = weight_rows
                dispatch_aux(turn).start()

    def step(t, carry):
        @pl.when(t == 1)
        def _():
            weigh()

        @pl.when(jnp.logical_and(t >= LEAD + LAG, t < blocks + LEAD + LAG))
        def _():
            k = t - LEAD - LAG
            copies = sum_first(k)
            nexts = sum_second(k)
            copies[0].wait_recv()
            pass_a[k] = (
                part_a[k, rows(half * x + quarter * (1 - y), quarter)].astype(jnp.float32)
                + first_a[k, rows(quarter * (1 - y), quarter)].astype(jnp.float32)
            ).astype(jnp.bfloat16)
            nexts[0].start()
            copies[1].wait_recv()
            pass_b[k] = (
                part_b[k, rows(half * y + quarter * (1 - x), quarter)].astype(jnp.float32)
                + first_b[k, rows(quarter * (1 - x), quarter)].astype(jnp.float32)
            ).astype(jnp.bfloat16)
            nexts[1].start()

        @pl.when(jnp.logical_and(t >= LEAD + 2 * LAG, t < blocks + LEAD + 2 * LAG))
        def _():
            k = t - LEAD - 2 * LAG
            copies = sum_second(k)
            nexts = spread_first(k)
            for i, (part, first, second, hidden, major, minor) in enumerate(
                (
                    (part_a, first_a, second_a, hidden_a, x, y),
                    (part_b, first_b, second_b, hidden_b, y, x),
                )
            ):
                copies[i].wait_recv()
                mine = rows(half * major + quarter * minor, quarter)
                total = (
                    part[k, mine].astype(jnp.float32)
                    + first[k, rows(quarter * minor, quarter)].astype(jnp.float32)
                    + second[k].astype(jnp.float32)
                )
                gate, up = total[:, :width], total[:, width:]
                hidden[k, mine] = (gate * sigmoid(gate) * up).astype(jnp.bfloat16)
                nexts[i].start()

        @pl.when(jnp.logical_and(t >= LEAD + 3 * LAG, t < blocks + LEAD + 3 * LAG))
        def _():
            k = t - LEAD - 3 * LAG
            for copy, follow in zip(spread_first(k), spread_second(k)):
                copy.wait_recv()
                follow.start()

        @pl.when(t < blocks)
        def _():
            k = t
            q = k // 2

            @pl.when(jnp.logical_and(k % 2 == 0, q > 1))
            def _():
                dispatch(q).wait_recv()
                forward(q).start()

            @pl.when(k % 2 == 1)
            def _():
                forward(q).wait_recv()

            block = rows_in[k]
            for part, columns in ((part_a, pl.ds(0, width)), (part_b, pl.ds(width, width))):
                part[k, :, :width] = dot(block, gate_w[:, columns], NN).astype(jnp.bfloat16)
                part[k, :, width:] = dot(block, up_w[:, columns], NN).astype(jnp.bfloat16)
            for copy in sum_first(k):
                copy.start()

        @pl.when(jnp.logical_and(t >= LEAD + 4 * LAG, t < blocks + LEAD + 4 * LAG))
        def _():
            k = t - LEAD - 4 * LAG
            q = k // 2
            for copy in spread_second(k):
                copy.wait_recv()
            result = dot(hidden_a[k], down_w[:width, :], NN) + dot(hidden_b[k], down_w[width:, :], NN)

            @pl.when(k % 2 == 0)
            def _():
                own_res[q] = result

            @pl.when(k % 2 == 1)
            def _():
                pair_out[q] = result.astype(jnp.bfloat16)
                pair(q).start()

        last = t - LEAD - 5 * LAG - 1

        @pl.when(jnp.logical_and(last >= 0, last % 2 == 0))
        def _():
            q = last // 2

            @pl.when(q == 2)
            def _():
                for turn in range(1, peers):
                    dispatch_aux(turn).wait_recv()
                    factors[turn] = as_columns(aux_in[turn])

            pair(q).wait_recv()
            columns = factors[turn_of(q), pl.ds(pl.multiple_of(half_of(q) * size, size), size), :]
            low, high = columns[:, 0:1], columns[:, 1:2]
            mine = jnp.where(core == 0, low, high)
            other = jnp.where(core == 0, high, low)
            both = (own_res[q] * mine + pair_in[q].astype(jnp.float32) * other).astype(jnp.bfloat16)

            @pl.when(q < 2)
            def _():
                back_in[back_rows(q), :] = both

            @pl.when(q >= 2)
            def _():
                back_out[q] = both
                give_back(q).start()

        return carry

    lax.fori_loop(0, blocks + LEAD + 5 * LAG, step, 0)
    for q in range(2, units):
        give_back(q).wait_recv()
    total = midway_ref[...].astype(jnp.float32) + dot(select[...], back_in[...], NN)
    out_ref[...] = total.astype(jnp.bfloat16)

    for q in range(units):
        forward(q).wait_send()
        pair(q).wait_send()
        if q > 1:
            dispatch(q).wait_send()
            give_back(q).wait_send()
    for turn in range(1, peers):
        dispatch_aux(turn).wait_send()

    def drain(k, carry):
        for copies in (sum_first(k), sum_second(k), spread_first(k), spread_second(k)):
            for copy in copies:
                copy.wait_send()
        return carry

    lax.fori_loop(0, blocks, drain, 0)


def routed_experts(normed, midway, expert_ids, route_weight, expert_gate, expert_up, expert_down):
    tokens, features = normed.shape
    hidden = expert_gate.shape[2]
    half = hidden // 2
    slots = tokens // 2
    size = slots // 2
    quarter = size // 4
    peers = GROUPS
    units = 2 * peers
    blocks = 2 * units
    bf = jnp.bfloat16
    whole = pl.BlockSpec(memory_space=pltpu.VMEM)
    far = pl.BlockSpec(memory_space=pltpu.HBM)
    dma = pltpu.SemaphoreType.DMA
    return pl.pallas_call(
        expert_kernel,
        in_specs=[far] * 2 + [whole] * 2 + [far] * 3,
        out_specs=whole,
        out_shape=jax.ShapeDtypeStruct((tokens, features), bf),
        scratch_shapes=[
            pltpu.VMEM((tokens, features), bf),
            pltpu.VMEM((tokens, features), bf),
            pltpu.VMEM((features, hidden), bf),
            pltpu.VMEM((features, hidden), bf),
            pltpu.VMEM((hidden, features), bf),
            pltpu.VMEM((tokens, peers * slots), bf),
            pltpu.VMEM((units, size, features), bf),
            pltpu.VMEM((peers, slots, slots), jnp.float32),
            pltpu.VMEM((peers, 8, slots), jnp.float32),
            pltpu.VMEM((peers, 8, slots), jnp.float32),
            pltpu.VMEM((blocks, size, features), bf),
            pltpu.VMEM((blocks, size, hidden), bf),
            pltpu.VMEM((blocks, size, hidden), bf),
            pltpu.VMEM((blocks, size // 2, hidden), bf),
            pltpu.VMEM((blocks, size // 2, hidden), bf),
            pltpu.VMEM((blocks, quarter, hidden), bf),
            pltpu.VMEM((blocks, quarter, hidden), bf),
            pltpu.VMEM((blocks, quarter, hidden), bf),
            pltpu.VMEM((blocks, quarter, hidden), bf),
            pltpu.VMEM((blocks, size, half), bf),
            pltpu.VMEM((blocks, size, half), bf),
            pltpu.VMEM((units, size, features), jnp.float32),
            pltpu.VMEM((units, size, features), bf),
            pltpu.VMEM((units, size, features), bf),
            pltpu.VMEM((units, size, features), bf),
            pltpu.VMEM((peers * slots, features), bf),
            dma((5,)),
            dma((units,)),
            dma((units,)),
            dma((peers,)),
            dma((peers,)),
            dma((units,)),
            dma((units,)),
            dma((8, blocks)),
            dma((8, blocks)),
            dma((units,)),
            dma((units,)),
            dma((units,)),
            dma((units,)),
        ],
        compiler_params=pltpu.CompilerParams(
            collective_id=4, has_side_effects=True, vmem_limit_bytes=66_900_000
        ),
        name="experts",
    )(normed, midway, expert_ids.T, route_weight.T, expert_gate, expert_up, expert_down)


def local(
    receptance,
    key_vectors,
    value_vectors,
    decay_logits,
    rate_logits,
    gate_logits,
    group_gain,
    residual,
    mixer_out,
    norm_gain,
    expert_ids,
    route_weight,
    expert_gate,
    expert_up,
    expert_down,
):
    paired_cores = lax.axis_size("sp") == 2 * GROUPS and lax.axis_size("tp") == 4
    if paired_cores and expert_gate.shape[0] == 1:
        normed, midway = mixed_tokens(
            receptance, key_vectors, value_vectors, decay_logits, rate_logits, gate_logits,
            group_gain, residual, mixer_out, norm_gain,
        )
        return routed_experts(
            normed, midway, expert_ids, route_weight, expert_gate, expert_up, expert_down
        )
    mixed_rows = time_mix(
        receptance, key_vectors, value_vectors, decay_logits, rate_logits, gate_logits, group_gain
    )
    tokens_here, features = residual.shape
    projected = jnp.dot(
        gather_columns(mixed_rows, "tp", 0),
        mixer_out,
        preferred_element_type=jnp.float32,
    )
    midway = (residual.astype(jnp.float32) + projected).astype(jnp.bfloat16)
    midway_f = midway.astype(jnp.float32)
    squares = lax.psum(jnp.sum(midway_f * midway_f, axis=1), "tp")
    inv_rms = lax.rsqrt(squares / D + EPS_NORM)
    normed = (midway_f * norm_gain[None, :] * inv_rms[:, None]).astype(jnp.bfloat16)
    routes = expert_ids.shape[1]
    experts_all = lax.axis_size("sp") * expert_gate.shape[0]
    capacity = 2 * tokens_here * routes // experts_all
    flat_ids = expert_ids.reshape(-1)
    onehot = (flat_ids[:, None] == jnp.arange(experts_all, dtype=jnp.int32)[None, :]).astype(
        jnp.int32
    )
    earlier_count = jnp.sum((jnp.cumsum(onehot, axis=0) - onehot) * onehot, axis=1)
    slot_of = flat_ids * capacity + earlier_count
    owner_token = jnp.arange(tokens_here * routes, dtype=jnp.int32) // routes
    slot_table = (
        jnp.full((experts_all * capacity,), tokens_here, jnp.int32).at[slot_of].set(owner_token)
    )
    padded = jnp.concatenate([normed, jnp.zeros((1, features), jnp.bfloat16)], axis=0)
    outgoing = padded[slot_table].reshape(experts_all, capacity, features)
    arrived = swap_blocks(outgoing, "sp", 2)
    arrived_rows = arrived.reshape(-1, features)
    paired = jnp.concatenate([expert_gate[0], expert_up[0]], axis=1)
    gate_up = lax.psum_scatter(
        jnp.dot(arrived_rows, paired, preferred_element_type=jnp.float32).astype(jnp.bfloat16),
        "tp",
        scatter_dimension=0,
        tiled=True,
    ).astype(jnp.float32)
    half_width = paired.shape[1] // 2
    hidden = (jax.nn.silu(gate_up[:, :half_width]) * gate_up[:, half_width:]).astype(jnp.bfloat16)
    expert_res = jnp.dot(
        gather_rows(hidden, "tp", 1),
        expert_down[0],
        preferred_element_type=jnp.float32,
    )
    returned = swap_blocks(
        expert_res.astype(jnp.bfloat16).reshape(-1, capacity, features), "sp", 3
    )
    picked = (
        returned.reshape(-1, features)[slot_of]
        .astype(jnp.float32)
        .reshape(tokens_here, routes, features)
    )
    routed_sum = jnp.sum(picked * route_weight[:, :, None], axis=1)
    return (midway_f + routed_sum).astype(jnp.bfloat16)


def solution(mesh):
    placed = (
        P("sp", "tp"),
        P("sp", "tp"),
        P("sp", "tp"),
        P("sp", "tp"),
        P("sp", "tp"),
        P("sp", "tp"),
        P("tp"),
        P("sp", "tp"),
        P(None, "tp"),
        P("tp"),
        P("sp", None),
        P("sp", None),
        P("sp", "tp", None),
        P("sp", "tp", None),
        P("sp", None, "tp"),
    )
    return jax.shard_map(
        local, mesh=mesh, in_specs=placed, out_specs=P("sp", "tp"), check_vma=False
    )
```

```python
import jax
import jax.numpy as jnp
from jax import lax
from jax.experimental import pallas as pl
from jax.experimental.pallas import tpu as pltpu
from jax.sharding import PartitionSpec as P

D = 4096
HEAD = 64
CHUNK = 128
EXP_HALF = 0.6065306597126334


EPS_GROUP = 0.00064
EPS_NORM = 1e-06


def split(x):
    hi = x.astype(jnp.bfloat16)
    lo = (x - hi.astype(jnp.float32)).astype(jnp.bfloat16)
    return hi, lo


def dot(a, b, dims):
    return lax.dot_general(a, b, (dims, ((), ())), preferred_element_type=jnp.float32)


NN = ((1,), (0,))
NT = ((1,), (1,))
TN = ((0,), (0,))


def dot3(a, b, dims=NN):
    return dot(a[0], b[0], dims) + (dot(a[0], b[1], dims) + dot(a[1], b[0], dims))


def dot2(a, b, dims=NN):
    return dot(a[0], b, dims) + dot(a[1], b, dims)


def sigmoid(x):
    return 1.0 / (1.0 + jnp.exp(-x))


def mix_kernel(r_ref, k_ref, v_ref, d_ref, a_ref, out_ref, state_ref):
    tokens = r_ref.shape[0]
    chunks = tokens // CHUNK
    row = lax.broadcasted_iota(jnp.int32, (CHUNK, CHUNK), 0)
    col = lax.broadcasted_iota(jnp.int32, (CHUNK, CHUNK), 1)
    strict = col < row
    causal = col <= row
    eye = jnp.where(col == row, 1.0, 0.0)
    ones_lower = jnp.where(causal, 1.0, 0.0).astype(jnp.bfloat16)
    low = lax.broadcasted_iota(jnp.int32, (CHUNK, 2 * HEAD), 1) < HEAD

    work = []
    for chunk in range(chunks):
        rows = pl.ds(chunk * CHUNK, CHUNK)
        recept = r_ref[rows, :].astype(jnp.float32)
        keyvec = k_ref[rows, :].astype(jnp.float32)
        logdec = -EXP_HALF * sigmoid(d_ref[rows, :].astype(jnp.float32))
        first, second = split(logdec)
        third = (logdec - first.astype(jnp.float32) - second.astype(jnp.float32)).astype(jnp.bfloat16)
        cum_in = dot(ones_lower, first, NN) + (
            dot(ones_lower, second, NN) + dot(ones_lower, third, NN)
        )
        cum_end = cum_in[CHUNK - 1 :, :]
        squares = keyvec * keyvec
        norms = jnp.where(
            low,
            jnp.sum(squares[:, :HEAD], axis=1, keepdims=True),
            jnp.sum(squares[:, HEAD:], axis=1, keepdims=True),
        )
        unit_key = keyvec * lax.rsqrt(1.0 + norms)
        correction = unit_key * sigmoid(a_ref[rows, :].astype(jnp.float32))
        growth = jnp.exp(-cum_in)
        tail = jnp.exp(cum_end - cum_in)
        r_scaled = recept * jnp.exp(cum_in)
        u_scaled = unit_key * jnp.exp(cum_in - logdec)
        queries = split(jnp.concatenate([u_scaled, r_scaled], axis=0))
        sources = split(jnp.concatenate([keyvec * growth, correction * growth], axis=0))
        tails = split(jnp.concatenate([keyvec * tail, -(correction * tail)], axis=0))
        keep = jnp.broadcast_to(jnp.exp(cum_end), (2 * HEAD, 2 * HEAD)).T
        values = v_ref[rows, :]
        for head in range(2):
            lanes = slice(head * HEAD, (head + 1) * HEAD)
            query = tuple(q[:, lanes] for q in queries)
            source = tuple(s[:, lanes] for s in sources)
            scores = dot3(query, source, NT)
            work.append(
                dict(
                    head=head,
                    chunk=chunk,
                    query=query,
                    tail=tuple(t[:, lanes] for t in tails),
                    keep=keep[lanes, :],
                    value=jnp.concatenate(
                        [values[:, lanes], jnp.zeros((CHUNK, HEAD), jnp.bfloat16)], axis=1
                    ),
                    key_both=split(
                        jnp.concatenate(
                            [
                                jnp.where(strict, scores[:CHUNK, :CHUNK], 0.0),
                                jnp.where(causal, scores[CHUNK:, :CHUNK], 0.0),
                            ],
                            axis=0,
                        )
                    ),
                    pull=jnp.where(strict, scores[:CHUNK, CHUNK:], 0.0),
                    corr_read=split(jnp.where(causal, scores[CHUNK:, CHUNK:], 0.0)),
                )
            )
    for item in work:
        item["inverse"] = eye - jnp.where(row // 2 == col // 2, item["pull"], 0.0)
        item["from_values"] = dot2(item["key_both"], item["value"])
    size = 2
    while size < CHUNK:
        joined = (row // (2 * size) == col // (2 * size)) & (row // size != col // size)
        halves = []
        for item in work:
            inverse = split(item["inverse"])
            between = split(jnp.where(joined, item["pull"], 0.0))
            halves.append((inverse, dot3(between, inverse)))
        for item, (inverse, half) in zip(work, halves):
            item["inverse"] = item["inverse"] - dot3(inverse, split(half))
        size *= 2
    key_row = lax.broadcasted_iota(jnp.int32, (HEAD, 2 * HEAD), 0)
    lane = lax.broadcasted_iota(jnp.int32, (HEAD, 2 * HEAD), 1)
    start = jnp.where(lane == key_row + HEAD, 1.0, 0.0)
    states = [start, start]
    for item in work:
        head = item["head"]
        state = states[head]
        from_start = dot3(item["query"], split(state)) + item["from_values"]
        pulled = dot3(split(item["inverse"]), split(from_start[:CHUNK]))
        pulled_parts = split(pulled)
        out_ref[pl.ds(item["chunk"] * CHUNK, CHUNK), pl.ds(head * 2 * HEAD, 2 * HEAD)] = (
            from_start[CHUNK:] - dot3(item["corr_read"], pulled_parts)
        )
        key_tail = tuple(t[:CHUNK] for t in item["tail"])
        corr_tail = tuple(t[CHUNK:] for t in item["tail"])
        states[head] = (
            item["keep"] * state
            + dot2(key_tail, item["value"], TN)
            + dot3(corr_tail, pulled_parts, TN)
        )
    for head in range(2):
        state_ref[pl.ds(head * HEAD, HEAD), :] = states[head].astype(jnp.bfloat16)


def read_kernel(place_ref, read_ref, maps_ref, gate_ref, gain_ref, out_ref):
    def one(step, carried):
        following = []
        for head in range(2):
            both = maps_ref[step, pl.ds(head * HEAD, HEAD), :]
            parts = split(carried[head])
            step_map = both[:, HEAD:]
            following.append(
                both[:, :HEAD].astype(jnp.float32)
                + dot(step_map, parts[0], NN)
                + dot(step_map, parts[1], NN)
            )
        return tuple(following)

    zero = jnp.zeros((HEAD, HEAD), jnp.float32)
    incoming = lax.fori_loop(0, place_ref[0], one, (zero, zero))
    scaled = []
    for head in range(2):
        both = read_ref[:, pl.ds(head * 2 * HEAD, 2 * HEAD)]
        state_read = both[:, :HEAD] + dot3(split(both[:, HEAD:]), split(incoming[head]))
        centred = state_read - jnp.mean(state_read, axis=1, keepdims=True)
        variance = jnp.mean(centred * centred, axis=1, keepdims=True)
        scaled.append(centred * lax.rsqrt(variance + EPS_GROUP))
    gated = (
        jnp.concatenate(scaled, axis=1)
        * gain_ref[...]
        * sigmoid(gate_ref[...].astype(jnp.float32))
    )
    out_ref[...] = gated.astype(jnp.bfloat16)


def time_mix(
    receptance, key_vectors, value_vectors, decay_logits, rate_logits, gate_logits, group_gain
):
    tokens_here, channels = receptance.shape
    pairs = channels // (2 * HEAD)
    wide = pl.BlockSpec((tokens_here, 2 * HEAD), lambda i: (0, i))
    double = pl.BlockSpec((tokens_here, 4 * HEAD), lambda i: (0, i))
    reads, states = pl.pallas_call(
        mix_kernel,
        grid=(pairs,),
        in_specs=[wide] * 5,
        out_specs=[double, pl.BlockSpec((2 * HEAD, 2 * HEAD), lambda i: (i, 0))],
        out_shape=[
            jax.ShapeDtypeStruct((tokens_here, 2 * channels), jnp.float32),
            jax.ShapeDtypeStruct((channels, 2 * HEAD), jnp.bfloat16),
        ],
        name="mix",
    )(receptance, key_vectors, value_vectors, decay_logits, rate_logits)
    maps = lax.all_gather(states, "sp")
    place = lax.axis_index("sp").astype(jnp.int32).reshape(1)
    return pl.pallas_call(
        read_kernel,
        grid=(pairs,),
        in_specs=[
            pl.BlockSpec(memory_space=pltpu.SMEM),
            double,
            pl.BlockSpec((maps.shape[0], 2 * HEAD, 2 * HEAD), lambda i: (0, i, 0)),
            wide,
            pl.BlockSpec((1, 2 * HEAD), lambda i: (0, i)),
        ],
        out_specs=wide,
        out_shape=jax.ShapeDtypeStruct((tokens_here, channels), jnp.bfloat16),
        name="read",
    )(place, reads, maps, gate_logits, group_gain.reshape(1, channels))


def exchange(x, axis, shape, source, target, collective_id, name):
    def kernel(x_ref, out_ref, stage, send_sem, recv_sem, local_sem):
        n = lax.axis_size(axis)
        me = lax.axis_index(axis)
        peers = [lax.rem(me + step, n) for step in range(1, n)]
        barrier = pltpu.get_barrier_semaphore()
        for peer in peers:
            pl.semaphore_signal(
                barrier, inc=1, device_id={axis: peer}, device_id_type=pl.DeviceIdType.MESH
            )
        pl.semaphore_wait(barrier, n - 1)
        copies = []
        for step, peer in enumerate(peers):
            copy = pltpu.make_async_remote_copy(
                src_ref=source(x_ref, peer),
                dst_ref=target(out_ref, me),
                send_sem=send_sem.at[step],
                recv_sem=recv_sem.at[step],
                device_id={axis: peer},
                device_id_type=pl.DeviceIdType.MESH,
            )
            copy.start()
            copies.append(copy)
        own = pltpu.make_async_copy(source(x_ref, me), stage, local_sem)
        own.start()
        own.wait()
        own = pltpu.make_async_copy(stage, target(out_ref, me), local_sem)
        own.start()
        own.wait()
        for copy in copies:
            copy.wait()

    n = lax.axis_size(axis)
    return pl.pallas_call(
        kernel,
        in_specs=[pl.BlockSpec(memory_space=pl.ANY)],
        out_specs=pl.BlockSpec(memory_space=pl.ANY),
        out_shape=jax.ShapeDtypeStruct(shape, x.dtype),
        scratch_shapes=[
            pltpu.VMEM(x.shape[-2:], x.dtype),
            pltpu.SemaphoreType.DMA((n - 1,)),
            pltpu.SemaphoreType.DMA((n - 1,)),
            pltpu.SemaphoreType.DMA,
        ],
        compiler_params=pltpu.CompilerParams(collective_id=collective_id, has_side_effects=True),
        name=name,
    )(x)


def gather_columns(x, axis, collective_id):
    rows, columns = x.shape
    return exchange(
        x,
        axis,
        (rows, lax.axis_size(axis) * columns),
        lambda ref, peer: ref,
        lambda ref, me: ref.at[:, pl.ds(pl.multiple_of(me * columns, columns), columns)],
        collective_id,
        "gather_columns",
    )


def gather_rows(x, axis, collective_id):
    rows, columns = x.shape
    return exchange(
        x,
        axis,
        (lax.axis_size(axis) * rows, columns),
        lambda ref, peer: ref,
        lambda ref, me: ref.at[pl.ds(pl.multiple_of(me * rows, rows), rows), :],
        collective_id,
        "gather_rows",
    )


def swap_blocks(x, axis, collective_id):
    return exchange(
        x, axis, x.shape, lambda ref, peer: ref.at[peer], lambda ref, me: ref.at[me],
        collective_id, "swap_blocks",
    )


MESH = pl.DeviceIdType.MESH
GROUPS = 4


def pack_left(a):
    hi, lo = split(a)
    return jnp.concatenate([hi, lo], axis=1)


def pack_right(b):
    both = jnp.concatenate(split(b), axis=1)
    return jnp.concatenate([both, both], axis=0)


def dot_packed(left, right):
    out = dot(left, right, NN)
    n = out.shape[1] // 2
    return out[:, :n] + out[:, n:]


def three(a, axis, second):
    hi, lo = split(a)
    return jnp.concatenate([hi, hi, lo] if second else [hi, lo, hi], axis=axis)


def lower_rows(a, size):
    starts = range(size, a.shape[0], 2 * size)
    return jnp.concatenate([a[at : at + size] for at in starts], axis=0)


def join_rows(a, lower, size):
    parts = []
    for i, at in enumerate(range(0, a.shape[0], 2 * size)):
        parts += [a[at : at + size], lower[i * size : (i + 1) * size]]
    return jnp.concatenate(parts, axis=0)


def spread_rows(lower, size):
    parts = []
    for at in range(0, lower.shape[0], size):
        parts += [jnp.zeros((size, lower.shape[1]), lower.dtype), lower[at : at + size]]
    return jnp.concatenate(parts, axis=0)


def mix_heads(recept_in, key_in, values_in, decay_in, rate_in, write_read, write_state):
    tokens, width = recept_in.shape
    chunks = tokens // CHUNK
    pairs = width // (2 * HEAD)
    row = lax.broadcasted_iota(jnp.int32, (CHUNK, CHUNK), 0)
    col = lax.broadcasted_iota(jnp.int32, (CHUNK, CHUNK), 1)
    strict = col < row
    causal = col <= row
    eye = jnp.where(col == row, 1.0, 0.0)
    ones_lower = jnp.where(causal, 1.0, 0.0).astype(jnp.bfloat16)
    ones_twice = jnp.concatenate([ones_lower, ones_lower], axis=1)
    low = lax.broadcasted_iota(jnp.int32, (CHUNK, 2 * HEAD), 1) < HEAD
    nothing = jnp.zeros((CHUNK, 2 * HEAD), jnp.bfloat16)

    work = []
    for chunk in range(chunks):
        rows = slice(chunk * CHUNK, (chunk + 1) * CHUNK)
        for pair in range(pairs):
            lanes = slice(pair * 2 * HEAD, (pair + 1) * 2 * HEAD)
            recept = recept_in[rows, lanes].astype(jnp.float32)
            keyvec = key_in[rows, lanes].astype(jnp.float32)
            values = values_in[rows, lanes]
            logdec = -EXP_HALF * sigmoid(decay_in[rows, lanes].astype(jnp.float32))
            first, second = split(logdec)
            third = (logdec - first.astype(jnp.float32) - second.astype(jnp.float32)).astype(
                jnp.bfloat16
            )
            cum_in = dot_packed(
                ones_twice,
                jnp.concatenate(
                    [
                        jnp.concatenate([first, third], axis=1),
                        jnp.concatenate([second, nothing], axis=1),
                    ],
                    axis=0,
                ),
            )
            cum_end = cum_in[CHUNK - 1 :, :]
            squares = keyvec * keyvec
            norms = jnp.where(
                low,
                jnp.sum(squares[:, :HEAD], axis=1, keepdims=True),
                jnp.sum(squares[:, HEAD:], axis=1, keepdims=True),
            )
            unit_key = keyvec * lax.rsqrt(1.0 + norms)
            correction = unit_key * sigmoid(rate_in[rows, lanes].astype(jnp.float32))
            growth = jnp.exp(-cum_in)
            tail = jnp.exp(cum_end - cum_in)
            r_scaled = recept * jnp.exp(cum_in)
            u_scaled = unit_key * jnp.exp(cum_in - logdec)
            queries = jnp.concatenate([u_scaled, r_scaled], axis=0)
            sources = jnp.concatenate([keyvec * growth, correction * growth], axis=0)
            tails = jnp.concatenate([(keyvec * tail).T, -(correction * tail).T], axis=1)
            tail_hi, tail_lo = split(tails)
            keep = jnp.broadcast_to(jnp.exp(cum_end), (2 * HEAD, 2 * HEAD)).T
            for head in range(2):
                part = slice(head * HEAD, (head + 1) * HEAD)
                query = three(queries[:, part], 1, False)
                scores = dot(query, three(sources[:, part], 1, True), NT)
                value = jnp.concatenate(
                    [values[:, part], jnp.zeros((CHUNK, HEAD), jnp.bfloat16)], axis=1
                )
                work.append(
                    dict(
                        head=2 * pair + head,
                        chunk=chunk,
                        query=query,
                        tail=jnp.concatenate([tail_hi[part, :], tail_lo[part, :]], axis=0),
                        keep=keep[part, :],
                        value=value,
                        key_both=pack_left(
                            jnp.concatenate(
                                [
                                    jnp.where(strict, scores[:CHUNK, :CHUNK], 0.0),
                                    jnp.where(causal, scores[CHUNK:, :CHUNK], 0.0),
                                ],
                                axis=0,
                            )
                        ),
                        pull=jnp.where(strict, scores[:CHUNK, CHUNK:], 0.0),
                        corr_read=pack_left(jnp.where(causal, scores[CHUNK:, CHUNK:], 0.0)),
                    )
                )
    for item in work:
        item["inverse"] = eye - jnp.where(row // 2 == col // 2, item["pull"], 0.0)
        value = item["value"]
        item["from_values"] = dot(
            item["key_both"], jnp.concatenate([value, value], axis=0), NN
        )
    size = 2
    while size < CHUNK:
        joined = (row // (2 * size) == col // (2 * size)) & (row // size != col // size)
        halves = []
        if size < 8:
            for item in work:
                between = pack_left(jnp.where(joined, item["pull"], 0.0))
                halves.append(dot_packed(between, pack_right(item["inverse"])))
            for item, half in zip(work, halves):
                item["inverse"] = item["inverse"] - dot_packed(
                    pack_left(item["inverse"]), pack_right(half)
                )
        else:
            for item in work:
                between = pack_left(lower_rows(jnp.where(joined, item["pull"], 0.0), size))
                halves.append(dot_packed(between, pack_right(item["inverse"])))
            for item, half in zip(work, halves):
                inverse = item["inverse"]
                below = lower_rows(inverse, size)
                update = dot_packed(pack_left(below), pack_right(spread_rows(half, size)))
                item["inverse"] = join_rows(inverse, below - update, size)
        size *= 2
    key_row = lax.broadcasted_iota(jnp.int32, (HEAD, 2 * HEAD), 0)
    lane = lax.broadcasted_iota(jnp.int32, (HEAD, 2 * HEAD), 1)
    start = jnp.where(lane == key_row + HEAD, 1.0, 0.0)
    states = [start] * (2 * pairs)
    for chunk in range(chunks):
        items = [item for item in work if item["chunk"] == chunk]
        froms = [
            dot(item["query"], three(states[item["head"]], 0, True), NN) + item["from_values"]
            for item in items
        ]
        pulls = [
            dot_packed(pack_left(item["inverse"]), pack_right(value[:CHUNK]))
            for item, value in zip(items, froms)
        ]
        for item, value, pulled in zip(items, froms, pulls):
            head = item["head"]
            write_read(
                chunk, head, value[CHUNK:] - dot_packed(item["corr_read"], pack_right(pulled))
            )
            hi, lo = split(pulled)
            right = jnp.concatenate(
                [
                    jnp.concatenate([item["value"], hi], axis=0),
                    jnp.concatenate([nothing, lo], axis=0),
                ],
                axis=1,
            )
            out = dot(item["tail"], right, NN)
            states[head] = (
                item["keep"] * states[head]
                + (out[:HEAD, : 2 * HEAD] + out[HEAD:, : 2 * HEAD])
                + out[:HEAD, 2 * HEAD :]
            )
    for head in range(2 * pairs):
        write_state(head, states[head].astype(jnp.bfloat16))


def mixer_kernel(
    r_ref,
    k_ref,
    v_ref,
    d_ref,
    a_ref,
    gate_ref,
    gain_ref,
    residual_ref,
    norm_ref,
    mixer_hbm,
    normed_ref,
    midway_ref,
    mixer_w,
    reads,
    maps_own,
    maps_in,
    joint,
    joint_in,
    carry_out,
    carry_in,
    carried,
    gathered,
    acc,
    sums,
    load_sem,
    swap_send,
    swap_recv,
    chain_send,
    chain_recv,
    joint_send,
    joint_recv,
    gather_send,
    gather_recv,
    sum_send,
    sum_recv,
):
    tokens, features = residual_ref.shape
    steps, _, wide = reads.shape
    width = wide // 2
    heads = width // HEAD
    tps = lax.axis_size("tp")
    chips = lax.axis_size("sp") // 2
    sp = lax.axis_index("sp")
    tp = lax.axis_index("tp")
    z, core = sp // 2, sp % 2
    partner = {"sp": z * 2 + (1 - core)}
    y, x = tp // 2, tp % 2
    x_peer = y * 2 + (1 - x)
    y_peer = (1 - y) * 2 + x
    peers = [{"tp": x_peer}, {"tp": y_peer}, {"tp": (1 - y) * 2 + (1 - x)}]

    def load(step, block):
        return pltpu.make_async_copy(
            mixer_hbm.at[pl.ds(pl.multiple_of(block * steps * width + step * width, width), width), :],
            mixer_w.at[step, pl.ds(block * width, width), :],
            load_sem.at[step, block],
        )

    def load_all(step, carry):
        for block in range(tps):
            load(step, block).start()
        return carry

    lax.fori_loop(0, steps, load_all, 0)

    barrier = pltpu.get_barrier_semaphore()
    friends = [partner] + peers
    friends += [{"sp": ((z + shift) % chips) * 2 + core} for shift in range(1, chips)]
    for friend in friends:
        pl.semaphore_signal(barrier, inc=1, device_id=friend, device_id_type=MESH)
    acc[...] = residual_ref[...].astype(jnp.float32)
    pl.semaphore_wait(barrier, len(friends))

    def remote(source, target, send, recv, device):
        return pltpu.make_async_remote_copy(
            src_ref=source, dst_ref=target, send_sem=send, recv_sem=recv,
            device_id=device, device_id_type=MESH,
        )

    def swap(j):
        return remote(maps_own.at[j], maps_in.at[j], swap_send.at[j], swap_recv.at[j], partner)

    def chain(j, hop, target):
        return remote(
            carry_out.at[j], carry_in.at[j], chain_send.at[hop, j], chain_recv.at[j],
            {"sp": target * 2 + core},
        )

    def hand_joint(j):
        return remote(
            joint.at[j], joint_in.at[j], joint_send.at[j], joint_recv.at[j],
            {"sp": (chips - 1) * 2 + core},
        )

    def columns(owner):
        return pl.ds(pl.multiple_of(owner * width, width), width)

    def gather(j):
        own = gathered.at[j, :, columns(tp)]
        return [
            remote(own, own, gather_send.at[i, j], gather_recv.at[i, j], peers[i]) for i in range(2)
        ]

    def relay(j):
        low = gathered.at[j, pl.ds(0, tokens // 2), columns(x_peer)]
        high = gathered.at[j, pl.ds(tokens // 2, tokens // 2), columns(y_peer)]
        return [
            remote(low, low, gather_send.at[2, j], gather_recv.at[2, j], peers[1]),
            remote(high, high, gather_send.at[3, j], gather_recv.at[3, j], peers[0]),
        ]

    def mix(i):
        lanes = pl.ds(pl.multiple_of(i * width, width), width)

        def write_read(chunk, head, value):
            reads[i, pl.ds(chunk * CHUNK, CHUNK), pl.ds(head * 2 * HEAD, 2 * HEAD)] = value

        def write_state(head, value):
            maps_own[i, pl.ds(head * HEAD, HEAD), :] = value

        mix_heads(
            r_ref[:, lanes], k_ref[:, lanes], v_ref[:, lanes], d_ref[:, lanes], a_ref[:, lanes],
            write_read, write_state,
        )
        swap(i).start()

    half_lane = lax.broadcasted_iota(jnp.int32, (HEAD, 2 * HEAD), 1) < HEAD

    def join(j):
        swap(j).wait_recv()
        for head in range(heads):
            part = pl.ds(head * HEAD, HEAD)
            own, other = maps_own[j, part, :], maps_in[j, part, :]
            first = jnp.where(core == 0, own, other)
            second = jnp.where(core == 0, other, own)
            both = dot(second[:, HEAD:], first, NN)
            joint[j, part, :] = both + jnp.where(half_lane, second.astype(jnp.float32), 0.0)

        @pl.when(z == 0)
        def _():
            carry_out[j] = jnp.concatenate(
                [joint[j, pl.ds(head * HEAD, HEAD), :][:, :HEAD] for head in range(heads)], axis=1
            ).astype(jnp.bfloat16)
            carried[j] = jnp.zeros((HEAD, width), jnp.bfloat16)
            chain(j, 0, 1).start()

        @pl.when(z == 2)
        def _():
            hand_joint(j).start()

    def advance(maps, j):
        following = []
        for head in range(heads):
            both = maps[j, pl.ds(head * HEAD, HEAD), :]
            value = carry_in[j, :, pl.ds(head * HEAD, HEAD)]
            following.append(both[:, :HEAD] + dot2(split(both[:, HEAD:]), value))
        return jnp.concatenate(following, axis=1).astype(jnp.bfloat16)

    def hop(j):
        chain(j, 0, 1).wait_recv()
        carried[j] = carry_in[j]
        carry_out[j] = advance(joint, j)
        chain(j, 0, 2).start()
        chain(j, 1, 3).start()

    def finish(j):
        @pl.when(z >= 2)
        def _():
            chain(j, 0, 1).wait_recv()

        @pl.when(z == 2)
        def _():
            carried[j] = carry_in[j]

        @pl.when(z == 3)
        def _():
            hand_joint(j).wait_recv()
            carried[j] = advance(joint_in, j)

        nothing = jnp.zeros((HEAD, HEAD), jnp.bfloat16)
        unit = jnp.where(
            lax.broadcasted_iota(jnp.int32, (HEAD, HEAD), 0)
            == lax.broadcasted_iota(jnp.int32, (HEAD, HEAD), 1),
            1.0,
            0.0,
        ).astype(jnp.bfloat16)
        state_parts = []
        for head in range(heads):
            value = carried[j, :, pl.ds(head * HEAD, HEAD)]
            other = maps_in[j, pl.ds(head * HEAD, HEAD), :]
            passed = other[:, :HEAD].astype(jnp.float32) + dot(other[:, HEAD:], value, NN)
            state_parts.append(split(jnp.where(core == 0, value.astype(jnp.float32), passed)))
        head_of = [
            lax.broadcasted_iota(jnp.int32, (4 * HEAD, 2 * HEAD), axis) // HEAD % 2
            for axis in range(2)
        ]
        average = jnp.where(head_of[0] == head_of[1], 1.0 / HEAD, 0.0).astype(jnp.bfloat16)
        for pair in range(heads // 2):
            here = [reads[j, :, pl.ds((2 * pair + i) * 2 * HEAD, 2 * HEAD)] for i in range(2)]
            hi, lo = split(jnp.concatenate(here, axis=1))
            (first_hi, first_lo), (second_hi, second_lo) = state_parts[2 * pair : 2 * pair + 2]
            wide_rows = [
                [unit, nothing, nothing, nothing],
                [first_hi, nothing, first_lo, nothing],
                [nothing, unit, nothing, nothing],
                [nothing, second_hi, nothing, second_lo],
            ]
            right = jnp.concatenate(
                [jnp.concatenate(blocks, axis=1) for blocks in wide_rows], axis=0
            )
            state_read = dot_packed(hi, right) + dot(lo, right[:, : 2 * HEAD], NN)
            centred = state_read - dot(pack_left(state_read), average, NN)
            variance = dot(pack_left(centred * centred), average, NN)
            lanes = pl.ds(pl.multiple_of(j * width + pair * 2 * HEAD, 2 * HEAD), 2 * HEAD)
            gated = (
                centred
                * lax.rsqrt(variance + EPS_GROUP)
                * gain_ref[:, lanes]
                * sigmoid(gate_ref[:, lanes].astype(jnp.float32))
            )
            own_lanes = pl.ds(pl.multiple_of(tp * width + pair * 2 * HEAD, 2 * HEAD), 2 * HEAD)
            gathered[j, :, own_lanes] = gated.astype(jnp.bfloat16)
        for copy in gather(j):
            copy.start()

    def pass_on(j):
        for copy, after in zip(gather(j), relay(j)):
            copy.wait_recv()
            after.start()

    def project(j):
        for block in range(tps):
            load(j, block).wait()
        for copy in relay(j):
            copy.wait_recv()
        acc[...] += dot(gathered[j], mixer_w[j], NN)

    def within(j):
        return jnp.logical_and(j >= 0, j < steps)

    def step(t, carry):
        @pl.when(jnp.logical_and(z == 1, within(t - 2)))
        def _():
            hop(t - 2)

        @pl.when(within(t))
        def _():
            mix(t)

        @pl.when(within(t - 1))
        def _():
            join(t - 1)

        @pl.when(within(t - 3))
        def _():
            pass_on(t - 3)

        @pl.when(jnp.logical_and(z == 0, within(t - 1)))
        def _():
            finish(t - 1)

        @pl.when(jnp.logical_and(z > 0, within(t - 2)))
        def _():
            finish(t - 2)

        @pl.when(within(t - 4))
        def _():
            project(t - 4)

        return carry

    lax.fori_loop(0, steps + 4, step, 0)

    midway = acc[...].astype(jnp.bfloat16)
    midway_ref[...] = midway
    midway_f = midway.astype(jnp.float32)
    squares = jnp.sum(midway_f * midway_f, axis=1, keepdims=True)
    sums[0] = jnp.broadcast_to(squares, (tokens, 128)).T[:8, :]
    copies = [
        remote(sums.at[0], sums.at[i + 1], sum_send.at[i], sum_recv.at[i], peer)
        for i, peer in enumerate(peers)
    ]
    for copy in copies:
        copy.start()
    scaled = midway_f * norm_ref[...]
    for copy in copies:
        copy.wait_recv()
    total = sums[0]
    for i in range(1, tps):
        total = total + sums[i]
    total = jnp.concatenate([total] * (128 // 8), axis=0).T[:, :1]
    normed_ref[...] = (scaled * lax.rsqrt(total / D + EPS_NORM)).astype(jnp.bfloat16)

    for copy in copies:
        copy.wait_send()

    def drain(j, carry):
        swap(j).wait_send()

        @pl.when(z < 2)
        def _():
            chain(j, 0, 1).wait_send()

        @pl.when(z == 1)
        def _():
            chain(j, 1, 1).wait_send()

        @pl.when(z == 2)
        def _():
            hand_joint(j).wait_send()

        for copy in gather(j) + relay(j):
            copy.wait_send()
        return carry

    lax.fori_loop(0, steps, drain, 0)


HEADS_PER_STEP = 4


def mixed_tokens(
    receptance, key_vectors, value_vectors, decay_logits, rate_logits, gate_logits, group_gain,
    residual, mixer_out, norm_gain,
):
    tokens, channels = receptance.shape
    features = residual.shape[1]
    tps = lax.axis_size("tp")
    width = HEADS_PER_STEP * HEAD
    steps = channels // width
    bf = jnp.bfloat16
    f32 = jnp.float32
    whole = pl.BlockSpec(memory_space=pltpu.VMEM)
    dma = pltpu.SemaphoreType.DMA
    return pl.pallas_call(
        mixer_kernel,
        in_specs=[whole] * 9 + [pl.BlockSpec(memory_space=pl.ANY)],
        out_specs=[whole, whole],
        out_shape=[jax.ShapeDtypeStruct((tokens, features), bf)] * 2,
        scratch_shapes=[
            pltpu.VMEM((steps, tps * width, features), bf),
            pltpu.VMEM((steps, tokens, 2 * width), f32),
            pltpu.VMEM((steps, width, 2 * HEAD), bf),
            pltpu.VMEM((steps, width, 2 * HEAD), bf),
            pltpu.VMEM((steps, width, 2 * HEAD), f32),
            pltpu.VMEM((steps, width, 2 * HEAD), f32),
            pltpu.VMEM((steps, HEAD, width), bf),
            pltpu.VMEM((steps, HEAD, width), bf),
            pltpu.VMEM((steps, HEAD, width), bf),
            pltpu.VMEM((steps, tokens, tps * width), bf),
            pltpu.VMEM((tokens, features), f32),
            pltpu.VMEM((tps, 8, tokens), f32),
            dma((steps, tps)),
            dma((steps,)),
            dma((steps,)),
            dma((2, steps)),
            dma((steps,)),
            dma((steps,)),
            dma((steps,)),
            dma((4, steps)),
            dma((4, steps)),
            dma((tps - 1,)),
            dma((tps - 1,)),
        ],
        compiler_params=pltpu.CompilerParams(
            collective_id=5, has_side_effects=True, vmem_limit_bytes=56 * 1024 * 1024
        ),
        name="mixer",
    )(
        receptance, key_vectors, value_vectors, decay_logits, rate_logits, gate_logits,
        group_gain.reshape(1, channels), residual, norm_gain.reshape(1, features), mixer_out,
    )


LAG = 1
LEAD = 1


def expert_kernel(
    normed_hbm,
    midway_hbm,
    ids_ref,
    weight_ref,
    gate_hbm,
    up_hbm,
    down_hbm,
    out_ref,
    normed_ref,
    midway_ref,
    gate_w,
    up_w,
    down_w,
    select,
    outgoing,
    factors,
    aux_out,
    aux_in,
    rows_in,
    part_a,
    part_b,
    first_a,
    first_b,
    pass_a,
    pass_b,
    second_a,
    second_b,
    hidden_a,
    hidden_b,
    own_res,
    pair_out,
    pair_in,
    back_out,
    back_in,
    load_sem,
    disp_send,
    disp_recv,
    aux_send,
    aux_recv,
    fwd_send,
    fwd_recv,
    tp_send,
    tp_recv,
    pair_send,
    pair_recv,
    back_send,
    back_recv,
):
    tokens = normed_ref.shape[0]
    size = outgoing.shape[1]
    slots = 2 * size
    quarter = size // 4
    half = size // 2
    width = hidden_a.shape[2]
    peers = GROUPS
    units = 2 * peers
    blocks = 2 * units
    sp = lax.axis_index("sp")
    tp = lax.axis_index("tp")
    z, core = sp // 2, sp % 2
    y, x = tp // 2, tp % 2
    x_peer = y * 2 + (1 - x)
    y_peer = (1 - y) * 2 + x

    def chip(turn):
        return 2 * ((z // 2 + turn // 2) % 2) + (z % 2 + turn % 2) % 2

    def turn_of(q):
        return (q + 6) // 8 + (q + 5) // 8 + (q + 3) // 8 - 2 * ((q + 1) // 8)

    def half_of(q):
        return (q + 7) // 8 - (q + 6) // 8 + (q + 4) // 8 - (q + 3) // 8 + (q + 2) // 8

    loads = [
        pltpu.make_async_copy(source.at[0], target, load_sem.at[i])
        for i, (source, target) in enumerate(((gate_hbm, gate_w), (up_hbm, up_w), (down_hbm, down_w)))
    ]
    load_rows = pltpu.make_async_copy(normed_hbm, normed_ref, load_sem.at[3])
    load_rows.start()
    loads.append(pltpu.make_async_copy(midway_hbm, midway_ref, load_sem.at[4]))
    for load in loads:
        load.start()

    partner = {"sp": z * 2 + (1 - core)}
    barrier = pltpu.get_barrier_semaphore()
    friends = [partner, {"tp": x_peer}, {"tp": y_peer}]
    friends += [{"sp": chip(turn) * 2 + core} for turn in range(1, peers)]
    for friend in friends:
        pl.semaphore_signal(barrier, inc=1, device_id=friend, device_id_type=MESH)

    def remote(source, target, send, recv, device):
        return pltpu.make_async_remote_copy(
            src_ref=source, dst_ref=target, send_sem=send, recv_sem=recv,
            device_id=device, device_id_type=MESH,
        )

    def dispatch(q):
        return remote(
            outgoing.at[q], rows_in.at[2 * q], disp_send.at[q], disp_recv.at[q],
            {"sp": chip(turn_of(q)) * 2 + core},
        )

    def dispatch_aux(turn):
        return remote(
            aux_out.at[turn], aux_in.at[turn], aux_send.at[turn], aux_recv.at[turn],
            {"sp": chip(turn) * 2 + core},
        )

    def forward(q):
        return remote(rows_in.at[2 * q], rows_in.at[2 * q + 1], fwd_send.at[q], fwd_recv.at[q], partner)

    def over_tp(kind, k, source, target, device):
        return remote(source, target, tp_send.at[kind, k], tp_recv.at[kind, k], {"tp": device})

    def rows(start, size):
        return pl.ds(pl.multiple_of(start, quarter), size)

    def sum_first(k):
        return (
            over_tp(0, k, part_a.at[k, rows(half * (1 - x), half)], first_a.at[k], x_peer),
            over_tp(1, k, part_b.at[k, rows(half * (1 - y), half)], first_b.at[k], y_peer),
        )

    def sum_second(k):
        return (
            over_tp(2, k, pass_a.at[k], second_a.at[k], y_peer),
            over_tp(3, k, pass_b.at[k], second_b.at[k], x_peer),
        )

    def spread_first(k):
        own_a = hidden_a.at[k, rows(half * x + quarter * y, quarter)]
        own_b = hidden_b.at[k, rows(half * y + quarter * x, quarter)]
        return (over_tp(4, k, own_a, own_a, y_peer), over_tp(5, k, own_b, own_b, x_peer))

    def spread_second(k):
        own_a = hidden_a.at[k, rows(half * x, half)]
        own_b = hidden_b.at[k, rows(half * y, half)]
        return (over_tp(6, k, own_a, own_a, x_peer), over_tp(7, k, own_b, own_b, y_peer))

    def pair(q):
        return remote(pair_out.at[q], pair_in.at[q], pair_send.at[q], pair_recv.at[q], partner)

    def back_rows(q):
        return pl.ds(pl.multiple_of(turn_of(q) * slots + half_of(q) * size, size), size)

    def give_back(q):
        return remote(
            back_out.at[q], back_in.at[back_rows(q), :], back_send.at[q], back_recv.at[q],
            {"sp": chip(turn_of(q)) * 2 + core},
        )

    def as_columns(few_rows):
        return jnp.concatenate([few_rows] * (slots // 8), axis=0).T

    def few_rows():
        few = jnp.concatenate(
            [ids_ref[...].astype(jnp.float32), weight_ref[...], jnp.zeros((4, tokens), jnp.float32)],
            axis=0,
        )
        return jnp.concatenate([few] * (128 // 8), axis=0).T

    ids = few_rows()[:, :2].astype(jnp.int32)
    lane = lax.broadcasted_iota(jnp.int32, (tokens, 128), 1)
    slot_lane = lax.broadcasted_iota(jnp.int32, (tokens, slots), 1).astype(jnp.float32)
    earlier = jnp.where(
        lax.broadcasted_iota(jnp.int32, (tokens, tokens), 1)
        < lax.broadcasted_iota(jnp.int32, (tokens, tokens), 0),
        1.0,
        0.0,
    ).astype(jnp.bfloat16)
    group_of = [chip(turn) for turn in range(peers)]
    member = [
        jnp.logical_and(ids[:, :1] >= 2 * group, ids[:, :1] < 2 * group + 2) for group in group_of
    ]
    members = jnp.zeros((tokens, 128), jnp.float32)
    for turn in range(peers):
        members = jnp.where(jnp.logical_and(lane == turn, member[turn]), 1.0, members)
    ranks = dot(earlier, members.astype(jnp.bfloat16), NN)
    load_rows.wait()
    normed = normed_ref[...]
    pl.semaphore_wait(barrier, len(friends))
    for turn in range(peers):
        chosen = jnp.where(
            jnp.logical_and(slot_lane == ranks[:, turn : turn + 1], member[turn]), 1.0, 0.0
        ).astype(jnp.bfloat16)
        select[:, turn * slots : (turn + 1) * slots] = chosen
        picked = dot(chosen, normed, TN).astype(jnp.bfloat16)
        for part in range(2):
            piece = picked[part * size : (part + 1) * size]
            if turn == 0:
                rows_in[2 * part] = piece
                forward(part).start()
            else:
                q = {(1, 0): 2, (2, 0): 3, (2, 1): 4, (3, 0): 5, (3, 1): 6, (1, 1): 7}[turn, part]
                outgoing[q] = piece
                if q < 7:
                    dispatch(q).start()
    dispatch(7).start()
    for load in loads:
        load.wait()

    def weigh():
        few = few_rows()
        lane_of = lax.broadcasted_iota(jnp.int32, (tokens, 128), 1)
        ids, weights = few[:, :2].astype(jnp.int32), few[:, 2:4]
        for turn in range(peers):
            parts = jnp.zeros((tokens, 128), jnp.float32)
            for expert in range(2):
                name = 2 * group_of[turn] + expert
                value = jnp.where(ids[:, :1] == name, weights[:, :1], 0.0) + jnp.where(
                    ids[:, 1:2] == name, weights[:, 1:2], 0.0
                )
                for piece in range(3):
                    term = value.astype(jnp.bfloat16).astype(jnp.float32)
                    parts = jnp.where(lane_of == 3 * expert + piece, term, parts)
                    value = value - term
            by_slot = dot(
                parts.astype(jnp.bfloat16), select[:, turn * slots : (turn + 1) * slots], TN
            )
            weight_rows = jnp.concatenate(
                [
                    by_slot[0:1] + by_slot[1:2] + by_slot[2:3],
                    by_slot[3:4] + by_slot[4:5] + by_slot[5:6],
                    jnp.zeros((6, slots), jnp.float32),
                ],
                axis=0,
            )
            if turn == 0:
                factors[0] = as_columns(weight_rows)
            else:
                aux_out[turn] = weight_rows
                dispatch_aux(turn).start()

    def step(t, carry):
        @pl.when(t == 1)
        def _():
            weigh()

        @pl.when(jnp.logical_and(t >= LEAD + LAG, t < blocks + LEAD + LAG))
        def _():
            k = t - LEAD - LAG
            copies = sum_first(k)
            nexts = sum_second(k)
            copies[0].wait_recv()
            pass_a[k] = (
                part_a[k, rows(half * x + quarter * (1 - y), quarter)].astype(jnp.float32)
                + first_a[k, rows(quarter * (1 - y), quarter)].astype(jnp.float32)
            ).astype(jnp.bfloat16)
            nexts[0].start()
            copies[1].wait_recv()
            pass_b[k] = (
                part_b[k, rows(half * y + quarter * (1 - x), quarter)].astype(jnp.float32)
                + first_b[k, rows(quarter * (1 - x), quarter)].astype(jnp.float32)
            ).astype(jnp.bfloat16)
            nexts[1].start()

        @pl.when(jnp.logical_and(t >= LEAD + 2 * LAG, t < blocks + LEAD + 2 * LAG))
        def _():
            k = t - LEAD - 2 * LAG
            copies = sum_second(k)
            nexts = spread_first(k)
            for i, (part, first, second, hidden, major, minor) in enumerate(
                (
                    (part_a, first_a, second_a, hidden_a, x, y),
                    (part_b, first_b, second_b, hidden_b, y, x),
                )
            ):
                copies[i].wait_recv()
                mine = rows(half * major + quarter * minor, quarter)
                total = (
                    part[k, mine].astype(jnp.float32)
                    + first[k, rows(quarter * minor, quarter)].astype(jnp.float32)
                    + second[k].astype(jnp.float32)
                )
                gate, up = total[:, :width], total[:, width:]
                hidden[k, mine] = (gate * sigmoid(gate) * up).astype(jnp.bfloat16)
                nexts[i].start()

        @pl.when(jnp.logical_and(t >= LEAD + 3 * LAG, t < blocks + LEAD + 3 * LAG))
        def _():
            k = t - LEAD - 3 * LAG
            for copy, follow in zip(spread_first(k), spread_second(k)):
                copy.wait_recv()
                follow.start()

        @pl.when(t < blocks)
        def _():
            k = t
            q = k // 2

            @pl.when(jnp.logical_and(k % 2 == 0, q > 1))
            def _():
                dispatch(q).wait_recv()
                forward(q).start()

            @pl.when(k % 2 == 1)
            def _():
                forward(q).wait_recv()

            block = rows_in[k]
            for part, columns in ((part_a, pl.ds(0, width)), (part_b, pl.ds(width, width))):
                part[k, :, :width] = dot(block, gate_w[:, columns], NN).astype(jnp.bfloat16)
                part[k, :, width:] = dot(block, up_w[:, columns], NN).astype(jnp.bfloat16)
            for copy in sum_first(k):
                copy.start()

        @pl.when(jnp.logical_and(t >= LEAD + 4 * LAG, t < blocks + LEAD + 4 * LAG))
        def _():
            k = t - LEAD - 4 * LAG
            q = k // 2
            for copy in spread_second(k):
                copy.wait_recv()
            result = dot(hidden_a[k], down_w[:width, :], NN) + dot(hidden_b[k], down_w[width:, :], NN)

            @pl.when(k % 2 == 0)
            def _():
                own_res[q] = result

            @pl.when(k % 2 == 1)
            def _():
                pair_out[q] = result.astype(jnp.bfloat16)
                pair(q).start()

        last = t - LEAD - 5 * LAG - 1

        @pl.when(jnp.logical_and(last >= 0, last % 2 == 0))
        def _():
            q = last // 2

            @pl.when(q == 2)
            def _():
                for turn in range(1, peers):
                    dispatch_aux(turn).wait_recv()
                    factors[turn] = as_columns(aux_in[turn])

            pair(q).wait_recv()
            columns = factors[turn_of(q), pl.ds(pl.multiple_of(half_of(q) * size, size), size), :]
            low, high = columns[:, 0:1], columns[:, 1:2]
            mine = jnp.where(core == 0, low, high)
            other = jnp.where(core == 0, high, low)
            both = (own_res[q] * mine + pair_in[q].astype(jnp.float32) * other).astype(jnp.bfloat16)

            @pl.when(q < 2)
            def _():
                back_in[back_rows(q), :] = both

            @pl.when(q >= 2)
            def _():
                back_out[q] = both
                give_back(q).start()

        return carry

    lax.fori_loop(0, blocks + LEAD + 5 * LAG, step, 0)
    for q in range(2, units):
        give_back(q).wait_recv()
    total = midway_ref[...].astype(jnp.float32) + dot(select[...], back_in[...], NN)
    out_ref[...] = total.astype(jnp.bfloat16)

    for q in range(units):
        forward(q).wait_send()
        pair(q).wait_send()
        if q > 1:
            dispatch(q).wait_send()
            give_back(q).wait_send()
    for turn in range(1, peers):
        dispatch_aux(turn).wait_send()

    def drain(k, carry):
        for copies in (sum_first(k), sum_second(k), spread_first(k), spread_second(k)):
            for copy in copies:
                copy.wait_send()
        return carry

    lax.fori_loop(0, blocks, drain, 0)


def routed_experts(normed, midway, expert_ids, route_weight, expert_gate, expert_up, expert_down):
    tokens, features = normed.shape
    hidden = expert_gate.shape[2]
    half = hidden // 2
    slots = tokens // 2
    size = slots // 2
    quarter = size // 4
    peers = GROUPS
    units = 2 * peers
    blocks = 2 * units
    bf = jnp.bfloat16
    whole = pl.BlockSpec(memory_space=pltpu.VMEM)
    far = pl.BlockSpec(memory_space=pltpu.HBM)
    dma = pltpu.SemaphoreType.DMA
    return pl.pallas_call(
        expert_kernel,
        in_specs=[far] * 2 + [whole] * 2 + [far] * 3,
        out_specs=whole,
        out_shape=jax.ShapeDtypeStruct((tokens, features), bf),
        scratch_shapes=[
            pltpu.VMEM((tokens, features), bf),
            pltpu.VMEM((tokens, features), bf),
            pltpu.VMEM((features, hidden), bf),
            pltpu.VMEM((features, hidden), bf),
            pltpu.VMEM((hidden, features), bf),
            pltpu.VMEM((tokens, peers * slots), bf),
            pltpu.VMEM((units, size, features), bf),
            pltpu.VMEM((peers, slots, slots), jnp.float32),
            pltpu.VMEM((peers, 8, slots), jnp.float32),
            pltpu.VMEM((peers, 8, slots), jnp.float32),
            pltpu.VMEM((blocks, size, features), bf),
            pltpu.VMEM((blocks, size, hidden), bf),
            pltpu.VMEM((blocks, size, hidden), bf),
            pltpu.VMEM((blocks, size // 2, hidden), bf),
            pltpu.VMEM((blocks, size // 2, hidden), bf),
            pltpu.VMEM((blocks, quarter, hidden), bf),
            pltpu.VMEM((blocks, quarter, hidden), bf),
            pltpu.VMEM((blocks, quarter, hidden), bf),
            pltpu.VMEM((blocks, quarter, hidden), bf),
            pltpu.VMEM((blocks, size, half), bf),
            pltpu.VMEM((blocks, size, half), bf),
            pltpu.VMEM((units, size, features), jnp.float32),
            pltpu.VMEM((units, size, features), bf),
            pltpu.VMEM((units, size, features), bf),
            pltpu.VMEM((units, size, features), bf),
            pltpu.VMEM((peers * slots, features), bf),
            dma((5,)),
            dma((units,)),
            dma((units,)),
            dma((peers,)),
            dma((peers,)),
            dma((units,)),
            dma((units,)),
            dma((8, blocks)),
            dma((8, blocks)),
            dma((units,)),
            dma((units,)),
            dma((units,)),
            dma((units,)),
        ],
        compiler_params=pltpu.CompilerParams(
            collective_id=4, has_side_effects=True, vmem_limit_bytes=66_900_000
        ),
        name="experts",
    )(normed, midway, expert_ids.T, route_weight.T, expert_gate, expert_up, expert_down)


def local(
    receptance,
    key_vectors,
    value_vectors,
    decay_logits,
    rate_logits,
    gate_logits,
    group_gain,
    residual,
    mixer_out,
    norm_gain,
    expert_ids,
    route_weight,
    expert_gate,
    expert_up,
    expert_down,
):
    paired_cores = lax.axis_size("sp") == 2 * GROUPS and lax.axis_size("tp") == 4
    if paired_cores and expert_gate.shape[0] == 1:
        normed, midway = mixed_tokens(
            receptance, key_vectors, value_vectors, decay_logits, rate_logits, gate_logits,
            group_gain, residual, mixer_out, norm_gain,
        )
        return routed_experts(
            normed, midway, expert_ids, route_weight, expert_gate, expert_up, expert_down
        )
    mixed_rows = time_mix(
        receptance, key_vectors, value_vectors, decay_logits, rate_logits, gate_logits, group_gain
    )
    tokens_here, features = residual.shape
    projected = jnp.dot(
        gather_columns(mixed_rows, "tp", 0),
        mixer_out,
        preferred_element_type=jnp.float32,
    )
    midway = (residual.astype(jnp.float32) + projected).astype(jnp.bfloat16)
    midway_f = midway.astype(jnp.float32)
    squares = lax.psum(jnp.sum(midway_f * midway_f, axis=1), "tp")
    inv_rms = lax.rsqrt(squares / D + EPS_NORM)
    normed = (midway_f * norm_gain[None, :] * inv_rms[:, None]).astype(jnp.bfloat16)
    routes = expert_ids.shape[1]
    experts_all = lax.axis_size("sp") * expert_gate.shape[0]
    capacity = 2 * tokens_here * routes // experts_all
    flat_ids = expert_ids.reshape(-1)
    onehot = (flat_ids[:, None] == jnp.arange(experts_all, dtype=jnp.int32)[None, :]).astype(
        jnp.int32
    )
    earlier_count = jnp.sum((jnp.cumsum(onehot, axis=0) - onehot) * onehot, axis=1)
    slot_of = flat_ids * capacity + earlier_count
    owner_token = jnp.arange(tokens_here * routes, dtype=jnp.int32) // routes
    slot_table = (
        jnp.full((experts_all * capacity,), tokens_here, jnp.int32).at[slot_of].set(owner_token)
    )
    padded = jnp.concatenate([normed, jnp.zeros((1, features), jnp.bfloat16)], axis=0)
    outgoing = padded[slot_table].reshape(experts_all, capacity, features)
    arrived = swap_blocks(outgoing, "sp", 2)
    arrived_rows = arrived.reshape(-1, features)
    paired = jnp.concatenate([expert_gate[0], expert_up[0]], axis=1)
    gate_up = lax.psum_scatter(
        jnp.dot(arrived_rows, paired, preferred_element_type=jnp.float32).astype(jnp.bfloat16),
        "tp",
        scatter_dimension=0,
        tiled=True,
    ).astype(jnp.float32)
    half_width = paired.shape[1] // 2
    hidden = (jax.nn.silu(gate_up[:, :half_width]) * gate_up[:, half_width:]).astype(jnp.bfloat16)
    expert_res = jnp.dot(
        gather_rows(hidden, "tp", 1),
        expert_down[0],
        preferred_element_type=jnp.float32,
    )
    returned = swap_blocks(
        expert_res.astype(jnp.bfloat16).reshape(-1, capacity, features), "sp", 3
    )
    picked = (
        returned.reshape(-1, features)[slot_of]
        .astype(jnp.float32)
        .reshape(tokens_here, routes, features)
    )
    routed_sum = jnp.sum(picked * route_weight[:, :, None], axis=1)
    return (midway_f + routed_sum).astype(jnp.bfloat16)


def solution(mesh):
    placed = (
        P("sp", "tp"),
        P("sp", "tp"),
        P("sp", "tp"),
        P("sp", "tp"),
        P("sp", "tp"),
        P("sp", "tp"),
        P("tp"),
        P("sp", "tp"),
        P(None, "tp"),
        P("tp"),
        P("sp", None),
        P("sp", None),
        P("sp", "tp", None),
        P("sp", "tp", None),
        P("sp", None, "tp"),
    )
    return jax.shard_map(
        local, mesh=mesh, in_specs=placed, out_specs=P("sp", "tp"), check_vma=False
    )
```
